32 devices in a mesh: sp: 8 (over z, y), dp: 4 (over x, core).
Axes of the slice: x: 2, y: 2, z: 4, core: 2. Of those that a mesh axis runs over, the one named last changes fastest.
Arguments:
- queries: bfloat16 [4, 2048, 1280], P('dp', None, 'sp'), may hold values from -6 to 6
- keys: bfloat16 [4, 1024, 1280], P('dp', None, 'sp'), may hold values from -6 to 6
- values: bfloat16 [4, 1024, 1280], P('dp', None, 'sp'), may hold values from -48 to 48
- q_gain: float32 [64], replicated, may hold values from 0.5 to 10
- k_gain: float32 [64], replicated, may hold values from 0.5 to 10
- w_out: bfloat16 [2048, 2048], P(None, 'dp'), may hold values from -0.125 to 0.125
Outputs:
- mixed: bfloat16 [4, 1280, 2048], P('dp', 'sp')
The draws below stay inside these ranges and needn't reach their ends.
All inputs are finite; a program needn't handle non-finite values.
Results may differ from the reference program's by a relative error of at most 0.0038.
The reference program's roundings to bfloat16 on the way count: a program that leaves them out, or rounds other values in their place, can miss the bound.
Values may be sent and summed in bfloat16 or wider, within the bound.
No kernel may reach another device: no remote copies, remote signals or barrier semaphores. Data moves between devices by JAX's collectives and lax.ppermute only.
A program may use at most 64 MiB of HBM per device.

```python
import jax
import jax.numpy as jnp
from jax import lax

HD = 64
QH = 32
KV = 16
D = 2048
GRID_W = 64
QW = 2048
KVW = 1024
TOKENS = 1280
SEQ_GROUPS = 4


def shared_keys(key):
    key_draw = jax.random.normal(jax.random.fold_in(key, 11), (SEQ_GROUPS, KVW, TOKENS), jnp.float32)
    return jnp.clip(key_draw, -6.0, 6.0)


def draw_keys(key, part):
    return shared_keys(key).astype(jnp.bfloat16)


def draw_queries(key, part):
    fresh_draw = jax.random.normal(jax.random.fold_in(key, 12), (SEQ_GROUPS, QW, TOKENS), jnp.float32)
    fresh_draw = jnp.clip(fresh_draw, -6.0, 6.0)
    return fresh_draw.astype(jnp.bfloat16)


def gain_draw(key, salt):
    noise_draw = jnp.clip(jax.random.normal(jax.random.fold_in(key, salt), (HD,), jnp.float32), -3.0, 3.0)
    return 1.25 * (1.0 + 0.18 * noise_draw)


def draw_q_gain(key, part):
    return gain_draw(key, 21)


def draw_k_gain(key, part):
    return gain_draw(key, 22)


def steps_of(rng, dims, split, least, top_value):
    level = 1.0
    for axis_at, parts in split:
        draws = jax.random.uniform(jax.random.fold_in(jax.random.fold_in(rng, 6), axis_at), (parts,), jnp.float32, least / len(split), top_value / len(split))
        level = level * jnp.repeat(jnp.exp(draws), dims[axis_at] // parts).reshape((-1,) + (1,) * (len(dims) - 1 - axis_at))
    return level


def noise(rng, shape, spread, reach, split=(), held_as=jnp.bfloat16):
    result = jax.random.normal(rng, shape, jnp.float32) * spread
    if len(split) > 0:
        result = steps_of(rng, shape, split, -0.22, 0.18) * result
    return jnp.clip(result, min=-reach, max=reach).astype(held_as)


def setup_inputs(seed: int = 0) -> dict:
    key_list = jax.random.split(jax.random.key(seed), 7)
    queries = draw_queries(jax.random.fold_in(key_list[6], 71), 0)
    keys = draw_keys(jax.random.fold_in(key_list[6], 71), 0)
    values = noise(key_list[2], (SEQ_GROUPS, KVW, TOKENS), 8.0, 48.0, ((0, 4), (2, 8)))
    q_gain = draw_q_gain(jax.random.fold_in(key_list[6], 71), 0)
    k_gain = draw_k_gain(jax.random.fold_in(key_list[6], 71), 0)
    w_out = noise(key_list[5], (QW, D), QW ** -0.5, 0.125, ((1, 4),))
    return dict(queries=queries, keys=keys, values=values, q_gain=q_gain, k_gain=k_gain, w_out=w_out)


epsilon = 1e-06
rotary_base = 10000.0

def rotary_tables(row_count):
    position = jnp.arange(row_count, dtype=jnp.int32)
    grid_row = (position // GRID_W).astype(jnp.float32)
    grid_col = (position % GRID_W).astype(jnp.float32)
    quarter = HD // 4
    inv_freq = rotary_base ** (-(2.0 * jnp.arange(quarter, dtype=jnp.float32)) / (HD // 2))
    row_angle = inv_freq[:, None] * grid_row[None, :]
    col_angle = inv_freq[:, None] * grid_col[None, :]
    cos_table = jnp.concatenate([jnp.cos(row_angle), jnp.cos(row_angle), jnp.cos(col_angle), jnp.cos(col_angle)], axis=0)
    sin_table = jnp.concatenate([jnp.sin(row_angle), jnp.sin(row_angle), jnp.sin(col_angle), jnp.sin(col_angle)], axis=0)
    return (cos_table, sin_table)

def normalize_turn(field, gain, cos_table, sin_table):
    head_count = field.shape[0] // HD
    values_f = field.astype(jnp.float32).reshape(head_count, HD, field.shape[1])
    normed = values_f * lax.rsqrt(lax.optimization_barrier(jnp.mean(values_f * values_f, axis=1, keepdims=True)) + epsilon) * gain[None, :, None]
    quarter = HD // 4
    quarters_of = normed.reshape(head_count, 4, quarter, field.shape[1])
    turned = jnp.concatenate([-quarters_of[:, 1], quarters_of[:, 0], -quarters_of[:, 3], quarters_of[:, 2]], axis=1)
    return (normed * cos_table[None] + turned * sin_table[None]).astype(jnp.bfloat16)

def reference(queries, keys, values, q_gain, k_gain, w_out):
    cos_table, sin_table = rotary_tables(TOKENS)
    group_size = QH // KV
    score_scale = HD ** (-0.5)

    def per_group(packed):
        query_rows, key_rows, value_rows = packed
        query_rot = normalize_turn(query_rows, q_gain, cos_table, sin_table)
        key_rot = normalize_turn(key_rows, k_gain, cos_table, sin_table)
        value_heads = value_rows.reshape(KV, HD, TOKENS)

        def per_head(head_index):
            query_one = lax.dynamic_index_in_dim(query_rot, head_index, 0, keepdims=False)
            key_one = lax.dynamic_index_in_dim(key_rot, head_index // group_size, 0, keepdims=False)
            value_one = lax.dynamic_index_in_dim(value_heads, head_index // group_size, 0, keepdims=False)
            scores = jnp.einsum('dq,dk->qk', query_one.astype(jnp.float32), key_one.astype(jnp.float32)) * score_scale
            row_max = lax.optimization_barrier(jnp.max(scores, axis=-1, keepdims=True))
            weights = jnp.exp(scores - row_max)
            weights = (weights / lax.optimization_barrier(jnp.sum(weights, axis=-1, keepdims=True))).astype(jnp.bfloat16)
            attended = jnp.einsum('qk,dk->dq', weights.astype(jnp.float32), value_one.astype(jnp.float32))
            return attended.astype(jnp.bfloat16)
        attended = lax.map(per_head, jnp.arange(QH, dtype=jnp.int32)).reshape(QW, TOKENS)
        return jnp.dot(attended.T, w_out, preferred_element_type=jnp.float32).astype(jnp.bfloat16)
    return lax.map(per_group, (queries, keys, values))
```

```python
import functools

import jax
import jax.numpy as jnp
from jax import lax
from jax.experimental import pallas as pl
from jax.experimental.pallas import tpu as pltpu
from jax.sharding import PartitionSpec as P

HD = 64
QH = 32
KV = 16
GRID_W = 64
GROUP = QH // KV
PAIR = GROUP * HD

epsilon = 1e-06
rotary_base = 10000.0
block_count = 8


def swapped(block, axis, apart):
    count = lax.axis_size(axis)
    route = []
    for low in range(count):
        high = low | 1 << apart
        if high != low and high < count:
            route += [(low, high), (high, low)]
    return lax.ppermute(block, axis, route)


def rotary_tables(first_row, row_count):
    position = first_row + lax.iota(jnp.int32, row_count)
    grid_row = (position // GRID_W).astype(jnp.float32)
    grid_col = (position % GRID_W).astype(jnp.float32)
    quarter = HD // 4
    inv_freq = rotary_base ** (-(2.0 * lax.iota(jnp.float32, quarter)) / (HD // 2))
    row_angle = inv_freq[:, None] * grid_row[None, :]
    col_angle = inv_freq[:, None] * grid_col[None, :]
    cos_table = jnp.concatenate(
        [jnp.cos(row_angle), jnp.cos(row_angle), jnp.cos(col_angle), jnp.cos(col_angle)], axis=0
    )
    sin_table = jnp.concatenate(
        [jnp.sin(row_angle), jnp.sin(row_angle), jnp.sin(col_angle), jnp.sin(col_angle)], axis=0
    )
    return (cos_table, sin_table)


def normalize_turn(field, gain, cos_table, sin_table):
    head_count = field.shape[0] // HD
    values_f = field.astype(jnp.float32).reshape(head_count, HD, field.shape[1])
    normed = (
        values_f
        * lax.rsqrt(jnp.mean(values_f * values_f, axis=1, keepdims=True) + epsilon)
        * gain[None, :, None]
    )
    quarter = HD // 4
    quarters_of = normed.reshape(head_count, 4, quarter, field.shape[1])
    turned = jnp.concatenate(
        [-quarters_of[:, 1], quarters_of[:, 0], -quarters_of[:, 3], quarters_of[:, 2]], axis=1
    )
    return (normed * cos_table[None] + turned * sin_table[None]).astype(jnp.bfloat16)


def attention_heads(query_heads, key_heads, value_heads, seq_len):
    kv_local = key_heads.shape[0]
    group_local = query_heads.shape[0] // kv_local
    query_split = query_heads.reshape(kv_local, group_local, HD, seq_len)
    score_scale = HD ** (-0.5)
    block_rows = seq_len // block_count

    def one_block(block_index, result):
        row_start = block_index * block_rows
        query_block = lax.dynamic_slice_in_dim(query_split, row_start, block_rows, 3)
        scores = (
            jnp.einsum("hgdq,hdk->hgqk", query_block, key_heads, preferred_element_type=jnp.float32)
            * score_scale
        )
        row_max = jnp.max(scores, axis=-1, keepdims=True)
        weights = jnp.exp(scores - row_max)
        weights = (weights / jnp.sum(weights, axis=-1, keepdims=True)).astype(jnp.bfloat16)
        attended = jnp.einsum(
            "hgqk,hdk->hgdq", weights, value_heads, preferred_element_type=jnp.float32
        )
        return lax.dynamic_update_slice_in_dim(result, attended.astype(jnp.bfloat16), row_start, 3)

    result = jnp.zeros(query_split.shape, jnp.bfloat16)
    result = lax.fori_loop(0, block_count, one_block, result)
    return result.reshape(query_heads.shape)


def plain_form(queries, keys, values, q_gain, k_gain, w_out):
    sp_count = lax.axis_size("sp")
    tok_rows = queries.shape[2]
    seq_len = tok_rows * sp_count
    cos_table, sin_table = rotary_tables(lax.axis_index("sp") * tok_rows, tok_rows)
    query_rot = normalize_turn(queries[0], q_gain, cos_table, sin_table)
    key_rot = normalize_turn(keys[0], k_gain, cos_table, sin_table)
    value_rows = values[0].reshape(KV, HD, tok_rows)
    query_heads = lax.all_to_all(query_rot, "sp", split_axis=0, concat_axis=2, tiled=True)
    share_count = max(sp_count // KV, 1)
    part_rows = tok_rows // share_count
    key_cut = (
        key_rot.reshape(KV, HD, share_count, part_rows)
        .transpose(0, 2, 1, 3)
        .reshape(KV * share_count, HD, part_rows)
    )
    value_cut = (
        value_rows.reshape(KV, HD, share_count, part_rows)
        .transpose(0, 2, 1, 3)
        .reshape(KV * share_count, HD, part_rows)
    )
    key_got, value_got = (
        lax.all_to_all(key_cut, "sp", split_axis=0, concat_axis=2, tiled=True),
        lax.all_to_all(value_cut, "sp", split_axis=0, concat_axis=2, tiled=True),
    )
    kv_local = key_got.shape[0]
    key_got = key_got.reshape(kv_local, HD, sp_count, part_rows)
    value_got = value_got.reshape(kv_local, HD, sp_count, part_rows)
    for bit_index in range(share_count.bit_length() - 1):
        key_other, value_other = swapped((key_got, value_got), "sp", bit_index)
        key_got = jnp.concatenate([key_got, key_other], axis=3)
        value_got = jnp.concatenate([value_got, value_other], axis=3)
    key_heads = key_got.reshape(kv_local, HD, seq_len)
    value_heads = value_got.reshape(kv_local, HD, seq_len)
    attended = attention_heads(query_heads, key_heads, value_heads, seq_len)
    token_heads = lax.all_to_all(attended, "sp", split_axis=2, concat_axis=0, tiled=True)
    token_rows = token_heads.reshape(QH * HD, tok_rows)
    product = lax.dot_general(
        token_rows,
        lax.all_gather(w_out, "dp", axis=1, tiled=True),
        (((0,), (0,)), ((), ())),
        preferred_element_type=jnp.float32,
    )
    mixed_rows = product.astype(jnp.bfloat16)
    return mixed_rows[None]


def turned_head(rows, gain, cos_table, sin_table):
    field = rows.astype(jnp.float32)
    normed = field * lax.rsqrt(jnp.mean(field * field, axis=0, keepdims=True) + epsilon) * gain
    quarter = HD // 4
    a, b, c, d = (normed[i * quarter : (i + 1) * quarter] for i in range(4))
    turned = jnp.concatenate([-b, a, -d, c], axis=0)
    return normed * cos_table + turned * sin_table


def turn_kernel(heads, q_ref, k_ref, v_ref, qg_ref, kg_ref, cos_ref, sin_ref, *out_refs):
    cos_table, sin_table = cos_ref[...], sin_ref[...]
    q_gain, k_gain = qg_ref[...], kg_ref[...]
    for i in range(heads):
        pair = [
            turned_head(q_ref[(GROUP * i + g) * HD : (GROUP * i + g + 1) * HD, :], q_gain, cos_table, sin_table)
            for g in range(GROUP)
        ]
        key = turned_head(k_ref[i * HD : (i + 1) * HD, :], k_gain, cos_table, sin_table)
        value = v_ref[i * HD : (i + 1) * HD, :].astype(jnp.float32)
        out_ref = out_refs[i]
        out_ref[0, :, :PAIR] = jnp.concatenate(pair, axis=0).T.astype(jnp.bfloat16)
        out_ref[0, :, PAIR:] = jnp.concatenate([key, value], axis=0).T.astype(jnp.bfloat16)


def turn_and_pack(queries, keys, values, q_gain, k_gain, cos_table, sin_table, sp_count):
    tok = queries.shape[1]
    heads = KV // sp_count
    whole = lambda shape: pl.BlockSpec(shape, lambda d: (0,) * len(shape))
    return pl.pallas_call(
        functools.partial(turn_kernel, heads),
        grid=(sp_count,),
        in_specs=[
            pl.BlockSpec((heads * PAIR, tok), lambda d: (d, 0)),
            pl.BlockSpec((heads * HD, tok), lambda d: (d, 0)),
            pl.BlockSpec((heads * HD, tok), lambda d: (d, 0)),
            whole((HD, 1)),
            whole((HD, 1)),
            whole((HD, tok)),
            whole((HD, tok)),
        ],
        out_specs=[pl.BlockSpec((1, tok, PAIR + 2 * HD), lambda d: (d, 0, 0))] * heads,
        out_shape=[jax.ShapeDtypeStruct((sp_count, tok, PAIR + 2 * HD), jnp.bfloat16)] * heads,
        cost_estimate=pl.CostEstimate(flops=40 * 3072 * tok, bytes_accessed=6 * 4096 * tok, transcendentals=0),
        name="turn",
    )(queries, keys, values, q_gain[:, None], k_gain[:, None], cos_table, sin_table)


SOFT_ROWS = 16


def attend_kernel(seq, rows, q_ref, kv_ref, out_ref, keys_scr, vals_scr, s_scr, w_scr):
    @pl.when(pl.program_id(0) == 0)
    def _():
        kv = kv_ref[...].astype(jnp.float32)
        lane = lax.broadcasted_iota(jnp.int32, kv.shape, 1)
        low = lane < HD
        other = pltpu.roll(kv, HD, 1)
        keys_scr[0:seq, :] = jnp.where(low, kv, 0.0).astype(jnp.bfloat16)
        keys_scr[seq : 2 * seq, :] = jnp.where(low, 0.0, other).astype(jnp.bfloat16)
        vals_scr[0:seq, :] = jnp.where(low, other, 0.0).astype(jnp.bfloat16)
        vals_scr[seq : 2 * seq, :] = jnp.where(low, 0.0, kv).astype(jnp.bfloat16)

    scale = HD ** (-0.5)
    s_scr[...] = lax.dot_general(
        q_ref[...], keys_scr[...], (((1,), (1,)), ((), ())), preferred_element_type=jnp.float32
    )
    for g in range(GROUP):
        for r in range(0, rows, SOFT_ROWS):
            s = s_scr[r : r + SOFT_ROWS, g * seq : (g + 1) * seq] * scale
            e = jnp.exp(s - jnp.max(s, axis=-1, keepdims=True))
            w = e * (1.0 / jnp.sum(e, axis=-1, keepdims=True))
            w_scr[r : r + SOFT_ROWS, g * seq : (g + 1) * seq] = w.astype(jnp.bfloat16)
    out_ref[...] = jnp.dot(w_scr[...], vals_scr[...], preferred_element_type=jnp.float32).astype(jnp.bfloat16)


def attend(packed):
    sp_count, tok, _ = packed.shape
    seq = sp_count * tok
    flat = packed.reshape(seq, PAIR + 2 * HD)
    rows = 256 if seq % 256 == 0 else tok
    return pl.pallas_call(
        functools.partial(attend_kernel, seq, rows),
        grid=(seq // rows,),
        in_specs=[
            pl.BlockSpec((rows, PAIR), lambda b: (b, 0)),
            pl.BlockSpec((seq, 2 * HD), lambda b: (0, 1)),
        ],
        out_specs=pl.BlockSpec((rows, PAIR), lambda b: (b, 0)),
        out_shape=jax.ShapeDtypeStruct((seq, PAIR), jnp.bfloat16),
        scratch_shapes=[
            pltpu.VMEM((GROUP * seq, 2 * HD), jnp.bfloat16),
            pltpu.VMEM((GROUP * seq, PAIR), jnp.bfloat16),
            pltpu.VMEM((rows, GROUP * seq), jnp.float32),
            pltpu.VMEM((rows, GROUP * seq), jnp.bfloat16),
        ],
        cost_estimate=pl.CostEstimate(
            flops=16 * seq * seq * HD, bytes_accessed=8 * seq * PAIR, transcendentals=GROUP * seq * seq
        ),
        name="attend",
    )(flat, flat).reshape(sp_count, tok, PAIR)


def project_kernel(parts, sp_count, att_refs, w_refs, out_ref, bufs, sems):
    me = lax.axis_index("dp")
    width = w_refs[0].shape[1]
    copies = [pltpu.make_async_copy(w_refs[i], bufs.at[i], sems.at[i]) for i in range(parts)]
    for copy in copies:
        copy.start()
    att = jnp.concatenate([att_ref[d] for d in range(sp_count) for att_ref in att_refs], axis=1)
    for i in range(parts):
        copies[i].wait()
        column = pl.multiple_of((me ^ i) * width, width)
        out_ref[:, pl.ds(column, width)] = jnp.dot(
            att, bufs[i], preferred_element_type=jnp.float32
        ).astype(jnp.bfloat16)


def project(attended, blocks):
    parts, heads = len(blocks), len(attended)
    sp_count, tok, _ = attended[0].shape
    depth, width = blocks[0].shape

    def body(*refs):
        project_kernel(parts, sp_count, refs[:heads], refs[heads : heads + parts], *refs[heads + parts :])

    return pl.pallas_call(
        body,
        in_specs=[pl.BlockSpec(memory_space=pltpu.VMEM)] * heads + [pl.BlockSpec(memory_space=pl.ANY)] * parts,
        out_specs=pl.BlockSpec(memory_space=pltpu.VMEM),
        out_shape=jax.ShapeDtypeStruct((tok, parts * width), jnp.bfloat16),
        scratch_shapes=[pltpu.VMEM((parts, depth, width), jnp.bfloat16), pltpu.SemaphoreType.DMA((parts,))],
        cost_estimate=pl.CostEstimate(
            flops=2 * tok * depth * width * parts, bytes_accessed=2 * depth * width * parts, transcendentals=0
        ),
        name="project",
    )(*attended, *blocks)


def column_blocks(w_out):
    count = lax.axis_size("dp")
    blocks = {0: w_out}
    for bit in reversed(range(count.bit_length() - 1)):
        route = [(i, i ^ (1 << bit)) for i in range(count)]
        for key in sorted(blocks):
            blocks[key | (1 << bit)] = lax.ppermute(blocks[key], "dp", route)
    return [blocks[i] for i in range(count)]


def head_form(queries, keys, values, q_gain, k_gain, w_out):
    sp_count = lax.axis_size("sp")
    tok = queries.shape[2]
    blocks = column_blocks(w_out)
    cos_table, sin_table = rotary_tables(lax.axis_index("sp") * tok, tok)
    packed = turn_and_pack(queries[0], keys[0], values[0], q_gain, k_gain, cos_table, sin_table, sp_count)
    attended = []
    for part in packed:
        got = lax.all_to_all(part, "sp", split_axis=0, concat_axis=0, tiled=True)
        attended.append(lax.all_to_all(attend(got), "sp", split_axis=0, concat_axis=0, tiled=True))
    return project(attended, blocks)[None]


def on_device(*args):
    sp_count, dp_count = lax.axis_size("sp"), lax.axis_size("dp")
    if KV % sp_count == 0 and dp_count & (dp_count - 1) == 0:
        return head_form(*args)
    return plain_form(*args)


def solution(mesh):
    placed = (
        P("dp", None, "sp"),
        P("dp", None, "sp"),
        P("dp", None, "sp"),
        P(),
        P(),
        P(None, "dp"),
    )
    return jax.shard_map(
        on_device, mesh=mesh, in_specs=placed, out_specs=P("dp", "sp", None), check_vma=False
    )
```

```python
import functools

import jax
import jax.numpy as jnp
from jax import lax
from jax.experimental import pallas as pl
from jax.experimental.pallas import tpu as pltpu
from jax.sharding import PartitionSpec as P

HD = 64
QH = 32
KV = 16
GRID_W = 64
GROUP = QH // KV

epsilon = 1e-06
rotary_base = 10000.0
block_count = 8


def swapped(block, axis, apart):
    count = lax.axis_size(axis)
    route = []
    for low in range(count):
        high = low | 1 << apart
        if high != low and high < count:
            route += [(low, high), (high, low)]
    return lax.ppermute(block, axis, route)


def rotary_tables(first_row, row_count):
    position = first_row + lax.iota(jnp.int32, row_count)
    grid_row = (position // GRID_W).astype(jnp.float32)
    grid_col = (position % GRID_W).astype(jnp.float32)
    quarter = HD // 4
    inv_freq = rotary_base ** (-(2.0 * lax.iota(jnp.float32, quarter)) / (HD // 2))
    row_angle = inv_freq[:, None] * grid_row[None, :]
    col_angle = inv_freq[:, None] * grid_col[None, :]
    cos_table = jnp.concatenate(
        [jnp.cos(row_angle), jnp.cos(row_angle), jnp.cos(col_angle), jnp.cos(col_angle)], axis=0
    )
    sin_table = jnp.concatenate(
        [jnp.sin(row_angle), jnp.sin(row_angle), jnp.sin(col_angle), jnp.sin(col_angle)], axis=0
    )
    return (cos_table, sin_table)


def normalize_turn(field, gain, cos_table, sin_table):
    head_count = field.shape[0] // HD
    values_f = field.astype(jnp.float32).reshape(head_count, HD, field.shape[1])
    normed = (
        values_f
        * lax.rsqrt(jnp.mean(values_f * values_f, axis=1, keepdims=True) + epsilon)
        * gain[None, :, None]
    )
    quarter = HD // 4
    quarters_of = normed.reshape(head_count, 4, quarter, field.shape[1])
    turned = jnp.concatenate(
        [-quarters_of[:, 1], quarters_of[:, 0], -quarters_of[:, 3], quarters_of[:, 2]], axis=1
    )
    return (normed * cos_table[None] + turned * sin_table[None]).astype(jnp.bfloat16)


def attention_heads(query_heads, key_heads, value_heads, seq_len):
    kv_local = key_heads.shape[0]
    group_local = query_heads.shape[0] // kv_local
    query_split = query_heads.reshape(kv_local, group_local, HD, seq_len)
    score_scale = HD ** (-0.5)
    block_rows = seq_len // block_count

    def one_block(block_index, result):
        row_start = block_index * block_rows
        query_block = lax.dynamic_slice_in_dim(query_split, row_start, block_rows, 3)
        scores = (
            jnp.einsum("hgdq,hdk->hgqk", query_block, key_heads, preferred_element_type=jnp.float32)
            * score_scale
        )
        row_max = jnp.max(scores, axis=-1, keepdims=True)
        weights = jnp.exp(scores - row_max)
        weights = (weights / jnp.sum(weights, axis=-1, keepdims=True)).astype(jnp.bfloat16)
        attended = jnp.einsum(
            "hgqk,hdk->hgdq", weights, value_heads, preferred_element_type=jnp.float32
        )
        return lax.dynamic_update_slice_in_dim(result, attended.astype(jnp.bfloat16), row_start, 3)

    result = jnp.zeros(query_split.shape, jnp.bfloat16)
    result = lax.fori_loop(0, block_count, one_block, result)
    return result.reshape(query_heads.shape)


def plain_form(queries, keys, values, q_gain, k_gain, w_out):
    sp_count = lax.axis_size("sp")
    tok_rows = queries.shape[2]
    seq_len = tok_rows * sp_count
    cos_table, sin_table = rotary_tables(lax.axis_index("sp") * tok_rows, tok_rows)
    query_rot = normalize_turn(queries[0], q_gain, cos_table, sin_table)
    key_rot = normalize_turn(keys[0], k_gain, cos_table, sin_table)
    value_rows = values[0].reshape(KV, HD, tok_rows)
    query_heads = lax.all_to_all(query_rot, "sp", split_axis=0, concat_axis=2, tiled=True)
    share_count = max(sp_count // KV, 1)
    part_rows = tok_rows // share_count
    key_cut = (
        key_rot.reshape(KV, HD, share_count, part_rows)
        .transpose(0, 2, 1, 3)
        .reshape(KV * share_count, HD, part_rows)
    )
    value_cut = (
        value_rows.reshape(KV, HD, share_count, part_rows)
        .transpose(0, 2, 1, 3)
        .reshape(KV * share_count, HD, part_rows)
    )
    key_got, value_got = (
        lax.all_to_all(key_cut, "sp", split_axis=0, concat_axis=2, tiled=True),
        lax.all_to_all(value_cut, "sp", split_axis=0, concat_axis=2, tiled=True),
    )
    kv_local = key_got.shape[0]
    key_got = key_got.reshape(kv_local, HD, sp_count, part_rows)
    value_got = value_got.reshape(kv_local, HD, sp_count, part_rows)
    for bit_index in range(share_count.bit_length() - 1):
        key_other, value_other = swapped((key_got, value_got), "sp", bit_index)
        key_got = jnp.concatenate([key_got, key_other], axis=3)
        value_got = jnp.concatenate([value_got, value_other], axis=3)
    key_heads = key_got.reshape(kv_local, HD, seq_len)
    value_heads = value_got.reshape(kv_local, HD, seq_len)
    attended = attention_heads(query_heads, key_heads, value_heads, seq_len)
    token_heads = lax.all_to_all(attended, "sp", split_axis=2, concat_axis=0, tiled=True)
    token_rows = token_heads.reshape(QH * HD, tok_rows)
    product = lax.dot_general(
        token_rows,
        lax.all_gather(w_out, "dp", axis=1, tiled=True),
        (((0,), (0,)), ((), ())),
        preferred_element_type=jnp.float32,
    )
    mixed_rows = product.astype(jnp.bfloat16)
    return mixed_rows[None]


TILE = 128


def rotary_lanes(first_row, row_count):
    position = first_row + lax.broadcasted_iota(jnp.int32, (row_count, TILE), 0)
    lane = lax.broadcasted_iota(jnp.int32, (row_count, TILE), 1) % HD
    quarter = HD // 4
    inv_freq = rotary_base ** (-(2.0 * (lane % quarter).astype(jnp.float32)) / (HD // 2))
    place = jnp.where(lane < HD // 2, position // GRID_W, position % GRID_W).astype(jnp.float32)
    angle = inv_freq * place
    sine = jnp.sin(angle)
    return jnp.cos(angle), jnp.where((lane // quarter) % 2 == 0, -sine, sine)


def turn_kernel(groups, chunks, q_ref, k_ref, v_ref, qg_ref, kg_ref, cos_ref, sin_ref, *out_refs):
    home = lax.axis_index("sp") % groups
    cos_table, sin_table = cos_ref[...], sin_ref[...]
    quarter = HD // 4
    lane = lax.broadcasted_iota(jnp.int32, cos_table.shape, 1)
    even = (lane // quarter) % 2 == 0
    row_head = (lax.broadcasted_iota(jnp.int32, (2 * TILE, TILE), 0) % TILE) // HD
    col_head = lax.broadcasted_iota(jnp.int32, (2 * TILE, TILE), 1) // HD
    average = jnp.where(row_head == col_head, 1.0 / HD, 0.0).astype(jnp.bfloat16)

    def turned(tile, gain):
        field = tile.astype(jnp.float32)
        square = field * field
        coarse = square.astype(jnp.bfloat16)
        fine = (square - coarse.astype(jnp.float32)).astype(jnp.bfloat16)
        mean = jnp.dot(
            jnp.concatenate([coarse, fine], axis=1), average, preferred_element_type=jnp.float32
        )
        normed = field * lax.rsqrt(mean + epsilon) * gain
        partner = jnp.where(even, pltpu.roll(normed, TILE - quarter, 1), pltpu.roll(normed, quarter, 1))
        return (normed * cos_table + partner * sin_table).astype(jnp.bfloat16)

    both_refs, kv_refs = out_refs[: groups * chunks], out_refs[groups * chunks :]
    for c in range(chunks):
        for j in range(groups):
            place = (home ^ j) * chunks + c
            both, kv = both_refs[c * groups + j], kv_refs[c * groups + j]
            for p in range(2):
                lanes = pl.ds(pl.multiple_of((place * 2 + p) * TILE, TILE), TILE)
                both[:, p * TILE : (p + 1) * TILE] = turned(q_ref[:, lanes], qg_ref[...])
            lanes = pl.ds(pl.multiple_of(place * TILE, TILE), TILE)
            key, value = turned(k_ref[:, lanes], kg_ref[...]), v_ref[:, lanes]
            both[:, 2 * TILE : 3 * TILE] = key
            both[:, 3 * TILE :] = value
            kv[:, :TILE] = key
            kv[:, TILE:] = value


def in_vmem(count):
    return [pl.BlockSpec(memory_space=pltpu.VMEM)] * count


def params(mib):
    return pltpu.CompilerParams(vmem_limit_bytes=mib << 20)


def turn_and_pack(queries, keys, values, q_gain, k_gain, cos_table, sin_table, groups, chunks):
    tok = queries.shape[0]
    made = groups * chunks
    out = pl.pallas_call(
        functools.partial(turn_kernel, groups, chunks),
        in_specs=in_vmem(7),
        out_specs=in_vmem(2 * made),
        out_shape=[jax.ShapeDtypeStruct((tok, 4 * TILE), jnp.bfloat16)] * made
        + [jax.ShapeDtypeStruct((tok, 2 * TILE), jnp.bfloat16)] * made,
        compiler_params=params(16),
        cost_estimate=pl.CostEstimate(flops=40 * 3072 * tok, bytes_accessed=6 * 4096 * tok, transcendentals=0),
        name="turn",
    )(queries, keys, values, jnp.tile(q_gain[None], (1, 2)), jnp.tile(k_gain[None], (1, 2)), cos_table, sin_table)
    both = [out[c * groups : (c + 1) * groups] for c in range(chunks)]
    kv = [out[made + c * groups : made + (c + 1) * groups] for c in range(chunks)]
    return both, kv


SOFT_ROWS = 16


def attend_kernel(groups, *refs):
    both_refs, far_refs, out_refs = refs[:groups], refs[groups : 2 * groups], refs[2 * groups : 3 * groups]
    keys_scr, vals_scr, s_scr, w_scr = refs[3 * groups :]
    rows = both_refs[0].shape[0]
    seq = 2 * groups * rows
    pair = pl.program_id(0)
    first = pair == 0
    low = lax.broadcasted_iota(jnp.int32, (rows, TILE), 1) < HD

    def spread(tile, scr, i):
        tile = tile.astype(jnp.float32)
        other = pltpu.roll(tile, HD, 1)
        here, there = jnp.where(first, tile, other), jnp.where(first, other, tile)
        scr[i * rows : (i + 1) * rows, :] = jnp.where(low, here, 0.0).astype(jnp.bfloat16)
        scr[seq + i * rows : seq + (i + 1) * rows, :] = jnp.where(low, 0.0, there).astype(jnp.bfloat16)

    for i in range(groups):
        spread(both_refs[i][:, 2 * TILE : 3 * TILE], keys_scr, i)
        spread(both_refs[i][:, 3 * TILE :], vals_scr, i)
        spread(far_refs[i][:, :TILE], keys_scr, groups + i)
        spread(far_refs[i][:, TILE:], vals_scr, groups + i)

    factor = HD ** (-0.5) * 1.4426950408889634
    lanes = pl.ds(pl.multiple_of(pair * TILE, TILE), TILE)
    for j in range(groups):
        slot = j % 2
        s_scr[slot] = lax.dot_general(
            both_refs[j][:, lanes], keys_scr[...], (((1,), (1,)), ((), ())), preferred_element_type=jnp.float32
        )
        for g in range(GROUP):
            for r in range(0, rows, SOFT_ROWS):
                s = s_scr[slot, r : r + SOFT_ROWS, g * seq : (g + 1) * seq]
                e = jnp.exp2((s - jnp.max(s, axis=-1, keepdims=True)) * factor)
                w = e * (1.0 / jnp.sum(e, axis=-1, keepdims=True))
                w_scr[slot, r : r + SOFT_ROWS, g * seq : (g + 1) * seq] = w.astype(jnp.bfloat16)
        out_refs[j][:, lanes] = jnp.dot(
            w_scr[slot], vals_scr[...], preferred_element_type=jnp.float32
        ).astype(jnp.bfloat16)


def attend(both, far):
    groups = len(both)
    rows = both[0].shape[0]
    seq = 2 * groups * rows
    return pl.pallas_call(
        functools.partial(attend_kernel, groups),
        grid=(2,),
        in_specs=in_vmem(2 * groups),
        out_specs=in_vmem(groups),
        out_shape=[jax.ShapeDtypeStruct((rows, 2 * TILE), jnp.bfloat16)] * groups,
        scratch_shapes=[
            pltpu.VMEM((GROUP * seq, TILE), jnp.bfloat16),
            pltpu.VMEM((GROUP * seq, TILE), jnp.bfloat16),
            pltpu.VMEM((2, rows, GROUP * seq), jnp.float32),
            pltpu.VMEM((2, rows, GROUP * seq), jnp.bfloat16),
        ],
        compiler_params=params(24),
        cost_estimate=pl.CostEstimate(
            flops=16 * groups * rows * seq * HD, bytes_accessed=12 * seq * TILE, transcendentals=0
        ),
        name="attend",
    )(*both, *far)


def project_kernel(groups, parts, chunks, chunk, last, *refs):
    att_refs, w_refs = refs[:groups], refs[groups : groups + parts]
    acc_ref = refs[groups + parts] if chunk > 0 else None
    out_ref = refs[-1]
    me, home = lax.axis_index("dp"), lax.axis_index("sp") % groups
    width = w_refs[0].shape[1]
    for i in range(parts):
        column = pl.ds(pl.multiple_of((me ^ i) * width, width), width)
        total = acc_ref[:, column] if chunk > 0 else None
        for j in range(groups):
            row = pl.ds(pl.multiple_of(((home ^ j) * chunks + chunk) * 2 * TILE, 2 * TILE), 2 * TILE)
            term = jnp.dot(att_refs[j][...], w_refs[i][row, :], preferred_element_type=jnp.float32)
            total = term if total is None else total + term
        out_ref[:, column] = total.astype(out_ref.dtype)


def project(attended, blocks, acc, chunk, chunks):
    parts, groups = len(blocks), len(attended)
    last = chunk == chunks - 1
    tok = attended[0].shape[0]
    depth, width = blocks[0].shape
    extra = [] if acc is None else [acc]
    return pl.pallas_call(
        functools.partial(project_kernel, groups, parts, chunks, chunk, last),
        in_specs=in_vmem(groups + parts + len(extra)),
        out_specs=pl.BlockSpec(memory_space=pltpu.VMEM),
        out_shape=jax.ShapeDtypeStruct((tok, parts * width), jnp.bfloat16 if last else jnp.float32),
        compiler_params=params(16),
        cost_estimate=pl.CostEstimate(
            flops=2 * tok * depth * width * parts // chunks, bytes_accessed=2 * depth * width * parts // chunks,
            transcendentals=0,
        ),
        name="project",
    )(*attended, *blocks, *extra)


def exchanged(block, axis, flip):
    count = lax.axis_size(axis)
    return lax.ppermute(block, axis, [(i, i ^ flip) for i in range(count)])


def group_form(queries, keys, values, q_gain, k_gain, w_out):
    sp_count, dp_count = lax.axis_size("sp"), lax.axis_size("dp")
    tok = queries.shape[2]
    groups = sp_count // 2
    chunks = KV // groups // 2
    blocks = {0: w_out}
    bits = dp_count.bit_length() - 1
    top = 1 << (bits - 1)
    blocks[top] = exchanged(w_out, "dp", top)
    cos_table, sin_table = rotary_lanes(lax.axis_index("sp") * tok, tok)
    both, kv = turn_and_pack(
        queries[0].T, keys[0].T, values[0].T, q_gain, k_gain, cos_table, sin_table, groups, chunks
    )
    near, far = [], []
    for c in range(chunks):
        near.append([both[c][0]] + [exchanged(both[c][j], "sp", j) for j in range(1, groups)])
        far.append([exchanged(kv[c][j], "sp", groups + j) for j in range(groups)])
    back = []
    for c in range(chunks):
        done = attend(near[c], far[c])
        back.append([done[0]] + [exchanged(done[j], "sp", j) for j in range(1, groups)])
        if c == 0:
            blocks[top], back[0][0] = lax.optimization_barrier((blocks[top], back[0][0]))
            for bit in reversed(range(bits - 1)):
                for key in sorted(blocks):
                    blocks[key | (1 << bit)] = exchanged(blocks[key], "dp", 1 << bit)
    listed = [blocks[i] for i in range(dp_count)]
    acc = None
    for c in range(chunks):
        acc = project(back[c], listed, acc, c, chunks)
    return acc[None]


def on_device(*args):
    sp_count, dp_count = lax.axis_size("sp"), lax.axis_size("dp")
    powers = sp_count & (sp_count - 1) == 0 and dp_count & (dp_count - 1) == 0
    if powers and sp_count > 2 and dp_count > 1 and KV % sp_count == 0:
        return group_form(*args)
    return plain_form(*args)


def solution(mesh):
    placed = (
        P("dp", None, "sp"),
        P("dp", None, "sp"),
        P("dp", None, "sp"),
        P(),
        P(),
        P(None, "dp"),
    )
    return jax.shard_map(
        on_device, mesh=mesh, in_specs=placed, out_specs=P("dp", "sp", None), check_vma=False
    )
```

```python
import functools

import jax
import jax.numpy as jnp
from jax import lax
from jax.experimental import pallas as pl
from jax.experimental.pallas import tpu as pltpu
from jax.sharding import PartitionSpec as P


HD = 64
QH = 32
KV = 16
GRID_W = 64
GROUP = QH // KV

epsilon = 1e-06
rotary_base = 10000.0
block_count = 8


def swapped(block, axis, apart):
    count = lax.axis_size(axis)
    route = []
    for low in range(count):
        high = low | 1 << apart
        if high != low and high < count:
            route += [(low, high), (high, low)]
    return lax.ppermute(block, axis, route)


def rotary_tables(first_row, row_count):
    position = first_row + lax.iota(jnp.int32, row_count)
    grid_row = (position // GRID_W).astype(jnp.float32)
    grid_col = (position % GRID_W).astype(jnp.float32)
    quarter = HD // 4
    inv_freq = rotary_base ** (-(2.0 * lax.iota(jnp.float32, quarter)) / (HD // 2))
    row_angle = inv_freq[:, None] * grid_row[None, :]
    col_angle = inv_freq[:, None] * grid_col[None, :]
    cos_table = jnp.concatenate(
        [jnp.cos(row_angle), jnp.cos(row_angle), jnp.cos(col_angle), jnp.cos(col_angle)], axis=0
    )
    sin_table = jnp.concatenate(
        [jnp.sin(row_angle), jnp.sin(row_angle), jnp.sin(col_angle), jnp.sin(col_angle)], axis=0
    )
    return (cos_table, sin_table)


def normalize_turn(field, gain, cos_table, sin_table):
    head_count = field.shape[0] // HD
    values_f = field.astype(jnp.float32).reshape(head_count, HD, field.shape[1])
    normed = (
        values_f
        * lax.rsqrt(jnp.mean(values_f * values_f, axis=1, keepdims=True) + epsilon)
        * gain[None, :, None]
    )
    quarter = HD // 4
    quarters_of = normed.reshape(head_count, 4, quarter, field.shape[1])
    turned = jnp.concatenate(
        [-quarters_of[:, 1], quarters_of[:, 0], -quarters_of[:, 3], quarters_of[:, 2]], axis=1
    )
    return (normed * cos_table[None] + turned * sin_table[None]).astype(jnp.bfloat16)


def attention_heads(query_heads, key_heads, value_heads, seq_len):
    kv_local = key_heads.shape[0]
    group_local = query_heads.shape[0] // kv_local
    query_split = query_heads.reshape(kv_local, group_local, HD, seq_len)
    score_scale = HD ** (-0.5)
    block_rows = seq_len // block_count

    def one_block(block_index, result):
        row_start = block_index * block_rows
        query_block = lax.dynamic_slice_in_dim(query_split, row_start, block_rows, 3)
        scores = (
            jnp.einsum("hgdq,hdk->hgqk", query_block, key_heads, preferred_element_type=jnp.float32)
            * score_scale
        )
        row_max = jnp.max(scores, axis=-1, keepdims=True)
        weights = jnp.exp(scores - row_max)
        weights = (weights / jnp.sum(weights, axis=-1, keepdims=True)).astype(jnp.bfloat16)
        attended = jnp.einsum(
            "hgqk,hdk->hgdq", weights, value_heads, preferred_element_type=jnp.float32
        )
        return lax.dynamic_update_slice_in_dim(result, attended.astype(jnp.bfloat16), row_start, 3)

    result = jnp.zeros(query_split.shape, jnp.bfloat16)
    result = lax.fori_loop(0, block_count, one_block, result)
    return result.reshape(query_heads.shape)


def plain_form(queries, keys, values, q_gain, k_gain, w_out):
    sp_count = lax.axis_size("sp")
    tok_rows = queries.shape[2]
    seq_len = tok_rows * sp_count
    cos_table, sin_table = rotary_tables(lax.axis_index("sp") * tok_rows, tok_rows)
    query_rot = normalize_turn(queries[0], q_gain, cos_table, sin_table)
    key_rot = normalize_turn(keys[0], k_gain, cos_table, sin_table)
    value_rows = values[0].reshape(KV, HD, tok_rows)
    query_heads = lax.all_to_all(query_rot, "sp", split_axis=0, concat_axis=2, tiled=True)
    share_count = max(sp_count // KV, 1)
    part_rows = tok_rows // share_count
    key_cut = (
        key_rot.reshape(KV, HD, share_count, part_rows)
        .transpose(0, 2, 1, 3)
        .reshape(KV * share_count, HD, part_rows)
    )
    value_cut = (
        value_rows.reshape(KV, HD, share_count, part_rows)
        .transpose(0, 2, 1, 3)
        .reshape(KV * share_count, HD, part_rows)
    )
    key_got, value_got = (
        lax.all_to_all(key_cut, "sp", split_axis=0, concat_axis=2, tiled=True),
        lax.all_to_all(value_cut, "sp", split_axis=0, concat_axis=2, tiled=True),
    )
    kv_local = key_got.shape[0]
    key_got = key_got.reshape(kv_local, HD, sp_count, part_rows)
    value_got = value_got.reshape(kv_local, HD, sp_count, part_rows)
    for bit_index in range(share_count.bit_length() - 1):
        key_other, value_other = swapped((key_got, value_got), "sp", bit_index)
        key_got = jnp.concatenate([key_got, key_other], axis=3)
        value_got = jnp.concatenate([value_got, value_other], axis=3)
    key_heads = key_got.reshape(kv_local, HD, seq_len)
    value_heads = value_got.reshape(kv_local, HD, seq_len)
    attended = attention_heads(query_heads, key_heads, value_heads, seq_len)
    token_heads = lax.all_to_all(attended, "sp", split_axis=2, concat_axis=0, tiled=True)
    token_rows = token_heads.reshape(QH * HD, tok_rows)
    product = lax.dot_general(
        token_rows,
        lax.all_gather(w_out, "dp", axis=1, tiled=True),
        (((0,), (0,)), ((), ())),
        preferred_element_type=jnp.float32,
    )
    mixed_rows = product.astype(jnp.bfloat16)
    return mixed_rows[None]


TILE = 128


def rotary_lanes(first_row, row_count):
    position = first_row + lax.broadcasted_iota(jnp.int32, (row_count, TILE), 0)
    lane = lax.broadcasted_iota(jnp.int32, (row_count, TILE), 1) % HD
    quarter = HD // 4
    inv_freq = rotary_base ** (-(2.0 * (lane % quarter).astype(jnp.float32)) / (HD // 2))
    place = jnp.where(lane < HD // 2, position // GRID_W, position % GRID_W).astype(jnp.float32)
    angle = inv_freq * place
    sine = jnp.sin(angle)
    return jnp.cos(angle), jnp.where((lane // quarter) % 2 == 0, -sine, sine)


def turn_kernel(groups, chunks, *refs):
    sources, (cos_ref, sin_ref), out_refs = refs[:5], refs[5:7], refs[7:-6]
    held, sems = refs[-6:-1], refs[-1]
    copies = [pltpu.make_async_copy(src, dst, sems.at[i]) for i, (src, dst) in enumerate(zip(sources, held))]
    for copy in copies:
        copy.start()
    for copy in copies:
        copy.wait()
    q_ref, k_ref, v_ref, qg_ref, kg_ref = held
    home = lax.axis_index("sp") % groups
    cos_table, sin_table = cos_ref[...], sin_ref[...]
    q_gain = jnp.concatenate([qg_ref[...]] * 2, axis=1)
    k_gain = jnp.concatenate([kg_ref[...]] * 2, axis=1)
    quarter = HD // 4
    lane = lax.broadcasted_iota(jnp.int32, cos_table.shape, 1)
    even = (lane // quarter) % 2 == 0
    row_head = (lax.broadcasted_iota(jnp.int32, (2 * TILE, TILE), 0) % TILE) // HD
    col_head = lax.broadcasted_iota(jnp.int32, (2 * TILE, TILE), 1) // HD
    average = jnp.where(row_head == col_head, 1.0 / HD, 0.0).astype(jnp.bfloat16)

    def turned(tile, gain):
        field = tile.astype(jnp.float32)
        square = field * field
        coarse = square.astype(jnp.bfloat16)
        fine = (square - coarse.astype(jnp.float32)).astype(jnp.bfloat16)
        mean = jnp.dot(
            jnp.concatenate([coarse, fine], axis=1), average, preferred_element_type=jnp.float32
        )
        normed = field * lax.rsqrt(mean + epsilon) * gain
        partner = jnp.where(even, pltpu.roll(normed, TILE - quarter, 1), pltpu.roll(normed, quarter, 1))
        return (normed * cos_table + partner * sin_table).astype(jnp.bfloat16)

    both_refs, kv_refs = out_refs[: groups * chunks], out_refs[groups * chunks :]
    for c in range(chunks):
        for j in range(groups):
            place = (home ^ j) * chunks + c
            both, kv = both_refs[c * groups + j], kv_refs[c * groups + j]
            for p in range(2):
                lanes = pl.ds(pl.multiple_of((place * 2 + p) * TILE, TILE), TILE)
                both[:, p * TILE : (p + 1) * TILE] = turned(q_ref[:, lanes], q_gain)
            lanes = pl.ds(pl.multiple_of(place * TILE, TILE), TILE)
            key, value = turned(k_ref[:, lanes], k_gain), v_ref[:, lanes]
            both[:, 2 * TILE : 3 * TILE] = key
            both[:, 3 * TILE :] = value
            kv[:, :TILE] = key
            kv[:, TILE:] = value


def in_vmem(count):
    return [pl.BlockSpec(memory_space=pltpu.VMEM)] * count


def params(mib):
    return pltpu.CompilerParams(vmem_limit_bytes=mib << 20)


def turn_and_pack(queries, keys, values, q_gain, k_gain, cos_table, sin_table, groups, chunks):
    tok = queries.shape[0]
    made = groups * chunks
    out = pl.pallas_call(
        functools.partial(turn_kernel, groups, chunks),
        in_specs=[pl.BlockSpec(memory_space=pltpu.HBM)] * 5 + in_vmem(2),
        out_specs=in_vmem(2 * made),
        out_shape=[jax.ShapeDtypeStruct((tok, 4 * TILE), jnp.bfloat16)] * made
        + [jax.ShapeDtypeStruct((tok, 2 * TILE), jnp.bfloat16)] * made,
        scratch_shapes=[pltpu.VMEM(x.shape, x.dtype) for x in (queries, keys, values)]
        + [pltpu.VMEM((1, HD), jnp.float32)] * 2
        + [pltpu.SemaphoreType.DMA((5,))],
        compiler_params=params(16),
        cost_estimate=pl.CostEstimate(flops=40 * 3072 * tok, bytes_accessed=6 * 4096 * tok, transcendentals=0),
        name="turn",
    )(queries, keys, values, q_gain[None], k_gain[None], cos_table, sin_table)
    both = [out[c * groups : (c + 1) * groups] for c in range(chunks)]
    kv = [out[made + c * groups : made + (c + 1) * groups] for c in range(chunks)]
    return both, kv


SOFT_ROWS = 16


def attend_kernel(groups, *refs):
    both_refs, far_refs, out_refs = refs[:groups], refs[groups : 2 * groups], refs[2 * groups : 3 * groups]
    keys_scr, vals_scr, s_scr, w_scr = refs[3 * groups :]
    rows = both_refs[0].shape[0]
    seq = 2 * groups * rows
    pair = pl.program_id(0)
    first = pair == 0
    low = lax.broadcasted_iota(jnp.int32, (rows, TILE), 1) < HD

    def spread(tile, scr, i):
        tile = tile.astype(jnp.float32)
        other = pltpu.roll(tile, HD, 1)
        here, there = jnp.where(first, tile, other), jnp.where(first, other, tile)
        scr[i * rows : (i + 1) * rows, :] = jnp.where(low, here, 0.0).astype(jnp.bfloat16)
        scr[seq + i * rows : seq + (i + 1) * rows, :] = jnp.where(low, 0.0, there).astype(jnp.bfloat16)

    for i in range(groups):
        spread(both_refs[i][:, 2 * TILE : 3 * TILE], keys_scr, i)
        spread(both_refs[i][:, 3 * TILE :], vals_scr, i)
        spread(far_refs[i][:, :TILE], keys_scr, groups + i)
        spread(far_refs[i][:, TILE:], vals_scr, groups + i)

    factor = HD ** (-0.5) * 1.4426950408889634
    lanes = pl.ds(pl.multiple_of(pair * TILE, TILE), TILE)
    for j in range(groups):
        slot = j % 2
        s_scr[slot] = lax.dot_general(
            both_refs[j][:, lanes], keys_scr[...], (((1,), (1,)), ((), ())), preferred_element_type=jnp.float32
        )
        for g in range(GROUP):
            for r in range(0, rows, SOFT_ROWS):
                s = s_scr[slot, r : r + SOFT_ROWS, g * seq : (g + 1) * seq]
                e = jnp.exp2((s - jnp.max(s, axis=-1, keepdims=True)) * factor)
                w = e * (1.0 / jnp.sum(e, axis=-1, keepdims=True))
                w_scr[slot, r : r + SOFT_ROWS, g * seq : (g + 1) * seq] = w.astype(jnp.bfloat16)
        out_refs[j][:, lanes] = jnp.dot(
            w_scr[slot], vals_scr[...], preferred_element_type=jnp.float32
        ).astype(jnp.bfloat16)


def attend(both, far):
    groups = len(both)
    rows = both[0].shape[0]
    seq = 2 * groups * rows
    return pl.pallas_call(
        functools.partial(attend_kernel, groups),
        grid=(2,),
        in_specs=in_vmem(2 * groups),
        out_specs=in_vmem(groups),
        out_shape=[jax.ShapeDtypeStruct((rows, 2 * TILE), jnp.bfloat16)] * groups,
        scratch_shapes=[
            pltpu.VMEM((GROUP * seq, TILE), jnp.bfloat16),
            pltpu.VMEM((GROUP * seq, TILE), jnp.bfloat16),
            pltpu.VMEM((2, rows, GROUP * seq), jnp.float32),
            pltpu.VMEM((2, rows, GROUP * seq), jnp.bfloat16),
        ],
        compiler_params=params(24),
        cost_estimate=pl.CostEstimate(
            flops=16 * groups * rows * seq * HD, bytes_accessed=12 * seq * TILE, transcendentals=0
        ),
        name="attend",
    )(*both, *far)


def project_kernel(groups, chunks, early, late, *refs):
    att_refs, refs = refs[: groups * chunks], refs[groups * chunks :]
    home = lax.axis_index("sp") % groups

    def product(w_ref):
        total = None
        for c in range(chunks):
            for j in range(groups):
                row = pl.ds(pl.multiple_of(((home ^ j) * chunks + c) * 2 * TILE, 2 * TILE), 2 * TILE)
                term = jnp.dot(att_refs[c * groups + j][...], w_ref[row, :], preferred_element_type=jnp.float32)
                total = term if total is None else total + term
        return total.astype(jnp.bfloat16)

    if late is None:
        for i, w_ref, out_ref in zip(early, refs[: len(early)], refs[len(early) :]):
            out_ref[...] = product(w_ref)
        return
    me = lax.axis_index("dp")
    w_refs, early_refs, out_ref = refs[: len(late)], refs[len(late) : -1], refs[-1]
    width = w_refs[0].shape[1]
    column = lambda i: pl.ds(pl.multiple_of((me ^ i) * width, width), width)
    for i, early_ref in zip(early, early_refs):
        out_ref[:, column(i)] = early_ref[...]
    for i, w_ref in zip(late, w_refs):
        out_ref[:, column(i)] = product(w_ref)


def project(attended, blocks, early, late=None, made=()):
    chunks, groups = len(attended), len(attended[0])
    tok = attended[0][0].shape[0]
    depth, width = blocks[0].shape
    flat = [piece for chunk in attended for piece in chunk]
    which = early if late is None else late
    if late is None:
        out_shape = [jax.ShapeDtypeStruct((tok, width), jnp.bfloat16)] * len(early)
        out_specs = in_vmem(len(early))
    else:
        out_shape = jax.ShapeDtypeStruct((tok, len(blocks) * width), jnp.bfloat16)
        out_specs = pl.BlockSpec(memory_space=pltpu.VMEM)
    return pl.pallas_call(
        functools.partial(project_kernel, groups, chunks, early, late),
        in_specs=in_vmem(len(flat) + len(which) + len(made)),
        out_specs=out_specs,
        out_shape=out_shape,
        compiler_params=params(16),
        cost_estimate=pl.CostEstimate(
            flops=2 * tok * depth * width * len(which), bytes_accessed=2 * depth * width * len(which),
            transcendentals=0,
        ),
        name="project",
    )(*flat, *[blocks[i] for i in which], *made)


def exchanged(block, axis, flip):
    count = lax.axis_size(axis)
    return lax.ppermute(block, axis, [(i, i ^ flip) for i in range(count)])


def group_form(queries, keys, values, q_gain, k_gain, w_out):
    sp_count, dp_count = lax.axis_size("sp"), lax.axis_size("dp")
    tok = queries.shape[2]
    groups = sp_count // 2
    chunks = KV // groups // 2
    bits = dp_count.bit_length() - 1
    top = 1 << (bits - 1)
    blocks = {0: w_out, top: exchanged(w_out, "dp", top)}
    early, late = [0], [top]
    for bit in reversed(range(bits - 1)):
        for listed in (early, late):
            for key in list(listed):
                blocks[key | 1 << bit] = exchanged(blocks[key], "dp", 1 << bit)
                listed.append(key | 1 << bit)
    cos_table, sin_table = rotary_lanes(lax.axis_index("sp") * tok, tok)
    both, kv = turn_and_pack(queries[0].T, keys[0].T, values[0].T, q_gain, k_gain, cos_table, sin_table, groups, chunks)
    near, far = [], []
    for c in range(chunks):
        near.append([both[c][0]] + [exchanged(both[c][j], "sp", j) for j in range(1, groups)])
        far.append([exchanged(kv[c][j], "sp", groups + j) for j in range(groups)])
    back = []
    for c in range(chunks):
        done = attend(near[c], far[c])
        back.append([done[0]] + [exchanged(done[j], "sp", j) for j in range(1, groups)])
    listed = [blocks[i] for i in range(dp_count)]
    made = project(back, listed, early)
    mixed = project(back, listed, early, late, made)
    return mixed[None]


def grouped(sp_count, dp_count):
    powers = sp_count & (sp_count - 1) == 0 and dp_count & (dp_count - 1) == 0
    return powers and sp_count > 2 and dp_count > 1 and KV % sp_count == 0


def on_device(*args):
    if grouped(lax.axis_size("sp"), lax.axis_size("dp")):
        return group_form(*args)
    return plain_form(*args)


def solution(mesh):
    placed = (
        P("dp", None, "sp"),
        P("dp", None, "sp"),
        P("dp", None, "sp"),
        P(),
        P(),
        P(None, "dp"),
    )
    return jax.shard_map(
        on_device, mesh=mesh, in_specs=placed, out_specs=P("dp", "sp", None), check_vma=False
    )
```

```python
import functools

import jax
import jax.numpy as jnp
from jax import lax
from jax.experimental import pallas as pl
from jax.experimental.pallas import tpu as pltpu
from jax.sharding import PartitionSpec as P


HD = 64
QH = 32
KV = 16
GRID_W = 64
GROUP = QH // KV

epsilon = 1e-06
rotary_base = 10000.0
block_count = 8


def swapped(block, axis, apart):
    count = lax.axis_size(axis)
    route = []
    for low in range(count):
        high = low | 1 << apart
        if high != low and high < count:
            route += [(low, high), (high, low)]
    return lax.ppermute(block, axis, route)


def rotary_tables(first_row, row_count):
    position = first_row + lax.iota(jnp.int32, row_count)
    grid_row = (position // GRID_W).astype(jnp.float32)
    grid_col = (position % GRID_W).astype(jnp.float32)
    quarter = HD // 4
    inv_freq = rotary_base ** (-(2.0 * lax.iota(jnp.float32, quarter)) / (HD // 2))
    row_angle = inv_freq[:, None] * grid_row[None, :]
    col_angle = inv_freq[:, None] * grid_col[None, :]
    cos_table = jnp.concatenate(
        [jnp.cos(row_angle), jnp.cos(row_angle), jnp.cos(col_angle), jnp.cos(col_angle)], axis=0
    )
    sin_table = jnp.concatenate(
        [jnp.sin(row_angle), jnp.sin(row_angle), jnp.sin(col_angle), jnp.sin(col_angle)], axis=0
    )
    return (cos_table, sin_table)


def normalize_turn(field, gain, cos_table, sin_table):
    head_count = field.shape[0] // HD
    values_f = field.astype(jnp.float32).reshape(head_count, HD, field.shape[1])
    normed = (
        values_f
        * lax.rsqrt(jnp.mean(values_f * values_f, axis=1, keepdims=True) + epsilon)
        * gain[None, :, None]
    )
    quarter = HD // 4
    quarters_of = normed.reshape(head_count, 4, quarter, field.shape[1])
    turned = jnp.concatenate(
        [-quarters_of[:, 1], quarters_of[:, 0], -quarters_of[:, 3], quarters_of[:, 2]], axis=1
    )
    return (normed * cos_table[None] + turned * sin_table[None]).astype(jnp.bfloat16)


def attention_heads(query_heads, key_heads, value_heads, seq_len):
    kv_local = key_heads.shape[0]
    group_local = query_heads.shape[0] // kv_local
    query_split = query_heads.reshape(kv_local, group_local, HD, seq_len)
    score_scale = HD ** (-0.5)
    block_rows = seq_len // block_count

    def one_block(block_index, result):
        row_start = block_index * block_rows
        query_block = lax.dynamic_slice_in_dim(query_split, row_start, block_rows, 3)
        scores = (
            jnp.einsum("hgdq,hdk->hgqk", query_block, key_heads, preferred_element_type=jnp.float32)
            * score_scale
        )
        row_max = jnp.max(scores, axis=-1, keepdims=True)
        weights = jnp.exp(scores - row_max)
        weights = (weights / jnp.sum(weights, axis=-1, keepdims=True)).astype(jnp.bfloat16)
        attended = jnp.einsum(
            "hgqk,hdk->hgdq", weights, value_heads, preferred_element_type=jnp.float32
        )
        return lax.dynamic_update_slice_in_dim(result, attended.astype(jnp.bfloat16), row_start, 3)

    result = jnp.zeros(query_split.shape, jnp.bfloat16)
    result = lax.fori_loop(0, block_count, one_block, result)
    return result.reshape(query_heads.shape)


def plain_form(queries, keys, values, q_gain, k_gain, w_out):
    sp_count = lax.axis_size("sp")
    tok_rows = queries.shape[2]
    seq_len = tok_rows * sp_count
    cos_table, sin_table = rotary_tables(lax.axis_index("sp") * tok_rows, tok_rows)
    query_rot = normalize_turn(queries[0], q_gain, cos_table, sin_table)
    key_rot = normalize_turn(keys[0], k_gain, cos_table, sin_table)
    value_rows = values[0].reshape(KV, HD, tok_rows)
    query_heads = lax.all_to_all(query_rot, "sp", split_axis=0, concat_axis=2, tiled=True)
    share_count = max(sp_count // KV, 1)
    part_rows = tok_rows // share_count
    key_cut = (
        key_rot.reshape(KV, HD, share_count, part_rows)
        .transpose(0, 2, 1, 3)
        .reshape(KV * share_count, HD, part_rows)
    )
    value_cut = (
        value_rows.reshape(KV, HD, share_count, part_rows)
        .transpose(0, 2, 1, 3)
        .reshape(KV * share_count, HD, part_rows)
    )
    key_got, value_got = (
        lax.all_to_all(key_cut, "sp", split_axis=0, concat_axis=2, tiled=True),
        lax.all_to_all(value_cut, "sp", split_axis=0, concat_axis=2, tiled=True),
    )
    kv_local = key_got.shape[0]
    key_got = key_got.reshape(kv_local, HD, sp_count, part_rows)
    value_got = value_got.reshape(kv_local, HD, sp_count, part_rows)
    for bit_index in range(share_count.bit_length() - 1):
        key_other, value_other = swapped((key_got, value_got), "sp", bit_index)
        key_got = jnp.concatenate([key_got, key_other], axis=3)
        value_got = jnp.concatenate([value_got, value_other], axis=3)
    key_heads = key_got.reshape(kv_local, HD, seq_len)
    value_heads = value_got.reshape(kv_local, HD, seq_len)
    attended = attention_heads(query_heads, key_heads, value_heads, seq_len)
    token_heads = lax.all_to_all(attended, "sp", split_axis=2, concat_axis=0, tiled=True)
    token_rows = token_heads.reshape(QH * HD, tok_rows)
    product = lax.dot_general(
        token_rows,
        lax.all_gather(w_out, "dp", axis=1, tiled=True),
        (((0,), (0,)), ((), ())),
        preferred_element_type=jnp.float32,
    )
    mixed_rows = product.astype(jnp.bfloat16)
    return mixed_rows[None]


TILE = 128


def rotary_lanes(first_row, row_count):
    position = first_row + lax.broadcasted_iota(jnp.int32, (row_count, TILE), 0)
    lane = lax.broadcasted_iota(jnp.int32, (row_count, TILE), 1) % HD
    quarter = HD // 4
    inv_freq = rotary_base ** (-(2.0 * (lane % quarter).astype(jnp.float32)) / (HD // 2))
    place = jnp.where(lane < HD // 2, position // GRID_W, position % GRID_W).astype(jnp.float32)
    angle = inv_freq * place
    sine = jnp.sin(angle)
    return jnp.cos(angle), jnp.where((lane // quarter) % 2 == 0, -sine, sine)


def turn_kernel(groups, chunks, *refs):
    sources, (cos_ref, sin_ref), out_refs = refs[:5], refs[5:7], refs[7:-6]
    held, sems = refs[-6:-1], refs[-1]
    copies = [pltpu.make_async_copy(src, dst, sems.at[i]) for i, (src, dst) in enumerate(zip(sources, held))]
    for copy in copies:
        copy.start()
    for copy in copies:
        copy.wait()
    q_ref, k_ref, v_ref, qg_ref, kg_ref = held
    home = lax.axis_index("sp") % groups
    cos_table, sin_table = cos_ref[...], sin_ref[...]
    q_gain = jnp.concatenate([qg_ref[...]] * 2, axis=1)
    k_gain = jnp.concatenate([kg_ref[...]] * 2, axis=1)
    quarter = HD // 4
    lane = lax.broadcasted_iota(jnp.int32, cos_table.shape, 1)
    even = (lane // quarter) % 2 == 0
    row_head = (lax.broadcasted_iota(jnp.int32, (2 * TILE, TILE), 0) % TILE) // HD
    col_head = lax.broadcasted_iota(jnp.int32, (2 * TILE, TILE), 1) // HD
    average = jnp.where(row_head == col_head, 1.0 / HD, 0.0).astype(jnp.bfloat16)

    def turned(tile, gain):
        field = tile.astype(jnp.float32)
        square = field * field
        coarse = square.astype(jnp.bfloat16)
        fine = (square - coarse.astype(jnp.float32)).astype(jnp.bfloat16)
        mean = jnp.dot(
            jnp.concatenate([coarse, fine], axis=1), average, preferred_element_type=jnp.float32
        )
        normed = field * lax.rsqrt(mean + epsilon) * gain
        partner = jnp.where(even, pltpu.roll(normed, TILE - quarter, 1), pltpu.roll(normed, quarter, 1))
        return (normed * cos_table + partner * sin_table).astype(jnp.bfloat16)

    both_refs, kv_refs = out_refs[: groups * chunks], out_refs[groups * chunks :]
    for c in range(chunks):
        for j in range(groups):
            place = (home ^ j) * chunks + c
            both, kv = both_refs[c * groups + j], kv_refs[c * groups + j]
            for p in range(2):
                lanes = pl.ds(pl.multiple_of((place * 2 + p) * TILE, TILE), TILE)
                both[:, p * TILE : (p + 1) * TILE] = turned(q_ref[:, lanes], q_gain)
            lanes = pl.ds(pl.multiple_of(place * TILE, TILE), TILE)
            key, value = turned(k_ref[:, lanes], k_gain), v_ref[:, lanes]
            both[:, 2 * TILE : 3 * TILE] = key
            both[:, 3 * TILE :] = value
            kv[:, :TILE] = key
            kv[:, TILE:] = value


def in_vmem(count):
    return [pl.BlockSpec(memory_space=pltpu.VMEM)] * count


def params(mib):
    return pltpu.CompilerParams(vmem_limit_bytes=mib << 20)


def turn_and_pack(queries, keys, values, q_gain, k_gain, cos_table, sin_table, groups, chunks):
    tok = queries.shape[0]
    made = groups * chunks
    out = pl.pallas_call(
        functools.partial(turn_kernel, groups, chunks),
        in_specs=[pl.BlockSpec(memory_space=pltpu.HBM)] * 5 + in_vmem(2),
        out_specs=in_vmem(2 * made),
        out_shape=[jax.ShapeDtypeStruct((tok, 4 * TILE), jnp.bfloat16)] * made
        + [jax.ShapeDtypeStruct((tok, 2 * TILE), jnp.bfloat16)] * made,
        scratch_shapes=[pltpu.VMEM(x.shape, x.dtype) for x in (queries, keys, values)]
        + [pltpu.VMEM((1, HD), jnp.float32)] * 2
        + [pltpu.SemaphoreType.DMA((5,))],
        compiler_params=params(60),
        cost_estimate=pl.CostEstimate(flops=40 * 3072 * tok, bytes_accessed=6 * 4096 * tok, transcendentals=0),
        name="turn",
    )(queries, keys, values, q_gain[None], k_gain[None], cos_table, sin_table)
    both = [out[c * groups : (c + 1) * groups] for c in range(chunks)]
    kv = [out[made + c * groups : made + (c + 1) * groups] for c in range(chunks)]
    return both, kv


def spread_kernel(groups, *refs):
    near_refs, far_refs, (keys_ref, vals_ref) = refs[:groups], refs[groups : 2 * groups], refs[2 * groups :]
    rows = near_refs[0].shape[0]
    seq = 2 * groups * rows
    low = lax.broadcasted_iota(jnp.int32, (rows, TILE), 1) < HD
    tiles = [(ref[:, 2 * TILE : 3 * TILE], ref[:, 3 * TILE :]) for ref in near_refs]
    tiles += [(ref[:, :TILE], ref[:, TILE:]) for ref in far_refs]
    for i, pair in enumerate(tiles):
        for tile, out_ref in zip(pair, (keys_ref, vals_ref)):
            tile = tile.astype(jnp.float32)
            other = pltpu.roll(tile, HD, 1)
            here = slice(i * rows, (i + 1) * rows)
            there = slice(seq + i * rows, seq + (i + 1) * rows)
            out_ref[0, here, :] = jnp.where(low, tile, 0.0).astype(jnp.bfloat16)
            out_ref[0, there, :] = jnp.where(low, 0.0, other).astype(jnp.bfloat16)
            out_ref[1, here, :] = jnp.where(low, other, 0.0).astype(jnp.bfloat16)
            out_ref[1, there, :] = jnp.where(low, 0.0, tile).astype(jnp.bfloat16)


def spread(near, far):
    groups, rows = len(near), near[0].shape[0]
    made = jax.ShapeDtypeStruct((2, GROUP * 2 * groups * rows, TILE), jnp.bfloat16)
    return pl.pallas_call(
        functools.partial(spread_kernel, groups),
        in_specs=in_vmem(2 * groups),
        out_specs=in_vmem(2),
        out_shape=[made] * 2,
        compiler_params=params(16),
        cost_estimate=pl.CostEstimate(flops=1 << 22, bytes_accessed=1 << 22, transcendentals=0),
        name="spread",
    )(*near, *far)


SOFT_ROWS = 8


def attend_kernel(count, *refs):
    query_refs, (keys_ref, vals_ref), out_refs = refs[:count], refs[count : count + 2], refs[count + 2 : -2]
    s_scr, w_scr = refs[-2:]
    rows = query_refs[0].shape[0]
    seq = keys_ref.shape[1] // GROUP
    factor = HD ** (-0.5) * 1.4426950408889634

    def scores(p):
        query = jnp.concatenate([ref[:, p * TILE : (p + 1) * TILE] for ref in query_refs], axis=0)
        s_scr[p] = lax.dot_general(
            query, keys_ref[p], (((1,), (1,)), ((), ())), preferred_element_type=jnp.float32
        )

    scores(0)
    for p in range(2):
        if p == 0:
            scores(1)
        for g in range(GROUP):
            for r in range(0, count * rows, SOFT_ROWS):
                s = s_scr[p, r : r + SOFT_ROWS, g * seq : (g + 1) * seq]
                e = jnp.exp2((s - jnp.max(s, axis=-1, keepdims=True)) * factor)
                w = e * (1.0 / jnp.sum(e, axis=-1, keepdims=True))
                w_scr[p, r : r + SOFT_ROWS, g * seq : (g + 1) * seq] = w.astype(jnp.bfloat16)
        attended = jnp.dot(w_scr[p], vals_ref[p], preferred_element_type=jnp.float32).astype(jnp.bfloat16)
        for i, out_ref in enumerate(out_refs):
            out_ref[:, p * TILE : (p + 1) * TILE] = attended[i * rows : (i + 1) * rows]


def attend(near, keys, vals):
    count, rows = len(near), near[0].shape[0]
    wide = keys.shape[1]
    return pl.pallas_call(
        functools.partial(attend_kernel, count),
        in_specs=in_vmem(count + 2),
        out_specs=in_vmem(count),
        out_shape=[jax.ShapeDtypeStruct((rows, 2 * TILE), jnp.bfloat16)] * count,
        scratch_shapes=[
            pltpu.VMEM((2, count * rows, wide), jnp.float32),
            pltpu.VMEM((2, count * rows, wide), jnp.bfloat16),
        ],
        compiler_params=params(24),
        cost_estimate=pl.CostEstimate(
            flops=8 * count * rows * wide * TILE, bytes_accessed=8 * wide * TILE, transcendentals=0
        ),
        name="attend",
    )(*near, keys, vals)


def project_kernel(groups, chunks, early, late, *refs):
    att_refs, refs = refs[: groups * chunks], refs[groups * chunks :]
    bufs, sems = refs[-2:]
    home = lax.axis_index("sp") % groups
    which = early if late is None else late
    w_refs = refs[: len(which)]
    deep = chunks * 2 * TILE
    row = lambda j: pl.ds(pl.multiple_of((home ^ j) * deep, deep), deep)
    copies = [
        [pltpu.make_async_copy(w_ref.at[row(j), :], bufs.at[i, j], sems.at[i, j]) for j in range(groups)]
        for i, w_ref in enumerate(w_refs)
    ]
    for copy in sum(copies, []):
        copy.start()
    parts = [jnp.concatenate([att_refs[c * groups + j][...] for c in range(chunks)], axis=1) for j in range(groups)]

    def product(i):
        total = None
        for j in range(groups):
            copies[i][j].wait()
            term = jnp.dot(parts[j], bufs[i, j], preferred_element_type=jnp.float32)
            total = term if total is None else total + term
        return total.astype(jnp.bfloat16)

    if late is None:
        for i, out_ref in enumerate(refs[len(which) : -2]):
            out_ref[...] = product(i)
        return
    me = lax.axis_index("dp")
    early_refs, out_ref = refs[len(which) : -3], refs[-3]
    width = w_refs[0].shape[1]
    column = lambda i: pl.ds(pl.multiple_of((me ^ i) * width, width), width)
    for i, early_ref in zip(early, early_refs):
        out_ref[:, column(i)] = early_ref[...]
    for n, i in enumerate(late):
        out_ref[:, column(i)] = product(n)


def project(attended, blocks, early, late=None, made=()):
    chunks, groups = len(attended), len(attended[0])
    tok = attended[0][0].shape[0]
    depth, width = blocks[0].shape
    flat = [piece for chunk in attended for piece in chunk]
    which = early if late is None else late
    if late is None:
        out_shape = [jax.ShapeDtypeStruct((tok, width), jnp.bfloat16)] * len(early)
        out_specs = in_vmem(len(early))
    else:
        out_shape = jax.ShapeDtypeStruct((tok, len(blocks) * width), jnp.bfloat16)
        out_specs = pl.BlockSpec(memory_space=pltpu.VMEM)
    return pl.pallas_call(
        functools.partial(project_kernel, groups, chunks, early, late),
        in_specs=in_vmem(len(flat)) + [pl.BlockSpec(memory_space=pl.ANY)] * len(which) + in_vmem(len(made)),
        out_specs=out_specs,
        out_shape=out_shape,
        scratch_shapes=[
            pltpu.VMEM((len(which), groups, depth // groups, width), jnp.bfloat16),
            pltpu.SemaphoreType.DMA((len(which), groups)),
        ],
        compiler_params=params(16),
        cost_estimate=pl.CostEstimate(
            flops=2 * tok * depth * width * len(which), bytes_accessed=2 * depth * width * len(which),
            transcendentals=0,
        ),
        name="project",
    )(*flat, *[blocks[i] for i in which], *made)


def exchanged(block, axis, flip):
    count = lax.axis_size(axis)
    return lax.ppermute(block, axis, [(i, i ^ flip) for i in range(count)])


def group_form(queries, keys, values, q_gain, k_gain, w_out):
    sp_count, dp_count = lax.axis_size("sp"), lax.axis_size("dp")
    tok = queries.shape[2]
    groups = sp_count // 2
    chunks = KV // groups // 2
    bits = dp_count.bit_length() - 1
    top = 1 << (bits - 1)
    blocks = {0: w_out, top: exchanged(w_out, "dp", top)}
    early, late = [0], [top]
    for bit in reversed(range(bits - 1)):
        for listed in (early, late):
            for key in list(listed):
                blocks[key | 1 << bit] = exchanged(blocks[key], "dp", 1 << bit)
                listed.append(key | 1 << bit)
    early, late = early + late[:1], late[1:]
    cos_table, sin_table = rotary_lanes(lax.axis_index("sp") * tok, tok)
    both, kv = turn_and_pack(queries[0].T, keys[0].T, values[0].T, q_gain, k_gain, cos_table, sin_table, groups, chunks)
    near, far = [], []
    for c in range(chunks):
        near.append([both[c][0]] + [exchanged(both[c][j], "sp", j) for j in range(1, groups)])
        far.append([exchanged(kv[c][j], "sp", groups + j) for j in range(groups)])
    back = []
    for c in range(chunks):
        ready = spread(near[c], far[c])
        got = [None] * groups
        for first in reversed(range(0, groups, 2)):
            done = attend(near[c][first : first + 2], *ready)
            for j in (first + 1, first):
                got[j] = exchanged(done[j - first], "sp", j) if j else done[0]
        back.append(got)
    listed = [blocks[i] for i in range(dp_count)]
    made = project(back, listed, early)
    mixed = project(back, listed, early, late, made)
    return mixed[None]


def grouped(sp_count, dp_count):
    powers = sp_count & (sp_count - 1) == 0 and dp_count & (dp_count - 1) == 0
    return powers and sp_count > 2 and dp_count > 1 and KV % sp_count == 0


def on_device(*args):
    if grouped(lax.axis_size("sp"), lax.axis_size("dp")):
        return group_form(*args)
    return plain_form(*args)


def solution(mesh):
    placed = (
        P("dp", None, "sp"),
        P("dp", None, "sp"),
        P("dp", None, "sp"),
        P(),
        P(),
        P(None, "dp"),
    )
    return jax.shard_map(
        on_device, mesh=mesh, in_specs=placed, out_specs=P("dp", "sp", None), check_vma=False
    )
```

```python
import functools

import jax
import jax.numpy as jnp
from jax import lax
from jax.experimental import pallas as pl
from jax.experimental.pallas import tpu as pltpu
from jax.sharding import PartitionSpec as P


HD = 64
QH = 32
KV = 16
GRID_W = 64
GROUP = QH // KV

epsilon = 1e-06
rotary_base = 10000.0
block_count = 8


def swapped(block, axis, apart):
    count = lax.axis_size(axis)
    route = []
    for low in range(count):
        high = low | 1 << apart
        if high != low and high < count:
            route += [(low, high), (high, low)]
    return lax.ppermute(block, axis, route)


def rotary_tables(first_row, row_count):
    position = first_row + lax.iota(jnp.int32, row_count)
    grid_row = (position // GRID_W).astype(jnp.float32)
    grid_col = (position % GRID_W).astype(jnp.float32)
    quarter = HD // 4
    inv_freq = rotary_base ** (-(2.0 * lax.iota(jnp.float32, quarter)) / (HD // 2))
    row_angle = inv_freq[:, None] * grid_row[None, :]
    col_angle = inv_freq[:, None] * grid_col[None, :]
    cos_table = jnp.concatenate(
        [jnp.cos(row_angle), jnp.cos(row_angle), jnp.cos(col_angle), jnp.cos(col_angle)], axis=0
    )
    sin_table = jnp.concatenate(
        [jnp.sin(row_angle), jnp.sin(row_angle), jnp.sin(col_angle), jnp.sin(col_angle)], axis=0
    )
    return (cos_table, sin_table)


def normalize_turn(field, gain, cos_table, sin_table):
    head_count = field.shape[0] // HD
    values_f = field.astype(jnp.float32).reshape(head_count, HD, field.shape[1])
    normed = (
        values_f
        * lax.rsqrt(jnp.mean(values_f * values_f, axis=1, keepdims=True) + epsilon)
        * gain[None, :, None]
    )
    quarter = HD // 4
    quarters_of = normed.reshape(head_count, 4, quarter, field.shape[1])
    turned = jnp.concatenate(
        [-quarters_of[:, 1], quarters_of[:, 0], -quarters_of[:, 3], quarters_of[:, 2]], axis=1
    )
    return (normed * cos_table[None] + turned * sin_table[None]).astype(jnp.bfloat16)


def attention_heads(query_heads, key_heads, value_heads, seq_len):
    kv_local = key_heads.shape[0]
    group_local = query_heads.shape[0] // kv_local
    query_split = query_heads.reshape(kv_local, group_local, HD, seq_len)
    score_scale = HD ** (-0.5)
    block_rows = seq_len // block_count

    def one_block(block_index, result):
        row_start = block_index * block_rows
        query_block = lax.dynamic_slice_in_dim(query_split, row_start, block_rows, 3)
        scores = (
            jnp.einsum("hgdq,hdk->hgqk", query_block, key_heads, preferred_element_type=jnp.float32)
            * score_scale
        )
        row_max = jnp.max(scores, axis=-1, keepdims=True)
        weights = jnp.exp(scores - row_max)
        weights = (weights / jnp.sum(weights, axis=-1, keepdims=True)).astype(jnp.bfloat16)
        attended = jnp.einsum(
            "hgqk,hdk->hgdq", weights, value_heads, preferred_element_type=jnp.float32
        )
        return lax.dynamic_update_slice_in_dim(result, attended.astype(jnp.bfloat16), row_start, 3)

    result = jnp.zeros(query_split.shape, jnp.bfloat16)
    result = lax.fori_loop(0, block_count, one_block, result)
    return result.reshape(query_heads.shape)


def plain_form(queries, keys, values, q_gain, k_gain, w_out):
    sp_count = lax.axis_size("sp")
    tok_rows = queries.shape[2]
    seq_len = tok_rows * sp_count
    cos_table, sin_table = rotary_tables(lax.axis_index("sp") * tok_rows, tok_rows)
    query_rot = normalize_turn(queries[0], q_gain, cos_table, sin_table)
    key_rot = normalize_turn(keys[0], k_gain, cos_table, sin_table)
    value_rows = values[0].reshape(KV, HD, tok_rows)
    query_heads = lax.all_to_all(query_rot, "sp", split_axis=0, concat_axis=2, tiled=True)
    share_count = max(sp_count // KV, 1)
    part_rows = tok_rows // share_count
    key_cut = (
        key_rot.reshape(KV, HD, share_count, part_rows)
        .transpose(0, 2, 1, 3)
        .reshape(KV * share_count, HD, part_rows)
    )
    value_cut = (
        value_rows.reshape(KV, HD, share_count, part_rows)
        .transpose(0, 2, 1, 3)
        .reshape(KV * share_count, HD, part_rows)
    )
    key_got, value_got = (
        lax.all_to_all(key_cut, "sp", split_axis=0, concat_axis=2, tiled=True),
        lax.all_to_all(value_cut, "sp", split_axis=0, concat_axis=2, tiled=True),
    )
    kv_local = key_got.shape[0]
    key_got = key_got.reshape(kv_local, HD, sp_count, part_rows)
    value_got = value_got.reshape(kv_local, HD, sp_count, part_rows)
    for bit_index in range(share_count.bit_length() - 1):
        key_other, value_other = swapped((key_got, value_got), "sp", bit_index)
        key_got = jnp.concatenate([key_got, key_other], axis=3)
        value_got = jnp.concatenate([value_got, value_other], axis=3)
    key_heads = key_got.reshape(kv_local, HD, seq_len)
    value_heads = value_got.reshape(kv_local, HD, seq_len)
    attended = attention_heads(query_heads, key_heads, value_heads, seq_len)
    token_heads = lax.all_to_all(attended, "sp", split_axis=2, concat_axis=0, tiled=True)
    token_rows = token_heads.reshape(QH * HD, tok_rows)
    product = lax.dot_general(
        token_rows,
        lax.all_gather(w_out, "dp", axis=1, tiled=True),
        (((0,), (0,)), ((), ())),
        preferred_element_type=jnp.float32,
    )
    mixed_rows = product.astype(jnp.bfloat16)
    return mixed_rows[None]


TILE = 128


def rotary_lanes(first_row, row_count):
    position = first_row + lax.broadcasted_iota(jnp.int32, (row_count, TILE), 0)
    lane = lax.broadcasted_iota(jnp.int32, (row_count, TILE), 1) % HD
    quarter = HD // 4
    inv_freq = rotary_base ** (-(2.0 * (lane % quarter).astype(jnp.float32)) / (HD // 2))
    place = jnp.where(lane < HD // 2, position // GRID_W, position % GRID_W).astype(jnp.float32)
    angle = inv_freq * place
    sine = jnp.sin(angle)
    return jnp.cos(angle), jnp.where((lane // quarter) % 2 == 0, -sine, sine)


def turn_kernel(groups, chunks, *refs):
    sources, (gain_ref, cos_ref, sin_ref), out_refs = refs[:3], refs[3:6], refs[6:-4]
    (q_ref, k_ref, v_ref), sems = refs[-4:-1], refs[-1]
    copies = [pltpu.make_async_copy(src, dst, sems.at[i]) for i, (src, dst) in enumerate(zip(sources, refs[-4:-1]))]
    for copy in copies:
        copy.start()
    quarter = HD // 4
    home = home_of(groups)
    row_head = (lax.broadcasted_iota(jnp.int32, (2 * TILE, TILE), 0) % TILE) // HD
    col_head = lax.broadcasted_iota(jnp.int32, (2 * TILE, TILE), 1) // HD
    average = jnp.where(row_head == col_head, 1.0 / HD, 0.0).astype(jnp.bfloat16)
    cos_table, sin_table = cos_ref[...], sin_ref[...]
    even = (lax.broadcasted_iota(jnp.int32, cos_table.shape, 1) // quarter) % 2 == 0
    q_gain, k_gain = gain_ref[0:1, :], gain_ref[1:2, :]
    for copy in copies:
        copy.wait()

    def turned(tile, gain):
        field = tile.astype(jnp.float32)
        square = field * field
        coarse = square.astype(jnp.bfloat16)
        fine = (square - coarse.astype(jnp.float32)).astype(jnp.bfloat16)
        mean = jnp.dot(
            jnp.concatenate([coarse, fine], axis=1), average, preferred_element_type=jnp.float32
        )
        normed = field * lax.rsqrt(mean + epsilon) * gain
        partner = jnp.where(even, pltpu.roll(normed, TILE - quarter, 1), pltpu.roll(normed, quarter, 1))
        return (normed * cos_table + partner * sin_table).astype(jnp.bfloat16)

    for c in range(chunks):
        for j in range(groups):
            place = (home ^ j) * chunks + c
            both, kv = out_refs[c * groups + j], out_refs[groups * chunks + c * groups + j]
            for p in range(2):
                lanes = pl.ds(pl.multiple_of((place * 2 + p) * TILE, TILE), TILE)
                both[:, p * TILE : (p + 1) * TILE] = turned(q_ref[:, lanes], q_gain)
            lanes = pl.ds(pl.multiple_of(place * TILE, TILE), TILE)
            key, value = turned(k_ref[:, lanes], k_gain), v_ref[:, lanes]
            both[:, 2 * TILE : 3 * TILE] = key
            both[:, 3 * TILE :] = value
            kv[:, :TILE] = key
            kv[:, TILE:] = value


def in_vmem(count):
    return [pl.BlockSpec(memory_space=pltpu.VMEM)] * count


def params(mib):
    return pltpu.CompilerParams(vmem_limit_bytes=mib << 20)


def turn_and_pack(queries, keys, values, q_gain, k_gain, cos_table, sin_table, groups, chunks):
    tok = queries.shape[0]
    made = groups * chunks
    shapes = [jax.ShapeDtypeStruct((tok, 4 * TILE), jnp.bfloat16)] * made
    shapes += [jax.ShapeDtypeStruct((tok, 2 * TILE), jnp.bfloat16)] * made
    gains = jnp.concatenate([q_gain, q_gain, k_gain, k_gain]).reshape(2, TILE)
    out = pl.pallas_call(
        functools.partial(turn_kernel, groups, chunks),
        in_specs=[pl.BlockSpec(memory_space=pltpu.HBM)] * 3 + in_vmem(3),
        out_specs=in_vmem(2 * made),
        out_shape=shapes,
        scratch_shapes=[pltpu.VMEM(x.shape, x.dtype) for x in (queries, keys, values)]
        + [pltpu.SemaphoreType.DMA((3,))],
        compiler_params=params(52),
        cost_estimate=pl.CostEstimate(flops=40 * 3072 * tok, bytes_accessed=6 * 4096 * tok, transcendentals=0),
        name="turn",
    )(queries, keys, values, gains, cos_table, sin_table)
    both = [out[c * groups : (c + 1) * groups] for c in range(chunks)]
    kv = [out[made + c * groups : made + (c + 1) * groups] for c in range(chunks)]
    return both, kv


def spread_kernel(groups, *refs):
    near_refs, far_refs, (keys_ref, vals_ref) = refs[:groups], refs[groups : 2 * groups], refs[2 * groups :]
    rows = near_refs[0].shape[0]
    seq = 2 * groups * rows
    low = lax.broadcasted_iota(jnp.int32, (rows, TILE), 1) < HD
    tiles = [(ref[:, 2 * TILE : 3 * TILE], ref[:, 3 * TILE :]) for ref in near_refs]
    tiles += [(ref[:, :TILE], ref[:, TILE:]) for ref in far_refs]
    for i, pair in enumerate(tiles):
        for tile, out_ref in zip(pair, (keys_ref, vals_ref)):
            tile = tile.astype(jnp.float32)
            other = pltpu.roll(tile, HD, 1)
            here = slice(i * rows, (i + 1) * rows)
            there = slice(seq + i * rows, seq + (i + 1) * rows)
            out_ref[0, here, :] = jnp.where(low, tile, 0.0).astype(jnp.bfloat16)
            out_ref[0, there, :] = jnp.where(low, 0.0, other).astype(jnp.bfloat16)
            out_ref[1, here, :] = jnp.where(low, other, 0.0).astype(jnp.bfloat16)
            out_ref[1, there, :] = jnp.where(low, 0.0, tile).astype(jnp.bfloat16)


def spread(near, far):
    groups, rows = len(near), near[0].shape[0]
    made = jax.ShapeDtypeStruct((2, GROUP * 2 * groups * rows, TILE), jnp.bfloat16)
    return pl.pallas_call(
        functools.partial(spread_kernel, groups),
        in_specs=in_vmem(2 * groups),
        out_specs=in_vmem(2),
        out_shape=[made] * 2,
        compiler_params=params(16),
        cost_estimate=pl.CostEstimate(flops=1 << 22, bytes_accessed=1 << 22, transcendentals=0),
        name="spread",
    )(*near, *far)


SOFT_ROWS = 8


def attend_kernel(count, *refs):
    query_refs, (keys_ref, vals_ref), out_refs = refs[:count], refs[count : count + 2], refs[count + 2 : -2]
    s_scr, w_scr = refs[-2:]
    rows = query_refs[0].shape[0]
    seq = keys_ref.shape[1] // GROUP
    factor = HD ** (-0.5) * 1.4426950408889634

    def scores(p):
        query = jnp.concatenate([ref[:, p * TILE : (p + 1) * TILE] for ref in query_refs], axis=0)
        s_scr[p] = lax.dot_general(
            query, keys_ref[p], (((1,), (1,)), ((), ())), preferred_element_type=jnp.float32
        )

    scores(0)
    for p in range(2):
        if p == 0:
            scores(1)
        for g in range(GROUP):
            for r in range(0, count * rows, SOFT_ROWS):
                s = s_scr[p, r : r + SOFT_ROWS, g * seq : (g + 1) * seq]
                e = jnp.exp2((s - jnp.max(s, axis=-1, keepdims=True)) * factor)
                w = e * (1.0 / jnp.sum(e, axis=-1, keepdims=True))
                w_scr[p, r : r + SOFT_ROWS, g * seq : (g + 1) * seq] = w.astype(jnp.bfloat16)
        attended = jnp.dot(w_scr[p], vals_ref[p], preferred_element_type=jnp.float32).astype(jnp.bfloat16)
        for i, out_ref in enumerate(out_refs):
            out_ref[:, p * TILE : (p + 1) * TILE] = attended[i * rows : (i + 1) * rows]


def attend(near, keys, vals):
    count, rows = len(near), near[0].shape[0]
    wide = keys.shape[1]
    return pl.pallas_call(
        functools.partial(attend_kernel, count),
        in_specs=in_vmem(count + 2),
        out_specs=in_vmem(count),
        out_shape=[jax.ShapeDtypeStruct((rows, 2 * TILE), jnp.bfloat16)] * count,
        scratch_shapes=[
            pltpu.VMEM((2, count * rows, wide), jnp.float32),
            pltpu.VMEM((2, count * rows, wide), jnp.bfloat16),
        ],
        compiler_params=params(32),
        cost_estimate=pl.CostEstimate(
            flops=8 * count * rows * wide * TILE, bytes_accessed=8 * wide * TILE, transcendentals=0
        ),
        name="attend",
    )(*near, keys, vals)


def home_of(groups):
    return lax.axis_index("sp") % groups


def loads(sources, held, sems, groups):
    copies = []
    for i, source in enumerate(sources):
        deep = source.shape[0] // groups
        rows = [pl.ds(pl.multiple_of((home_of(groups) ^ j) * deep, deep), deep) for j in range(groups)]
        copies.append(
            [pltpu.make_async_copy(source.at[rows[j], :], held[i].at[j], sems.at[i, j]) for j in range(groups)]
        )
    for row in copies:
        for copy in row:
            copy.start()
    return copies


def term(att_ref, held_ref, j, c):
    rows = slice(c * 2 * TILE, (c + 1) * 2 * TILE)
    return jnp.dot(att_ref[...], held_ref[j, rows, :], preferred_element_type=jnp.float32)


def first_kernel(groups, *refs):
    att_refs, sources, refs = refs[:groups], refs[groups : groups + 2], refs[groups + 2 :]
    held, sums, sems = refs[0:2], refs[2:4], refs[4]
    copies = loads(sources, held, sems, groups)
    for i in range(2):
        total = None
        for j in range(groups):
            copies[i][j].wait()
            part = term(att_refs[j], held[i], j, 0)
            total = part if total is None else total + part
        sums[i][...] = total


def second_kernel(groups, *refs):
    att_refs, own_ref, source, refs = refs[:groups], refs[groups], refs[groups + 1], refs[groups + 2 :]
    held_a, held_b, sum_a, sum_b = refs[0:4]
    held, sums, sems = refs[4], refs[5:8], refs[8]
    copies = loads([source], [held], sems, groups)
    sums[0][...] = sum_a[...] + term(own_ref, held_a, 0, 1)
    sums[1][...] = sum_b[...] + term(own_ref, held_b, 0, 1)
    total = None
    for j in range(groups):
        copies[0][j].wait()
        part = term(att_refs[j], held, j, 0)
        total = part if total is None else total + part
    sums[2][...] = total + term(own_ref, held, 0, 1)


def third_kernel(groups, *refs):
    first_refs, second_refs, refs = refs[:groups], refs[groups : 2 * groups], refs[2 * groups :]
    source, held, sums, out_ref = refs[0], refs[1:4], refs[4:7], refs[7]
    last, made, sems, out_sems = refs[8:]
    copies = loads([source], [last], sems, groups)
    me = lax.axis_index("dp")
    width = source.shape[1]

    def leave(i):
        column = pl.ds(pl.multiple_of((me ^ i) * width, width), width)
        copy = pltpu.make_async_copy(made.at[i], out_ref.at[:, column], out_sems.at[i])
        copy.start()
        return copy

    leaving = []
    for i in range(3):
        total = sums[i][...]
        for j in range(1, groups):
            total = total + term(second_refs[j], held[i], j, 1)
        made[i] = total.astype(jnp.bfloat16)
        leaving.append(leave(i))
    total = None
    for j in range(groups):
        copies[0][j].wait()
        part = term(first_refs[j], last, j, 0) + term(second_refs[j], last, j, 1)
        total = part if total is None else total + part
    made[3] = total.astype(jnp.bfloat16)
    leaving.append(leave(3))
    for copy in leaving:
        copy.wait()


def project_call(kernel, groups, inputs, spaces, out_shape, scratch, flops):
    many = isinstance(out_shape, list)
    return pl.pallas_call(
        functools.partial(kernel, groups),
        in_specs=[pl.BlockSpec(memory_space=space) for space in spaces],
        out_specs=in_vmem(len(out_shape)) if many else pl.BlockSpec(memory_space=pl.ANY),
        out_shape=out_shape,
        scratch_shapes=scratch,
        compiler_params=params(16),
        cost_estimate=pl.CostEstimate(flops=flops, bytes_accessed=1 << 22, transcendentals=0),
        name="project",
    )(*inputs)


def exchanged(block, axis, flip):
    count = lax.axis_size(axis)
    return lax.ppermute(block, axis, [(i, i ^ flip) for i in range(count)])


def group_form(queries, keys, values, q_gain, k_gain, w_out):
    sp_count = lax.axis_size("sp")
    tok = queries.shape[2]
    groups = sp_count // 2
    chunks = KV // groups // 2
    deep, width = w_out.shape[0] // groups, w_out.shape[1]
    across = exchanged(w_out, "dp", 2)
    beside = exchanged(w_out, "dp", 1)
    corner = exchanged(across, "dp", 1)
    cos_table, sin_table = rotary_lanes(lax.axis_index("sp") * tok, tok)
    both, kv = turn_and_pack(queries[0].T, keys[0].T, values[0].T, q_gain, k_gain, cos_table, sin_table, groups, chunks)
    near, far = [], []
    for c in range(chunks):
        near.append([both[c][0]] + [exchanged(both[c][j], "sp", j) for j in range(1, groups)])
        far.append([exchanged(kv[c][j], "sp", groups + j) for j in range(groups)])
    back = []
    for c in range(chunks):
        ready = spread(near[c], far[c])
        away = attend(near[c][1:], *ready)
        local = attend(near[c][:1], *ready)
        back.append(list(local) + [exchanged(away[j - 1], "sp", j) for j in range(1, groups)])

    vmem, hbm = pltpu.VMEM, pl.ANY
    held = jax.ShapeDtypeStruct((groups, deep, width), jnp.bfloat16)
    summed = jax.ShapeDtypeStruct((tok, width), jnp.float32)
    flops = 2 * tok * groups * deep * width
    held_a, held_b, sum_a, sum_b = project_call(
        first_kernel,
        groups,
        [*back[0], w_out, beside],
        [vmem] * groups + [hbm] * 2,
        [held] * 2 + [summed] * 2,
        [pltpu.SemaphoreType.DMA((2, groups))],
        flops,
    )
    held_c, *sums = project_call(
        second_kernel,
        groups,
        [*back[0], back[1][0], across, held_a, held_b, sum_a, sum_b],
        [vmem] * (groups + 1) + [hbm] + [vmem] * 4,
        [held] + [summed] * 3,
        [pltpu.SemaphoreType.DMA((1, groups))],
        flops,
    )
    mixed = project_call(
        third_kernel,
        groups,
        [*back[0], *back[1], corner, held_a, held_b, held_c, *sums],
        [vmem] * (2 * groups) + [hbm] + [vmem] * 6,
        jax.ShapeDtypeStruct((tok, 4 * width), jnp.bfloat16),
        [
            pltpu.VMEM(held.shape, held.dtype),
            pltpu.VMEM((4, tok, width), jnp.bfloat16),
            pltpu.SemaphoreType.DMA((1, groups)),
            pltpu.SemaphoreType.DMA((4,)),
        ],
        2 * flops,
    )
    return mixed[None]


def grouped(sp_count, dp_count):
    return dp_count == 4 and KV == 2 * sp_count and sp_count // 2 == 4


def on_device(*args):
    if grouped(lax.axis_size("sp"), lax.axis_size("dp")):
        return group_form(*args)
    return plain_form(*args)


def solution(mesh):
    placed = (
        P("dp", None, "sp"),
        P("dp", None, "sp"),
        P("dp", None, "sp"),
        P(),
        P(),
        P(None, "dp"),
    )
    return jax.shard_map(
        on_device, mesh=mesh, in_specs=placed, out_specs=P("dp", "sp", None), check_vma=False
    )
```

```python
import functools

import jax
import jax.numpy as jnp
from jax import lax
from jax.experimental import pallas as pl
from jax.experimental.pallas import tpu as pltpu
from jax.sharding import PartitionSpec as P


HD = 64
QH = 32
KV = 16
GRID_W = 64
GROUP = QH // KV

epsilon = 1e-06
rotary_base = 10000.0
block_count = 8


def swapped(block, axis, apart):
    count = lax.axis_size(axis)
    route = []
    for low in range(count):
        high = low | 1 << apart
        if high != low and high < count:
            route += [(low, high), (high, low)]
    return lax.ppermute(block, axis, route)


def rotary_tables(first_row, row_count):
    position = first_row + lax.iota(jnp.int32, row_count)
    grid_row = (position // GRID_W).astype(jnp.float32)
    grid_col = (position % GRID_W).astype(jnp.float32)
    quarter = HD // 4
    inv_freq = rotary_base ** (-(2.0 * lax.iota(jnp.float32, quarter)) / (HD // 2))
    row_angle = inv_freq[:, None] * grid_row[None, :]
    col_angle = inv_freq[:, None] * grid_col[None, :]
    cos_table = jnp.concatenate(
        [jnp.cos(row_angle), jnp.cos(row_angle), jnp.cos(col_angle), jnp.cos(col_angle)], axis=0
    )
    sin_table = jnp.concatenate(
        [jnp.sin(row_angle), jnp.sin(row_angle), jnp.sin(col_angle), jnp.sin(col_angle)], axis=0
    )
    return (cos_table, sin_table)


def normalize_turn(field, gain, cos_table, sin_table):
    head_count = field.shape[0] // HD
    values_f = field.astype(jnp.float32).reshape(head_count, HD, field.shape[1])
    normed = (
        values_f
        * lax.rsqrt(jnp.mean(values_f * values_f, axis=1, keepdims=True) + epsilon)
        * gain[None, :, None]
    )
    quarter = HD // 4
    quarters_of = normed.reshape(head_count, 4, quarter, field.shape[1])
    turned = jnp.concatenate(
        [-quarters_of[:, 1], quarters_of[:, 0], -quarters_of[:, 3], quarters_of[:, 2]], axis=1
    )
    return (normed * cos_table[None] + turned * sin_table[None]).astype(jnp.bfloat16)


def attention_heads(query_heads, key_heads, value_heads, seq_len):
    kv_local = key_heads.shape[0]
    group_local = query_heads.shape[0] // kv_local
    query_split = query_heads.reshape(kv_local, group_local, HD, seq_len)
    score_scale = HD ** (-0.5)
    block_rows = seq_len // block_count

    def one_block(block_index, result):
        row_start = block_index * block_rows
        query_block = lax.dynamic_slice_in_dim(query_split, row_start, block_rows, 3)
        scores = (
            jnp.einsum("hgdq,hdk->hgqk", query_block, key_heads, preferred_element_type=jnp.float32)
            * score_scale
        )
        row_max = jnp.max(scores, axis=-1, keepdims=True)
        weights = jnp.exp(scores - row_max)
        weights = (weights / jnp.sum(weights, axis=-1, keepdims=True)).astype(jnp.bfloat16)
        attended = jnp.einsum(
            "hgqk,hdk->hgdq", weights, value_heads, preferred_element_type=jnp.float32
        )
        return lax.dynamic_update_slice_in_dim(result, attended.astype(jnp.bfloat16), row_start, 3)

    result = jnp.zeros(query_split.shape, jnp.bfloat16)
    result = lax.fori_loop(0, block_count, one_block, result)
    return result.reshape(query_heads.shape)


def plain_form(queries, keys, values, q_gain, k_gain, w_out):
    sp_count = lax.axis_size("sp")
    tok_rows = queries.shape[2]
    seq_len = tok_rows * sp_count
    cos_table, sin_table = rotary_tables(lax.axis_index("sp") * tok_rows, tok_rows)
    query_rot = normalize_turn(queries[0], q_gain, cos_table, sin_table)
    key_rot = normalize_turn(keys[0], k_gain, cos_table, sin_table)
    value_rows = values[0].reshape(KV, HD, tok_rows)
    query_heads = lax.all_to_all(query_rot, "sp", split_axis=0, concat_axis=2, tiled=True)
    share_count = max(sp_count // KV, 1)
    part_rows = tok_rows // share_count
    key_cut = (
        key_rot.reshape(KV, HD, share_count, part_rows)
        .transpose(0, 2, 1, 3)
        .reshape(KV * share_count, HD, part_rows)
    )
    value_cut = (
        value_rows.reshape(KV, HD, share_count, part_rows)
        .transpose(0, 2, 1, 3)
        .reshape(KV * share_count, HD, part_rows)
    )
    key_got, value_got = (
        lax.all_to_all(key_cut, "sp", split_axis=0, concat_axis=2, tiled=True),
        lax.all_to_all(value_cut, "sp", split_axis=0, concat_axis=2, tiled=True),
    )
    kv_local = key_got.shape[0]
    key_got = key_got.reshape(kv_local, HD, sp_count, part_rows)
    value_got = value_got.reshape(kv_local, HD, sp_count, part_rows)
    for bit_index in range(share_count.bit_length() - 1):
        key_other, value_other = swapped((key_got, value_got), "sp", bit_index)
        key_got = jnp.concatenate([key_got, key_other], axis=3)
        value_got = jnp.concatenate([value_got, value_other], axis=3)
    key_heads = key_got.reshape(kv_local, HD, seq_len)
    value_heads = value_got.reshape(kv_local, HD, seq_len)
    attended = attention_heads(query_heads, key_heads, value_heads, seq_len)
    token_heads = lax.all_to_all(attended, "sp", split_axis=2, concat_axis=0, tiled=True)
    token_rows = token_heads.reshape(QH * HD, tok_rows)
    product = lax.dot_general(
        token_rows,
        lax.all_gather(w_out, "dp", axis=1, tiled=True),
        (((0,), (0,)), ((), ())),
        preferred_element_type=jnp.float32,
    )
    mixed_rows = product.astype(jnp.bfloat16)
    return mixed_rows[None]


TILE = 128


def rotary_lanes(first_row, row_count):
    position = first_row + lax.broadcasted_iota(jnp.int32, (row_count, TILE), 0)
    lane = lax.broadcasted_iota(jnp.int32, (row_count, TILE), 1) % HD
    quarter = HD // 4
    index = lax.broadcasted_iota(jnp.int32, (1, TILE), 1) % quarter
    inv_freq = jnp.zeros((1, TILE), jnp.float32)
    for i in range(quarter):
        inv_freq = jnp.where(index == i, rotary_base ** (-(2.0 * i) / (HD // 2)), inv_freq)
    place = jnp.where(lane < HD // 2, position // GRID_W, position % GRID_W).astype(jnp.float32)
    angle = inv_freq * place
    sine = jnp.sin(angle)
    return jnp.cos(angle), jnp.where((lane // quarter) % 2 == 0, -sine, sine)


def turn_kernel(groups, chunks, *refs):
    sources, gain_ref, out_refs, held, sems = refs[:3], refs[3], refs[4:-4], refs[-4:-1], refs[-1]
    q_ref, k_ref, v_ref = held
    copies = [pltpu.make_async_copy(src, dst, sems.at[i]) for i, (src, dst) in enumerate(zip(sources, held))]
    for copy in copies:
        copy.start()
    quarter = HD // 4
    home = home_of(groups)
    row_head = (lax.broadcasted_iota(jnp.int32, (2 * TILE, TILE), 0) % TILE) // HD
    col_head = lax.broadcasted_iota(jnp.int32, (2 * TILE, TILE), 1) // HD
    average = jnp.where(row_head == col_head, 1.0 / HD, 0.0).astype(jnp.bfloat16)
    tok = q_ref.shape[0]
    cos_table, sin_table = rotary_lanes(lax.axis_index("sp") * tok, tok)
    even = (lax.broadcasted_iota(jnp.int32, cos_table.shape, 1) // quarter) % 2 == 0
    for copy in copies:
        copy.wait()
    q_gain, k_gain = gain_ref[0:1, :], gain_ref[1:2, :]

    def turned(tile, gain):
        field = tile.astype(jnp.float32)
        square = field * field
        coarse = square.astype(jnp.bfloat16)
        fine = (square - coarse.astype(jnp.float32)).astype(jnp.bfloat16)
        mean = jnp.dot(
            jnp.concatenate([coarse, fine], axis=1), average, preferred_element_type=jnp.float32
        )
        normed = field * lax.rsqrt(mean + epsilon) * gain
        partner = jnp.where(even, pltpu.roll(normed, TILE - quarter, 1), pltpu.roll(normed, quarter, 1))
        return (normed * cos_table + partner * sin_table).astype(jnp.bfloat16)

    for c in range(chunks):
        for j in range(groups):
            place = (home ^ j) * chunks + c
            both, kv = out_refs[c * groups + j], out_refs[groups * chunks + c * groups + j]
            for p in range(2):
                lanes = pl.ds(pl.multiple_of((place * 2 + p) * TILE, TILE), TILE)
                both[:, p * TILE : (p + 1) * TILE] = turned(q_ref[:, lanes], q_gain)
            lanes = pl.ds(pl.multiple_of(place * TILE, TILE), TILE)
            key, value = turned(k_ref[:, lanes], k_gain), v_ref[:, lanes]
            both[:, 2 * TILE : 3 * TILE] = key
            both[:, 3 * TILE :] = value
            kv[:, :TILE] = key
            kv[:, TILE:] = value


def in_vmem(count):
    return [pl.BlockSpec(memory_space=pltpu.VMEM)] * count


def params(mib):
    return pltpu.CompilerParams(vmem_limit_bytes=mib << 20)


def turn_and_pack(queries, keys, values, q_gain, k_gain, groups, chunks):
    tok = queries.shape[0]
    made = groups * chunks
    shapes = [jax.ShapeDtypeStruct((tok, 4 * TILE), jnp.bfloat16)] * made
    shapes += [jax.ShapeDtypeStruct((tok, 2 * TILE), jnp.bfloat16)] * made
    out = pl.pallas_call(
        functools.partial(turn_kernel, groups, chunks),
        in_specs=[pl.BlockSpec(memory_space=pltpu.HBM)] * 3 + in_vmem(1),
        out_specs=in_vmem(2 * made),
        out_shape=shapes,
        scratch_shapes=[pltpu.VMEM(x.shape, x.dtype) for x in (queries, keys, values)]
        + [pltpu.SemaphoreType.DMA((3,))],
        compiler_params=params(52),
        cost_estimate=pl.CostEstimate(flops=40 * 3072 * tok, bytes_accessed=6 * 4096 * tok, transcendentals=0),
        name="turn",
    )(queries, keys, values, jnp.concatenate([q_gain, q_gain, k_gain, k_gain]).reshape(2, TILE))
    both = [out[c * groups : (c + 1) * groups] for c in range(chunks)]
    kv = [out[made + c * groups : made + (c + 1) * groups] for c in range(chunks)]
    return both, kv


def spread_kernel(groups, *refs):
    near_refs, far_refs, (keys_ref, vals_ref) = refs[:groups], refs[groups : 2 * groups], refs[2 * groups :]
    rows = near_refs[0].shape[0]
    seq = 2 * groups * rows
    low = lax.broadcasted_iota(jnp.int32, (rows, TILE), 1) < HD
    tiles = [(ref[:, 2 * TILE : 3 * TILE], ref[:, 3 * TILE :]) for ref in near_refs]
    tiles += [(ref[:, :TILE], ref[:, TILE:]) for ref in far_refs]
    for i, pair in enumerate(tiles):
        for tile, out_ref in zip(pair, (keys_ref, vals_ref)):
            tile = tile.astype(jnp.float32)
            other = pltpu.roll(tile, HD, 1)
            here = slice(i * rows, (i + 1) * rows)
            there = slice(seq + i * rows, seq + (i + 1) * rows)
            out_ref[0, here, :] = jnp.where(low, tile, 0.0).astype(jnp.bfloat16)
            out_ref[0, there, :] = jnp.where(low, 0.0, other).astype(jnp.bfloat16)
            out_ref[1, here, :] = jnp.where(low, other, 0.0).astype(jnp.bfloat16)
            out_ref[1, there, :] = jnp.where(low, 0.0, tile).astype(jnp.bfloat16)


def spread(near, far):
    groups, rows = len(near), near[0].shape[0]
    made = jax.ShapeDtypeStruct((2, GROUP * 2 * groups * rows, TILE), jnp.bfloat16)
    return pl.pallas_call(
        functools.partial(spread_kernel, groups),
        in_specs=in_vmem(2 * groups),
        out_specs=in_vmem(2),
        out_shape=[made] * 2,
        compiler_params=params(16),
        cost_estimate=pl.CostEstimate(flops=1 << 22, bytes_accessed=1 << 22, transcendentals=0),
        name="spread",
    )(*near, *far)


SOFT_ROWS = 8


def attend_kernel(count, *refs):
    query_refs, (keys_ref, vals_ref), out_refs = refs[:count], refs[count : count + 2], refs[count + 2 : -2]
    s_scr, w_scr = refs[-2:]
    rows = query_refs[0].shape[0]
    seq = keys_ref.shape[1] // GROUP
    factor = HD ** (-0.5) * 1.4426950408889634

    def scores(p):
        query = jnp.concatenate([ref[:, p * TILE : (p + 1) * TILE] for ref in query_refs], axis=0)
        s_scr[p] = lax.dot_general(
            query, keys_ref[p], (((1,), (1,)), ((), ())), preferred_element_type=jnp.float32
        )

    scores(0)
    for p in range(2):
        if p == 0:
            scores(1)
        for g in range(GROUP):
            for r in range(0, count * rows, SOFT_ROWS):
                s = s_scr[p, r : r + SOFT_ROWS, g * seq : (g + 1) * seq]
                e = jnp.exp2((s - jnp.max(s, axis=-1, keepdims=True)) * factor)
                w = e * (1.0 / jnp.sum(e, axis=-1, keepdims=True))
                w_scr[p, r : r + SOFT_ROWS, g * seq : (g + 1) * seq] = w.astype(jnp.bfloat16)
        attended = jnp.dot(w_scr[p], vals_ref[p], preferred_element_type=jnp.float32).astype(jnp.bfloat16)
        for i, out_ref in enumerate(out_refs):
            out_ref[:, p * TILE : (p + 1) * TILE] = attended[i * rows : (i + 1) * rows]


def attend(near, keys, vals):
    count, rows = len(near), near[0].shape[0]
    wide = keys.shape[1]
    return pl.pallas_call(
        functools.partial(attend_kernel, count),
        in_specs=in_vmem(count + 2),
        out_specs=in_vmem(count),
        out_shape=[jax.ShapeDtypeStruct((rows, 2 * TILE), jnp.bfloat16)] * count,
        scratch_shapes=[
            pltpu.VMEM((2, count * rows, wide), jnp.float32),
            pltpu.VMEM((2, count * rows, wide), jnp.bfloat16),
        ],
        compiler_params=params(32),
        cost_estimate=pl.CostEstimate(
            flops=8 * count * rows * wide * TILE, bytes_accessed=8 * wide * TILE, transcendentals=0
        ),
        name="attend",
    )(*near, keys, vals)


def home_of(groups):
    return lax.axis_index("sp") % groups


def loads(sources, held, sems, groups):
    copies = []
    for i, source in enumerate(sources):
        deep = source.shape[0] // groups
        rows = [pl.ds(pl.multiple_of((home_of(groups) ^ j) * deep, deep), deep) for j in range(groups)]
        copies.append(
            [pltpu.make_async_copy(source.at[rows[j], :], held[i].at[j], sems.at[i, j]) for j in range(groups)]
        )
    for row in copies:
        for copy in row:
            copy.start()
    return copies


def term(att_ref, held_ref, j, c):
    rows = slice(c * 2 * TILE, (c + 1) * 2 * TILE)
    return jnp.dot(att_ref[...], held_ref[j, rows, :], preferred_element_type=jnp.float32)


def load_kernel(groups, *refs):
    for row in loads(refs[0:2], refs[2:4], refs[4], groups):
        for copy in row:
            copy.wait()


def first_kernel(groups, *refs):
    att_refs, own_ref, source, refs = refs[:groups], refs[groups], refs[groups + 1], refs[groups + 2 :]
    held, last, sums, sems = refs[0:2], refs[2], refs[3:6], refs[6]
    copies = loads([source], [last], sems, groups)
    for i, held_ref in enumerate((*held, last)):
        total = None
        for j in range(groups):
            if i == 2:
                copies[0][j].wait()
            part = term(att_refs[j], held_ref, j, 0)
            total = part if total is None else total + part
        sums[i][...] = total + term(own_ref, held_ref, 0, 1)


def corner_rows(source, groups, j, c):
    deep = source.shape[0] // groups
    return pl.ds(pl.multiple_of((home_of(groups) ^ j) * deep + c * 2 * TILE, 2 * TILE), 2 * TILE)


def leave(total, i, width, made, out_ref, sem):
    made[...] = total.astype(jnp.bfloat16)
    column = pl.ds(pl.multiple_of((lax.axis_index("dp") ^ i) * width, width), width)
    copy = pltpu.make_async_copy(made, out_ref.at[:, column], sem)
    copy.start()
    return copy


def second_kernel(groups, *refs):
    att_refs, held, sums, (out_ref, made, sems) = refs[:-9], refs[-9:-6], refs[-6:-3], refs[-3:]
    leaving = []
    for i in range(3):
        total = sums[i][...]
        for j in range(1, groups):
            total = total + term(att_refs[j - 1], held[i], j, 1)
        leaving.append(leave(total, i, held[i].shape[2], made.at[i], out_ref, sems.at[i]))
    for copy in leaving:
        copy.wait()


def third_kernel(groups, *refs):
    parts, (source, _, out_ref, made, sem) = (refs[:groups], refs[groups : 2 * groups]), refs[2 * groups :]
    total = None
    for c in range(2):
        for j in range(groups):
            rows = corner_rows(source, groups, j, c)
            part = jnp.dot(parts[c][j][...], source[rows, :], preferred_element_type=jnp.float32)
            total = part if total is None else total + part
    leave(total, 3, source.shape[1], made, out_ref, sem).wait()


def project_call(kernel, groups, inputs, spaces, out_shape, scratch, flops, aliases={}):
    many = isinstance(out_shape, list)
    return pl.pallas_call(
        functools.partial(kernel, groups),
        in_specs=[pl.BlockSpec(memory_space=space) for space in spaces],
        out_specs=in_vmem(len(out_shape)) if many else pl.BlockSpec(memory_space=pl.ANY),
        out_shape=out_shape,
        scratch_shapes=scratch,
        input_output_aliases=aliases,
        compiler_params=params(16),
        cost_estimate=pl.CostEstimate(flops=flops, bytes_accessed=1 << 22, transcendentals=0),
        name="project",
    )(*inputs)


def exchanged(block, axis, flip):
    count = lax.axis_size(axis)
    return lax.ppermute(block, axis, [(i, i ^ flip) for i in range(count)])


def group_form(queries, keys, values, q_gain, k_gain, w_out):
    sp_count = lax.axis_size("sp")
    tok = queries.shape[2]
    groups = sp_count // 2
    chunks = KV // groups // 2
    deep, width = w_out.shape[0] // groups, w_out.shape[1]
    across = exchanged(w_out, "dp", 2)
    beside = exchanged(w_out, "dp", 1)
    corner = exchanged(across, "dp", 1)
    both, kv = turn_and_pack(queries[0].T, keys[0].T, values[0].T, q_gain, k_gain, groups, chunks)
    near, far = [], []
    for c in range(chunks):
        near.append([both[c][0]] + [exchanged(both[c][j], "sp", j) for j in range(1, groups)])
        far.append([exchanged(kv[c][j], "sp", groups + j) for j in range(groups)])
    back = []
    for c in range(chunks):
        ready = spread(near[c], far[c])
        away = attend(near[c][1:], *ready)
        local = attend(near[c][:1], *ready)
        back.append(list(local) + [exchanged(away[j - 1], "sp", j) for j in range(1, groups)])

    vmem, hbm = pltpu.VMEM, pl.ANY
    held = jax.ShapeDtypeStruct((groups, deep, width), jnp.bfloat16)
    summed = jax.ShapeDtypeStruct((tok, width), jnp.float32)
    flops = 2 * tok * groups * deep * width
    held_a, held_b = project_call(
        load_kernel, groups, [w_out, beside], [hbm] * 2, [held] * 2, [pltpu.SemaphoreType.DMA((2, groups))], flops
    )
    held_c, *sums = project_call(
        first_kernel,
        groups,
        [*back[0], back[1][0], across, held_a, held_b],
        [vmem] * (groups + 1) + [hbm] + [vmem] * 2,
        [held] + [summed] * 3,
        [pltpu.SemaphoreType.DMA((1, groups))],
        2 * flops,
    )
    whole = jax.ShapeDtypeStruct((tok, 4 * width), jnp.bfloat16)
    mixed = project_call(
        second_kernel,
        groups,
        [*back[1][1:], held_a, held_b, held_c, *sums],
        [vmem] * (groups + 5),
        whole,
        [pltpu.VMEM((3, tok, width), jnp.bfloat16), pltpu.SemaphoreType.DMA((3,))],
        flops,
    )
    mixed = project_call(
        third_kernel,
        groups,
        [*back[0], *back[1], corner, mixed],
        [vmem] * (2 * groups + 1) + [hbm],
        whole,
        [pltpu.VMEM((tok, width), jnp.bfloat16), pltpu.SemaphoreType.DMA(())],
        flops,
        {2 * groups + 1: 0},
    )
    return mixed[None]


def grouped(sp_count, dp_count):
    return dp_count == 4 and KV == 2 * sp_count and sp_count // 2 == 4


def on_device(*args):
    if grouped(lax.axis_size("sp"), lax.axis_size("dp")):
        return group_form(*args)
    return plain_form(*args)


def solution(mesh):
    placed = (
        P("dp", None, "sp"),
        P("dp", None, "sp"),
        P("dp", None, "sp"),
        P(),
        P(),
        P(None, "dp"),
    )
    return jax.shard_map(
        on_device, mesh=mesh, in_specs=placed, out_specs=P("dp", "sp", None), check_vma=False
    )
```

```python
import functools

import jax
import jax.numpy as jnp
from jax import lax
from jax.experimental import pallas as pl
from jax.experimental.pallas import tpu as pltpu
from jax.sharding import PartitionSpec as P


HD = 64
QH = 32
KV = 16
GRID_W = 64
GROUP = QH // KV

epsilon = 1e-06
rotary_base = 10000.0
block_count = 8


def swapped(block, axis, apart):
    count = lax.axis_size(axis)
    route = []
    for low in range(count):
        high = low | 1 << apart
        if high != low and high < count:
            route += [(low, high), (high, low)]
    return lax.ppermute(block, axis, route)


def rotary_tables(first_row, row_count):
    position = first_row + lax.iota(jnp.int32, row_count)
    grid_row = (position // GRID_W).astype(jnp.float32)
    grid_col = (position % GRID_W).astype(jnp.float32)
    quarter = HD // 4
    inv_freq = rotary_base ** (-(2.0 * lax.iota(jnp.float32, quarter)) / (HD // 2))
    row_angle = inv_freq[:, None] * grid_row[None, :]
    col_angle = inv_freq[:, None] * grid_col[None, :]
    cos_table = jnp.concatenate(
        [jnp.cos(row_angle), jnp.cos(row_angle), jnp.cos(col_angle), jnp.cos(col_angle)], axis=0
    )
    sin_table = jnp.concatenate(
        [jnp.sin(row_angle), jnp.sin(row_angle), jnp.sin(col_angle), jnp.sin(col_angle)], axis=0
    )
    return (cos_table, sin_table)


def normalize_turn(field, gain, cos_table, sin_table):
    head_count = field.shape[0] // HD
    values_f = field.astype(jnp.float32).reshape(head_count, HD, field.shape[1])
    normed = (
        values_f
        * lax.rsqrt(jnp.mean(values_f * values_f, axis=1, keepdims=True) + epsilon)
        * gain[None, :, None]
    )
    quarter = HD // 4
    quarters_of = normed.reshape(head_count, 4, quarter, field.shape[1])
    turned = jnp.concatenate(
        [-quarters_of[:, 1], quarters_of[:, 0], -quarters_of[:, 3], quarters_of[:, 2]], axis=1
    )
    return (normed * cos_table[None] + turned * sin_table[None]).astype(jnp.bfloat16)


def attention_heads(query_heads, key_heads, value_heads, seq_len):
    kv_local = key_heads.shape[0]
    group_local = query_heads.shape[0] // kv_local
    query_split = query_heads.reshape(kv_local, group_local, HD, seq_len)
    score_scale = HD ** (-0.5)
    block_rows = seq_len // block_count

    def one_block(block_index, result):
        row_start = block_index * block_rows
        query_block = lax.dynamic_slice_in_dim(query_split, row_start, block_rows, 3)
        scores = (
            jnp.einsum("hgdq,hdk->hgqk", query_block, key_heads, preferred_element_type=jnp.float32)
            * score_scale
        )
        row_max = jnp.max(scores, axis=-1, keepdims=True)
        weights = jnp.exp(scores - row_max)
        weights = (weights / jnp.sum(weights, axis=-1, keepdims=True)).astype(jnp.bfloat16)
        attended = jnp.einsum(
            "hgqk,hdk->hgdq", weights, value_heads, preferred_element_type=jnp.float32
        )
        return lax.dynamic_update_slice_in_dim(result, attended.astype(jnp.bfloat16), row_start, 3)

    result = jnp.zeros(query_split.shape, jnp.bfloat16)
    result = lax.fori_loop(0, block_count, one_block, result)
    return result.reshape(query_heads.shape)


def plain_form(queries, keys, values, q_gain, k_gain, w_out):
    sp_count = lax.axis_size("sp")
    tok_rows = queries.shape[2]
    seq_len = tok_rows * sp_count
    cos_table, sin_table = rotary_tables(lax.axis_index("sp") * tok_rows, tok_rows)
    query_rot = normalize_turn(queries[0], q_gain, cos_table, sin_table)
    key_rot = normalize_turn(keys[0], k_gain, cos_table, sin_table)
    value_rows = values[0].reshape(KV, HD, tok_rows)
    query_heads = lax.all_to_all(query_rot, "sp", split_axis=0, concat_axis=2, tiled=True)
    share_count = max(sp_count // KV, 1)
    part_rows = tok_rows // share_count
    key_cut = (
        key_rot.reshape(KV, HD, share_count, part_rows)
        .transpose(0, 2, 1, 3)
        .reshape(KV * share_count, HD, part_rows)
    )
    value_cut = (
        value_rows.reshape(KV, HD, share_count, part_rows)
        .transpose(0, 2, 1, 3)
        .reshape(KV * share_count, HD, part_rows)
    )
    key_got, value_got = (
        lax.all_to_all(key_cut, "sp", split_axis=0, concat_axis=2, tiled=True),
        lax.all_to_all(value_cut, "sp", split_axis=0, concat_axis=2, tiled=True),
    )
    kv_local = key_got.shape[0]
    key_got = key_got.reshape(kv_local, HD, sp_count, part_rows)
    value_got = value_got.reshape(kv_local, HD, sp_count, part_rows)
    for bit_index in range(share_count.bit_length() - 1):
        key_other, value_other = swapped((key_got, value_got), "sp", bit_index)
        key_got = jnp.concatenate([key_got, key_other], axis=3)
        value_got = jnp.concatenate([value_got, value_other], axis=3)
    key_heads = key_got.reshape(kv_local, HD, seq_len)
    value_heads = value_got.reshape(kv_local, HD, seq_len)
    attended = attention_heads(query_heads, key_heads, value_heads, seq_len)
    token_heads = lax.all_to_all(attended, "sp", split_axis=2, concat_axis=0, tiled=True)
    token_rows = token_heads.reshape(QH * HD, tok_rows)
    product = lax.dot_general(
        token_rows,
        lax.all_gather(w_out, "dp", axis=1, tiled=True),
        (((0,), (0,)), ((), ())),
        preferred_element_type=jnp.float32,
    )
    mixed_rows = product.astype(jnp.bfloat16)
    return mixed_rows[None]


TILE = 128


def rotary_lanes(first_row, row_count):
    position = first_row + lax.broadcasted_iota(jnp.int32, (row_count, TILE), 0)
    lane = lax.broadcasted_iota(jnp.int32, (row_count, TILE), 1) % HD
    quarter = HD // 4
    index = lax.broadcasted_iota(jnp.int32, (1, TILE), 1) % quarter
    inv_freq = jnp.zeros((1, TILE), jnp.float32)
    for i in range(quarter):
        inv_freq = jnp.where(index == i, rotary_base ** (-(2.0 * i) / (HD // 2)), inv_freq)
    place = jnp.where(lane < HD // 2, position // GRID_W, position % GRID_W).astype(jnp.float32)
    angle = inv_freq * place
    sine = jnp.sin(angle)
    return jnp.cos(angle), jnp.where((lane // quarter) % 2 == 0, -sine, sine)


def turn_kernel(groups, chunks, *refs):
    sources, gain_ref, out_refs, held, sems = refs[:3], refs[3], refs[4:-4], refs[-4:-1], refs[-1]
    q_ref, k_ref, v_ref = held
    copies = [pltpu.make_async_copy(src, dst, sems.at[i]) for i, (src, dst) in enumerate(zip(sources, held))]
    for copy in copies:
        copy.start()
    quarter = HD // 4
    home = home_of(groups)
    row_head = (lax.broadcasted_iota(jnp.int32, (2 * TILE, TILE), 0) % TILE) // HD
    col_head = lax.broadcasted_iota(jnp.int32, (2 * TILE, TILE), 1) // HD
    average = jnp.where(row_head == col_head, 1.0 / HD, 0.0).astype(jnp.bfloat16)
    tok = q_ref.shape[0]
    cos_table, sin_table = rotary_lanes(lax.axis_index("sp") * tok, tok)
    even = (lax.broadcasted_iota(jnp.int32, cos_table.shape, 1) // quarter) % 2 == 0
    for copy in copies:
        copy.wait()
    q_gain, k_gain = gain_ref[0:1, :], gain_ref[1:2, :]

    def turned(tile, gain):
        field = tile.astype(jnp.float32)
        square = field * field
        coarse = square.astype(jnp.bfloat16)
        fine = (square - coarse.astype(jnp.float32)).astype(jnp.bfloat16)
        mean = jnp.dot(
            jnp.concatenate([coarse, fine], axis=1), average, preferred_element_type=jnp.float32
        )
        normed = field * lax.rsqrt(mean + epsilon) * gain
        partner = jnp.where(even, pltpu.roll(normed, TILE - quarter, 1), pltpu.roll(normed, quarter, 1))
        return (normed * cos_table + partner * sin_table).astype(jnp.bfloat16)

    for c in range(chunks):
        for j in range(groups):
            place = (home ^ j) * chunks + c
            both, kv = out_refs[c * groups + j], out_refs[groups * chunks + c * groups + j]
            for p in range(2):
                lanes = pl.ds(pl.multiple_of((place * 2 + p) * TILE, TILE), TILE)
                both[:, p * TILE : (p + 1) * TILE] = turned(q_ref[:, lanes], q_gain)
            lanes = pl.ds(pl.multiple_of(place * TILE, TILE), TILE)
            key, value = turned(k_ref[:, lanes], k_gain), v_ref[:, lanes]
            both[:, 2 * TILE : 3 * TILE] = key
            both[:, 3 * TILE :] = value
            kv[:, :TILE] = key
            kv[:, TILE:] = value


def in_vmem(count):
    return [pl.BlockSpec(memory_space=pltpu.VMEM)] * count


def params(mib):
    return pltpu.CompilerParams(vmem_limit_bytes=mib << 20)


def turn_and_pack(queries, keys, values, q_gain, k_gain, groups, chunks):
    tok = queries.shape[0]
    made = groups * chunks
    shapes = [jax.ShapeDtypeStruct((tok, 4 * TILE), jnp.bfloat16)] * made
    shapes += [jax.ShapeDtypeStruct((tok, 2 * TILE), jnp.bfloat16)] * made
    out = pl.pallas_call(
        functools.partial(turn_kernel, groups, chunks),
        in_specs=[pl.BlockSpec(memory_space=pltpu.HBM)] * 3 + in_vmem(1),
        out_specs=in_vmem(2 * made),
        out_shape=shapes,
        scratch_shapes=[pltpu.VMEM(x.shape, x.dtype) for x in (queries, keys, values)]
        + [pltpu.SemaphoreType.DMA((3,))],
        compiler_params=params(52),
        cost_estimate=pl.CostEstimate(flops=40 * 3072 * tok, bytes_accessed=6 * 4096 * tok, transcendentals=0),
        name="turn",
    )(queries, keys, values, jnp.concatenate([q_gain, q_gain, k_gain, k_gain]).reshape(2, TILE))
    both = [out[c * groups : (c + 1) * groups] for c in range(chunks)]
    kv = [out[made + c * groups : made + (c + 1) * groups] for c in range(chunks)]
    return both, kv


def spread_kernel(groups, *refs):
    near_refs, far_refs, (keys_ref, vals_ref) = refs[:groups], refs[groups : 2 * groups], refs[2 * groups :]
    rows = near_refs[0].shape[0]
    seq = 2 * groups * rows
    low = lax.broadcasted_iota(jnp.int32, (rows, TILE), 1) < HD
    tiles = [(ref[:, 2 * TILE : 3 * TILE], ref[:, 3 * TILE :]) for ref in near_refs]
    tiles += [(ref[:, :TILE], ref[:, TILE:]) for ref in far_refs]
    for i, pair in enumerate(tiles):
        for tile, out_ref in zip(pair, (keys_ref, vals_ref)):
            tile = tile.astype(jnp.float32)
            other = pltpu.roll(tile, HD, 1)
            here = slice(i * rows, (i + 1) * rows)
            there = slice(seq + i * rows, seq + (i + 1) * rows)
            out_ref[0, here, :] = jnp.where(low, tile, 0.0).astype(jnp.bfloat16)
            out_ref[0, there, :] = jnp.where(low, 0.0, other).astype(jnp.bfloat16)
            out_ref[1, here, :] = jnp.where(low, other, 0.0).astype(jnp.bfloat16)
            out_ref[1, there, :] = jnp.where(low, 0.0, tile).astype(jnp.bfloat16)


def spread(near, far):
    groups, rows = len(near), near[0].shape[0]
    made = jax.ShapeDtypeStruct((2, GROUP * 2 * groups * rows, TILE), jnp.bfloat16)
    return pl.pallas_call(
        functools.partial(spread_kernel, groups),
        in_specs=in_vmem(2 * groups),
        out_specs=in_vmem(2),
        out_shape=[made] * 2,
        compiler_params=params(16),
        cost_estimate=pl.CostEstimate(flops=1 << 22, bytes_accessed=1 << 22, transcendentals=0),
        name="spread",
    )(*near, *far)


SOFT_ROWS = 8


def attend_kernel(count, *refs):
    query_refs, (keys_ref, vals_ref), out_refs = refs[:count], refs[count : count + 2], refs[count + 2 : -2]
    s_scr, w_scr = refs[-2:]
    rows = query_refs[0].shape[0]
    seq = keys_ref.shape[1] // GROUP
    factor = HD ** (-0.5) * 1.4426950408889634

    def scores(p):
        query = jnp.concatenate([ref[:, p * TILE : (p + 1) * TILE] for ref in query_refs], axis=0)
        s_scr[p] = lax.dot_general(
            query, keys_ref[p], (((1,), (1,)), ((), ())), preferred_element_type=jnp.float32
        )

    scores(0)
    for p in range(2):
        if p == 0:
            scores(1)
        for g in range(GROUP):
            for r in range(0, count * rows, SOFT_ROWS):
                s = s_scr[p, r : r + SOFT_ROWS, g * seq : (g + 1) * seq]
                e = jnp.exp2((s - jnp.max(s, axis=-1, keepdims=True)) * factor)
                w = e * (1.0 / jnp.sum(e, axis=-1, keepdims=True))
                w_scr[p, r : r + SOFT_ROWS, g * seq : (g + 1) * seq] = w.astype(jnp.bfloat16)
        attended = jnp.dot(w_scr[p], vals_ref[p], preferred_element_type=jnp.float32).astype(jnp.bfloat16)
        for i, out_ref in enumerate(out_refs):
            out_ref[:, p * TILE : (p + 1) * TILE] = attended[i * rows : (i + 1) * rows]


def attend(near, keys, vals):
    count, rows = len(near), near[0].shape[0]
    wide = keys.shape[1]
    return pl.pallas_call(
        functools.partial(attend_kernel, count),
        in_specs=in_vmem(count + 2),
        out_specs=in_vmem(count),
        out_shape=[jax.ShapeDtypeStruct((rows, 2 * TILE), jnp.bfloat16)] * count,
        scratch_shapes=[
            pltpu.VMEM((2, count * rows, wide), jnp.float32),
            pltpu.VMEM((2, count * rows, wide), jnp.bfloat16),
        ],
        compiler_params=params(32),
        cost_estimate=pl.CostEstimate(
            flops=8 * count * rows * wide * TILE, bytes_accessed=8 * wide * TILE, transcendentals=0
        ),
        name="attend",
    )(*near, keys, vals)


def home_of(groups):
    return lax.axis_index("sp") % groups


def term(att_ref, w_ref, groups, j, c):
    deep = w_ref.shape[0] // groups
    start = pl.multiple_of((home_of(groups) ^ j) * deep + c * 2 * TILE, 2 * TILE)
    return jnp.dot(att_ref[...], w_ref[pl.ds(start, 2 * TILE), :], preferred_element_type=jnp.float32)


def first_kernel(groups, *refs):
    att_refs, own_ref, w_refs, sums = refs[:groups], refs[groups], refs[groups + 1 : groups + 4], refs[groups + 4 :]
    for w_ref, sum_ref in zip(w_refs, sums):
        total = term(own_ref, w_ref, groups, 0, 1)
        for j in range(groups):
            total = total + term(att_refs[j], w_ref, groups, j, 0)
        sum_ref[...] = total


def second_kernel(groups, *refs):
    att_refs, w_refs, sums, made = refs[:-9], refs[-9:-6], refs[-6:-3], refs[-3:]
    for w_ref, sum_ref, made_ref in zip(w_refs, sums, made):
        total = sum_ref[...]
        for j in range(1, groups):
            total = total + term(att_refs[j - 1], w_ref, groups, j, 1)
        made_ref[...] = total.astype(jnp.bfloat16)


def third_kernel(groups, *refs):
    parts, refs = (refs[:groups], refs[groups : 2 * groups]), refs[2 * groups :]
    source, made, (out_ref, last, sems) = refs[0], refs[1:4], refs[4:]
    width = source.shape[1]

    def leave(i, ready):
        column = pl.ds(pl.multiple_of((lax.axis_index("dp") ^ i) * width, width), width)
        copy = pltpu.make_async_copy(ready, out_ref.at[:, column], sems.at[i])
        copy.start()
        return copy

    leaving = [leave(i, ready) for i, ready in enumerate(made)]
    total = None
    for c in range(2):
        for j in range(groups):
            part = term(parts[c][j], source, groups, j, c)
            total = part if total is None else total + part
    last[...] = total.astype(jnp.bfloat16)
    for copy in leaving + [leave(3, last)]:
        copy.wait()


def project_call(kernel, groups, inputs, out_shape, scratch, flops):
    many = isinstance(out_shape, list)
    return pl.pallas_call(
        functools.partial(kernel, groups),
        in_specs=in_vmem(len(inputs)),
        out_specs=in_vmem(len(out_shape)) if many else pl.BlockSpec(memory_space=pl.ANY),
        out_shape=out_shape,
        scratch_shapes=scratch,
        compiler_params=params(16),
        cost_estimate=pl.CostEstimate(flops=flops, bytes_accessed=1 << 22, transcendentals=0),
        name="project",
    )(*inputs)


def exchanged(block, axis, flip):
    count = lax.axis_size(axis)
    return lax.ppermute(block, axis, [(i, i ^ flip) for i in range(count)])


def group_form(queries, keys, values, q_gain, k_gain, w_out):
    sp_count = lax.axis_size("sp")
    tok = queries.shape[2]
    groups = sp_count // 2
    chunks = KV // groups // 2
    width = w_out.shape[1]
    across = exchanged(w_out, "dp", 2)
    beside = exchanged(w_out, "dp", 1)
    corner = exchanged(across, "dp", 1)
    both, kv = turn_and_pack(queries[0].T, keys[0].T, values[0].T, q_gain, k_gain, groups, chunks)
    near, far = [], []
    for c in range(chunks):
        near.append([both[c][0]] + [exchanged(both[c][j], "sp", j) for j in range(1, groups)])
        far.append([exchanged(kv[c][j], "sp", groups + j) for j in range(groups)])
    back = []
    for c in range(chunks):
        ready = spread(near[c], far[c])
        away = attend(near[c][1:], *ready)
        local = attend(near[c][:1], *ready)
        back.append(list(local) + [exchanged(away[j - 1], "sp", j) for j in range(1, groups)])

    near_blocks = [w_out, beside, across]
    block = lambda dtype: jax.ShapeDtypeStruct((tok, width), dtype)
    flops = 2 * tok * w_out.shape[0] * width
    sums = project_call(
        first_kernel, groups, [*back[0], back[1][0], *near_blocks], [block(jnp.float32)] * 3, [], 2 * flops
    )
    made = project_call(
        second_kernel, groups, [*back[1][1:], *near_blocks, *sums], [block(jnp.bfloat16)] * 3, [], flops
    )
    mixed = project_call(
        third_kernel,
        groups,
        [*back[0], *back[1], corner, *made],
        jax.ShapeDtypeStruct((tok, 4 * width), jnp.bfloat16),
        [pltpu.VMEM((tok, width), jnp.bfloat16), pltpu.SemaphoreType.DMA((4,))],
        flops,
    )
    return mixed[None]


def grouped(sp_count, dp_count):
    return dp_count == 4 and KV == 2 * sp_count and sp_count // 2 == 4


def on_device(*args):
    if grouped(lax.axis_size("sp"), lax.axis_size("dp")):
        return group_form(*args)
    return plain_form(*args)


def solution(mesh):
    placed = (
        P("dp", None, "sp"),
        P("dp", None, "sp"),
        P("dp", None, "sp"),
        P(),
        P(),
        P(None, "dp"),
    )
    return jax.shard_map(
        on_device, mesh=mesh, in_specs=placed, out_specs=P("dp", "sp", None), check_vma=False
    )
```

```python
import functools

import jax
import jax.numpy as jnp
from jax import lax
from jax.experimental import pallas as pl
from jax.experimental.pallas import tpu as pltpu
from jax.sharding import PartitionSpec as P


HD = 64
QH = 32
KV = 16
GRID_W = 64
GROUP = QH // KV

epsilon = 1e-06
rotary_base = 10000.0
block_count = 8


def swapped(block, axis, apart):
    count = lax.axis_size(axis)
    route = []
    for low in range(count):
        high = low | 1 << apart
        if high != low and high < count:
            route += [(low, high), (high, low)]
    return lax.ppermute(block, axis, route)


def rotary_tables(first_row, row_count):
    position = first_row + lax.iota(jnp.int32, row_count)
    grid_row = (position // GRID_W).astype(jnp.float32)
    grid_col = (position % GRID_W).astype(jnp.float32)
    quarter = HD // 4
    inv_freq = rotary_base ** (-(2.0 * lax.iota(jnp.float32, quarter)) / (HD // 2))
    row_angle = inv_freq[:, None] * grid_row[None, :]
    col_angle = inv_freq[:, None] * grid_col[None, :]
    cos_table = jnp.concatenate(
        [jnp.cos(row_angle), jnp.cos(row_angle), jnp.cos(col_angle), jnp.cos(col_angle)], axis=0
    )
    sin_table = jnp.concatenate(
        [jnp.sin(row_angle), jnp.sin(row_angle), jnp.sin(col_angle), jnp.sin(col_angle)], axis=0
    )
    return (cos_table, sin_table)


def normalize_turn(field, gain, cos_table, sin_table):
    head_count = field.shape[0] // HD
    values_f = field.astype(jnp.float32).reshape(head_count, HD, field.shape[1])
    normed = (
        values_f
        * lax.rsqrt(jnp.mean(values_f * values_f, axis=1, keepdims=True) + epsilon)
        * gain[None, :, None]
    )
    quarter = HD // 4
    quarters_of = normed.reshape(head_count, 4, quarter, field.shape[1])
    turned = jnp.concatenate(
        [-quarters_of[:, 1], quarters_of[:, 0], -quarters_of[:, 3], quarters_of[:, 2]], axis=1
    )
    return (normed * cos_table[None] + turned * sin_table[None]).astype(jnp.bfloat16)


def attention_heads(query_heads, key_heads, value_heads, seq_len):
    kv_local = key_heads.shape[0]
    group_local = query_heads.shape[0] // kv_local
    query_split = query_heads.reshape(kv_local, group_local, HD, seq_len)
    score_scale = HD ** (-0.5)
    block_rows = seq_len // block_count

    def one_block(block_index, result):
        row_start = block_index * block_rows
        query_block = lax.dynamic_slice_in_dim(query_split, row_start, block_rows, 3)
        scores = (
            jnp.einsum("hgdq,hdk->hgqk", query_block, key_heads, preferred_element_type=jnp.float32)
            * score_scale
        )
        row_max = jnp.max(scores, axis=-1, keepdims=True)
        weights = jnp.exp(scores - row_max)
        weights = (weights / jnp.sum(weights, axis=-1, keepdims=True)).astype(jnp.bfloat16)
        attended = jnp.einsum(
            "hgqk,hdk->hgdq", weights, value_heads, preferred_element_type=jnp.float32
        )
        return lax.dynamic_update_slice_in_dim(result, attended.astype(jnp.bfloat16), row_start, 3)

    result = jnp.zeros(query_split.shape, jnp.bfloat16)
    result = lax.fori_loop(0, block_count, one_block, result)
    return result.reshape(query_heads.shape)


def plain_form(queries, keys, values, q_gain, k_gain, w_out):
    sp_count = lax.axis_size("sp")
    tok_rows = queries.shape[2]
    seq_len = tok_rows * sp_count
    cos_table, sin_table = rotary_tables(lax.axis_index("sp") * tok_rows, tok_rows)
    query_rot = normalize_turn(queries[0], q_gain, cos_table, sin_table)
    key_rot = normalize_turn(keys[0], k_gain, cos_table, sin_table)
    value_rows = values[0].reshape(KV, HD, tok_rows)
    query_heads = lax.all_to_all(query_rot, "sp", split_axis=0, concat_axis=2, tiled=True)
    share_count = max(sp_count // KV, 1)
    part_rows = tok_rows // share_count
    key_cut = (
        key_rot.reshape(KV, HD, share_count, part_rows)
        .transpose(0, 2, 1, 3)
        .reshape(KV * share_count, HD, part_rows)
    )
    value_cut = (
        value_rows.reshape(KV, HD, share_count, part_rows)
        .transpose(0, 2, 1, 3)
        .reshape(KV * share_count, HD, part_rows)
    )
    key_got, value_got = (
        lax.all_to_all(key_cut, "sp", split_axis=0, concat_axis=2, tiled=True),
        lax.all_to_all(value_cut, "sp", split_axis=0, concat_axis=2, tiled=True),
    )
    kv_local = key_got.shape[0]
    key_got = key_got.reshape(kv_local, HD, sp_count, part_rows)
    value_got = value_got.reshape(kv_local, HD, sp_count, part_rows)
    for bit_index in range(share_count.bit_length() - 1):
        key_other, value_other = swapped((key_got, value_got), "sp", bit_index)
        key_got = jnp.concatenate([key_got, key_other], axis=3)
        value_got = jnp.concatenate([value_got, value_other], axis=3)
    key_heads = key_got.reshape(kv_local, HD, seq_len)
    value_heads = value_got.reshape(kv_local, HD, seq_len)
    attended = attention_heads(query_heads, key_heads, value_heads, seq_len)
    token_heads = lax.all_to_all(attended, "sp", split_axis=2, concat_axis=0, tiled=True)
    token_rows = token_heads.reshape(QH * HD, tok_rows)
    product = lax.dot_general(
        token_rows,
        lax.all_gather(w_out, "dp", axis=1, tiled=True),
        (((0,), (0,)), ((), ())),
        preferred_element_type=jnp.float32,
    )
    mixed_rows = product.astype(jnp.bfloat16)
    return mixed_rows[None]


TILE = 128


def rotary_lanes(first_row, row_count):
    position = first_row + lax.broadcasted_iota(jnp.int32, (row_count, TILE), 0)
    lane = lax.broadcasted_iota(jnp.int32, (row_count, TILE), 1) % HD
    quarter = HD // 4
    index = lax.broadcasted_iota(jnp.int32, (1, TILE), 1) % quarter
    inv_freq = jnp.zeros((1, TILE), jnp.float32)
    for i in range(quarter):
        inv_freq = jnp.where(index == i, rotary_base ** (-(2.0 * i) / (HD // 2)), inv_freq)
    place = jnp.where(lane < HD // 2, position // GRID_W, position % GRID_W).astype(jnp.float32)
    angle = inv_freq * place
    sine = jnp.sin(angle)
    return jnp.cos(angle), jnp.where((lane // quarter) % 2 == 0, -sine, sine)


def turn_kernel(groups, chunks, *refs):
    sources, gain_ref, out_refs, held, sems = refs[:3], refs[3], refs[4:-4], refs[-4:-1], refs[-1]
    q_ref, k_ref, v_ref = held
    copies = [pltpu.make_async_copy(src, dst, sems.at[i]) for i, (src, dst) in enumerate(zip(sources, held))]
    for copy in copies:
        copy.start()
    quarter = HD // 4
    home = home_of(groups)
    row_head = (lax.broadcasted_iota(jnp.int32, (2 * TILE, TILE), 0) % TILE) // HD
    col_head = lax.broadcasted_iota(jnp.int32, (2 * TILE, TILE), 1) // HD
    average = jnp.where(row_head == col_head, 1.0 / HD, 0.0).astype(jnp.bfloat16)
    tok = q_ref.shape[0]
    cos_table, sin_table = rotary_lanes(lax.axis_index("sp") * tok, tok)
    even = (lax.broadcasted_iota(jnp.int32, cos_table.shape, 1) // quarter) % 2 == 0
    for copy in copies:
        copy.wait()
    q_gain, k_gain = gain_ref[0:1, :], gain_ref[1:2, :]

    def turned(tile, gain):
        field = tile.astype(jnp.float32)
        square = field * field
        coarse = square.astype(jnp.bfloat16)
        fine = (square - coarse.astype(jnp.float32)).astype(jnp.bfloat16)
        mean = jnp.dot(
            jnp.concatenate([coarse, fine], axis=1), average, preferred_element_type=jnp.float32
        )
        normed = field * lax.rsqrt(mean + epsilon) * gain
        partner = jnp.where(even, pltpu.roll(normed, TILE - quarter, 1), pltpu.roll(normed, quarter, 1))
        return (normed * cos_table + partner * sin_table).astype(jnp.bfloat16)

    for c in range(chunks):
        for j in range(groups):
            place = (home ^ j) * chunks + c
            both, kv = out_refs[c * groups + j], out_refs[groups * chunks + c * groups + j]
            for p in range(2):
                lanes = pl.ds(pl.multiple_of((place * 2 + p) * TILE, TILE), TILE)
                both[:, p * TILE : (p + 1) * TILE] = turned(q_ref[:, lanes], q_gain)
            lanes = pl.ds(pl.multiple_of(place * TILE, TILE), TILE)
            key, value = turned(k_ref[:, lanes], k_gain), v_ref[:, lanes]
            both[:, 2 * TILE : 3 * TILE] = key
            both[:, 3 * TILE :] = value
            kv[:, :TILE] = key
            kv[:, TILE:] = value


def in_vmem(count):
    return [pl.BlockSpec(memory_space=pltpu.VMEM)] * count


def params(mib):
    return pltpu.CompilerParams(vmem_limit_bytes=mib << 20)


def turn_and_pack(queries, keys, values, q_gain, k_gain, groups, chunks):
    tok = queries.shape[0]
    made = groups * chunks
    shapes = [jax.ShapeDtypeStruct((tok, 4 * TILE), jnp.bfloat16)] * made
    shapes += [jax.ShapeDtypeStruct((tok, 2 * TILE), jnp.bfloat16)] * made
    out = pl.pallas_call(
        functools.partial(turn_kernel, groups, chunks),
        in_specs=[pl.BlockSpec(memory_space=pltpu.HBM)] * 3 + in_vmem(1),
        out_specs=in_vmem(2 * made),
        out_shape=shapes,
        scratch_shapes=[pltpu.VMEM(x.shape, x.dtype) for x in (queries, keys, values)]
        + [pltpu.SemaphoreType.DMA((3,))],
        compiler_params=params(52),
        cost_estimate=pl.CostEstimate(flops=40 * 3072 * tok, bytes_accessed=6 * 4096 * tok, transcendentals=0),
        name="turn",
    )(queries, keys, values, jnp.concatenate([q_gain, q_gain, k_gain, k_gain]).reshape(2, TILE))
    both = [out[c * groups : (c + 1) * groups] for c in range(chunks)]
    kv = [out[made + c * groups : made + (c + 1) * groups] for c in range(chunks)]
    return both, kv


def spread_tiles(tiles, out_ref):
    rows = tiles[0].shape[0]
    half = len(tiles) * rows
    low = lax.broadcasted_iota(jnp.int32, (rows, TILE), 1) < HD
    for i, tile in enumerate(tiles):
        tile = tile.astype(jnp.float32)
        other = pltpu.roll(tile, HD, 1)
        here = slice(i * rows, (i + 1) * rows)
        there = slice(half + i * rows, half + (i + 1) * rows)
        out_ref[0, here, :] = jnp.where(low, tile, 0.0).astype(jnp.bfloat16)
        out_ref[0, there, :] = jnp.where(low, 0.0, other).astype(jnp.bfloat16)
        out_ref[1, here, :] = jnp.where(low, other, 0.0).astype(jnp.bfloat16)
        out_ref[1, there, :] = jnp.where(low, 0.0, tile).astype(jnp.bfloat16)


def near_kernel(*refs):
    spread_tiles([ref[:, 2 * TILE : 3 * TILE] for ref in refs[:-1]], refs[-1])


def far_kernel(*refs):
    groups = len(refs[:-2]) // 2
    near_refs, far_refs, (keys_ref, vals_ref) = refs[:groups], refs[groups : 2 * groups], refs[-2:]
    spread_tiles([ref[:, :TILE] for ref in far_refs], keys_ref)
    spread_tiles([ref[:, 3 * TILE :] for ref in near_refs] + [ref[:, TILE:] for ref in far_refs], vals_ref)


def spread(kernel, sources, made):
    rows = GROUP * sources[0].shape[0]
    return pl.pallas_call(
        kernel,
        in_specs=in_vmem(len(sources)),
        out_specs=in_vmem(len(made)),
        out_shape=[jax.ShapeDtypeStruct((2, count * rows, TILE), jnp.bfloat16) for count in made],
        compiler_params=params(16),
        cost_estimate=pl.CostEstimate(flops=1 << 21, bytes_accessed=1 << 21, transcendentals=0),
        name="spread",
    )(*sources)


def score(query_refs, keys_ref, p):
    query = jnp.concatenate([ref[:, p * TILE : (p + 1) * TILE] for ref in query_refs], axis=0)
    return lax.dot_general(query, keys_ref[p], (((1,), (1,)), ((), ())), preferred_element_type=jnp.float32)


def score_kernel(*refs):
    for p in range(2):
        refs[-1][p] = score(refs[:-2], refs[-2], p)


def early_scores(near, keys):
    rows = len(near) * near[0].shape[0]
    return pl.pallas_call(
        score_kernel,
        in_specs=in_vmem(len(near) + 1),
        out_specs=pl.BlockSpec(memory_space=pltpu.VMEM),
        out_shape=jax.ShapeDtypeStruct((2, rows, keys.shape[1]), jnp.float32),
        compiler_params=params(16),
        cost_estimate=pl.CostEstimate(
            flops=4 * rows * keys.shape[1] * TILE, bytes_accessed=1 << 22, transcendentals=0
        ),
        name="score",
    )(*near, keys)


SOFT_ROWS = 8


def attend_kernel(count, given, *refs):
    query_refs, (near_keys, far_keys, vals), refs = refs[:count], refs[count : count + 3], refs[count + 3 :]
    out_refs, (near_s, far_s, w_scr) = refs[given : given + count], refs[given + count :]
    if given:
        near_s = refs[0]
    rows = query_refs[0].shape[0]
    half = near_keys.shape[1] // GROUP
    wide = near_keys.shape[1]
    factor = HD ** (-0.5) * 1.4426950408889634

    def scores(p):
        if not given:
            near_s[p] = score(query_refs, near_keys, p)
        far_s[p] = score(query_refs, far_keys, p)

    scores(0)
    for p in range(2):
        if p == 0:
            scores(1)
        for g in range(GROUP):
            lanes = slice(g * half, (g + 1) * half)
            for r in range(0, count * rows, SOFT_ROWS):
                s = jnp.concatenate([part[p, r : r + SOFT_ROWS, lanes] for part in (near_s, far_s)], axis=1)
                e = jnp.exp2((s - jnp.max(s, axis=-1, keepdims=True)) * factor)
                w = e * (1.0 / jnp.sum(e, axis=-1, keepdims=True))
                w_scr[p, r : r + SOFT_ROWS, g * wide : (g + 1) * wide] = w.astype(jnp.bfloat16)
        attended = jnp.dot(w_scr[p], vals[p], preferred_element_type=jnp.float32).astype(jnp.bfloat16)
        for i, out_ref in enumerate(out_refs):
            out_ref[:, p * TILE : (p + 1) * TILE] = attended[i * rows : (i + 1) * rows]


def attend(near, ready, early=None):
    count, rows = len(near), near[0].shape[0]
    wide = ready[0].shape[1]
    given = [] if early is None else [early]
    held = count * rows if early is None else SOFT_ROWS
    return pl.pallas_call(
        functools.partial(attend_kernel, count, len(given)),
        in_specs=in_vmem(count + 3 + len(given)),
        out_specs=in_vmem(count),
        out_shape=[jax.ShapeDtypeStruct((rows, 2 * TILE), jnp.bfloat16)] * count,
        scratch_shapes=[
            pltpu.VMEM((2, held, wide), jnp.float32),
            pltpu.VMEM((2, count * rows, wide), jnp.float32),
            pltpu.VMEM((2, count * rows, 2 * wide), jnp.bfloat16),
        ],
        compiler_params=params(32),
        cost_estimate=pl.CostEstimate(
            flops=16 * count * rows * wide * TILE, bytes_accessed=8 * wide * TILE, transcendentals=0
        ),
        name="attend",
    )(*near, *ready, *given)


def home_of(groups):
    return lax.axis_index("sp") % groups


def term(att_ref, w_ref, groups, j, c):
    deep = w_ref.shape[0] // groups
    start = pl.multiple_of((home_of(groups) ^ j) * deep + c * 2 * TILE, 2 * TILE)
    return jnp.dot(att_ref[...], w_ref[pl.ds(start, 2 * TILE), :], preferred_element_type=jnp.float32)


def first_kernel(groups, *refs):
    att_refs, own_ref, w_refs, sums = refs[:groups], refs[groups], refs[groups + 1 : groups + 4], refs[groups + 4 :]
    for w_ref, sum_ref in zip(w_refs, sums):
        total = term(own_ref, w_ref, groups, 0, 1)
        for j in range(groups):
            total = total + term(att_refs[j], w_ref, groups, j, 0)
        sum_ref[...] = total


def second_kernel(groups, *refs):
    att_refs, w_refs, sums, made = refs[:-9], refs[-9:-6], refs[-6:-3], refs[-3:]
    for w_ref, sum_ref, made_ref in zip(w_refs, sums, made):
        total = sum_ref[...]
        for j in range(1, groups):
            total = total + term(att_refs[j - 1], w_ref, groups, j, 1)
        made_ref[...] = total.astype(jnp.bfloat16)


def third_kernel(groups, *refs):
    parts, refs = (refs[:groups], refs[groups : 2 * groups]), refs[2 * groups :]
    source, made, (out_ref, last, sems) = refs[0], refs[1:4], refs[4:]
    width = source.shape[1]

    def leave(i, ready):
        column = pl.ds(pl.multiple_of((lax.axis_index("dp") ^ i) * width, width), width)
        copy = pltpu.make_async_copy(ready, out_ref.at[:, column], sems.at[i])
        copy.start()
        return copy

    leaving = [leave(i, ready) for i, ready in enumerate(made)]
    total = None
    for c in range(2):
        for j in range(groups):
            part = term(parts[c][j], source, groups, j, c)
            total = part if total is None else total + part
    last[...] = total.astype(jnp.bfloat16)
    for copy in leaving + [leave(3, last)]:
        copy.wait()


def project_call(kernel, groups, inputs, out_shape, scratch, flops):
    many = isinstance(out_shape, list)
    return pl.pallas_call(
        functools.partial(kernel, groups),
        in_specs=in_vmem(len(inputs)),
        out_specs=in_vmem(len(out_shape)) if many else pl.BlockSpec(memory_space=pl.ANY),
        out_shape=out_shape,
        scratch_shapes=scratch,
        compiler_params=params(16),
        cost_estimate=pl.CostEstimate(flops=flops, bytes_accessed=1 << 22, transcendentals=0),
        name="project",
    )(*inputs)


def exchanged(block, axis, flip):
    count = lax.axis_size(axis)
    return lax.ppermute(block, axis, [(i, i ^ flip) for i in range(count)])


def group_form(queries, keys, values, q_gain, k_gain, w_out):
    sp_count = lax.axis_size("sp")
    tok = queries.shape[2]
    groups = sp_count // 2
    chunks = KV // groups // 2
    width = w_out.shape[1]
    across = exchanged(w_out, "dp", 2)
    beside = exchanged(w_out, "dp", 1)
    corner = exchanged(across, "dp", 1)
    both, kv = turn_and_pack(queries[0].T, keys[0].T, values[0].T, q_gain, k_gain, groups, chunks)
    near, far = [], []
    for c in range(chunks):
        near.append([both[c][0]] + [exchanged(both[c][j], "sp", j) for j in range(1, groups)])
        far.append([exchanged(kv[c][j], "sp", groups + j) for j in range(groups)])
    back = []
    for c in range(chunks):
        early = None
        (near_keys,) = spread(near_kernel, near[c], [groups])
        if c:
            early = early_scores(near[c][1:], near_keys)
        ready = [near_keys, *spread(far_kernel, near[c] + far[c], [groups, 2 * groups])]
        away = attend(near[c][1:], ready, early)
        local = attend(near[c][:1], ready)
        back.append(list(local) + [exchanged(away[j - 1], "sp", j) for j in range(1, groups)])

    near_blocks = [w_out, beside, across]
    block = lambda dtype: jax.ShapeDtypeStruct((tok, width), dtype)
    flops = 2 * tok * w_out.shape[0] * width
    sums = project_call(
        first_kernel, groups, [*back[0], back[1][0], *near_blocks], [block(jnp.float32)] * 3, [], 2 * flops
    )
    made = project_call(
        second_kernel, groups, [*back[1][1:], *near_blocks, *sums], [block(jnp.bfloat16)] * 3, [], flops
    )
    mixed = project_call(
        third_kernel,
        groups,
        [*back[0], *back[1], corner, *made],
        jax.ShapeDtypeStruct((tok, 4 * width), jnp.bfloat16),
        [pltpu.VMEM((tok, width), jnp.bfloat16), pltpu.SemaphoreType.DMA((4,))],
        flops,
    )
    return mixed[None]


def grouped(sp_count, dp_count):
    return dp_count == 4 and KV == 2 * sp_count and sp_count // 2 == 4


def on_device(*args):
    if grouped(lax.axis_size("sp"), lax.axis_size("dp")):
        return group_form(*args)
    return plain_form(*args)


def solution(mesh):
    placed = (
        P("dp", None, "sp"),
        P("dp", None, "sp"),
        P("dp", None, "sp"),
        P(),
        P(),
        P(None, "dp"),
    )
    return jax.shard_map(
        on_device, mesh=mesh, in_specs=placed, out_specs=P("dp", "sp", None), check_vma=False
    )
```

```python
import functools

import jax
import jax.numpy as jnp
from jax import lax
from jax.experimental import pallas as pl
from jax.experimental.pallas import tpu as pltpu
from jax.sharding import PartitionSpec as P


HD = 64
QH = 32
KV = 16
GRID_W = 64
GROUP = QH // KV

epsilon = 1e-06
rotary_base = 10000.0
block_count = 8


def swapped(block, axis, apart):
    count = lax.axis_size(axis)
    route = []
    for low in range(count):
        high = low | 1 << apart
        if high != low and high < count:
            route += [(low, high), (high, low)]
    return lax.ppermute(block, axis, route)


def rotary_tables(first_row, row_count):
    position = first_row + lax.iota(jnp.int32, row_count)
    grid_row = (position // GRID_W).astype(jnp.float32)
    grid_col = (position % GRID_W).astype(jnp.float32)
    quarter = HD // 4
    inv_freq = rotary_base ** (-(2.0 * lax.iota(jnp.float32, quarter)) / (HD // 2))
    row_angle = inv_freq[:, None] * grid_row[None, :]
    col_angle = inv_freq[:, None] * grid_col[None, :]
    cos_table = jnp.concatenate(
        [jnp.cos(row_angle), jnp.cos(row_angle), jnp.cos(col_angle), jnp.cos(col_angle)], axis=0
    )
    sin_table = jnp.concatenate(
        [jnp.sin(row_angle), jnp.sin(row_angle), jnp.sin(col_angle), jnp.sin(col_angle)], axis=0
    )
    return (cos_table, sin_table)


def normalize_turn(field, gain, cos_table, sin_table):
    head_count = field.shape[0] // HD
    values_f = field.astype(jnp.float32).reshape(head_count, HD, field.shape[1])
    normed = (
        values_f
        * lax.rsqrt(jnp.mean(values_f * values_f, axis=1, keepdims=True) + epsilon)
        * gain[None, :, None]
    )
    quarter = HD // 4
    quarters_of = normed.reshape(head_count, 4, quarter, field.shape[1])
    turned = jnp.concatenate(
        [-quarters_of[:, 1], quarters_of[:, 0], -quarters_of[:, 3], quarters_of[:, 2]], axis=1
    )
    return (normed * cos_table[None] + turned * sin_table[None]).astype(jnp.bfloat16)


def attention_heads(query_heads, key_heads, value_heads, seq_len):
    kv_local = key_heads.shape[0]
    group_local = query_heads.shape[0] // kv_local
    query_split = query_heads.reshape(kv_local, group_local, HD, seq_len)
    score_scale = HD ** (-0.5)
    block_rows = seq_len // block_count

    def one_block(block_index, result):
        row_start = block_index * block_rows
        query_block = lax.dynamic_slice_in_dim(query_split, row_start, block_rows, 3)
        scores = (
            jnp.einsum("hgdq,hdk->hgqk", query_block, key_heads, preferred_element_type=jnp.float32)
            * score_scale
        )
        row_max = jnp.max(scores, axis=-1, keepdims=True)
        weights = jnp.exp(scores - row_max)
        weights = (weights / jnp.sum(weights, axis=-1, keepdims=True)).astype(jnp.bfloat16)
        attended = jnp.einsum(
            "hgqk,hdk->hgdq", weights, value_heads, preferred_element_type=jnp.float32
        )
        return lax.dynamic_update_slice_in_dim(result, attended.astype(jnp.bfloat16), row_start, 3)

    result = jnp.zeros(query_split.shape, jnp.bfloat16)
    result = lax.fori_loop(0, block_count, one_block, result)
    return result.reshape(query_heads.shape)


def plain_form(queries, keys, values, q_gain, k_gain, w_out):
    sp_count = lax.axis_size("sp")
    tok_rows = queries.shape[2]
    seq_len = tok_rows * sp_count
    cos_table, sin_table = rotary_tables(lax.axis_index("sp") * tok_rows, tok_rows)
    query_rot = normalize_turn(queries[0], q_gain, cos_table, sin_table)
    key_rot = normalize_turn(keys[0], k_gain, cos_table, sin_table)
    value_rows = values[0].reshape(KV, HD, tok_rows)
    query_heads = lax.all_to_all(query_rot, "sp", split_axis=0, concat_axis=2, tiled=True)
    share_count = max(sp_count // KV, 1)
    part_rows = tok_rows // share_count
    key_cut = (
        key_rot.reshape(KV, HD, share_count, part_rows)
        .transpose(0, 2, 1, 3)
        .reshape(KV * share_count, HD, part_rows)
    )
    value_cut = (
        value_rows.reshape(KV, HD, share_count, part_rows)
        .transpose(0, 2, 1, 3)
        .reshape(KV * share_count, HD, part_rows)
    )
    key_got, value_got = (
        lax.all_to_all(key_cut, "sp", split_axis=0, concat_axis=2, tiled=True),
        lax.all_to_all(value_cut, "sp", split_axis=0, concat_axis=2, tiled=True),
    )
    kv_local = key_got.shape[0]
    key_got = key_got.reshape(kv_local, HD, sp_count, part_rows)
    value_got = value_got.reshape(kv_local, HD, sp_count, part_rows)
    for bit_index in range(share_count.bit_length() - 1):
        key_other, value_other = swapped((key_got, value_got), "sp", bit_index)
        key_got = jnp.concatenate([key_got, key_other], axis=3)
        value_got = jnp.concatenate([value_got, value_other], axis=3)
    key_heads = key_got.reshape(kv_local, HD, seq_len)
    value_heads = value_got.reshape(kv_local, HD, seq_len)
    attended = attention_heads(query_heads, key_heads, value_heads, seq_len)
    token_heads = lax.all_to_all(attended, "sp", split_axis=2, concat_axis=0, tiled=True)
    token_rows = token_heads.reshape(QH * HD, tok_rows)
    product = lax.dot_general(
        token_rows,
        lax.all_gather(w_out, "dp", axis=1, tiled=True),
        (((0,), (0,)), ((), ())),
        preferred_element_type=jnp.float32,
    )
    mixed_rows = product.astype(jnp.bfloat16)
    return mixed_rows[None]


TILE = 128


def rotary_lanes(first_row, row_count):
    position = first_row + lax.broadcasted_iota(jnp.int32, (row_count, TILE), 0)
    lane = lax.broadcasted_iota(jnp.int32, (row_count, TILE), 1) % HD
    quarter = HD // 4
    index = lax.broadcasted_iota(jnp.int32, (1, TILE), 1) % quarter
    inv_freq = jnp.zeros((1, TILE), jnp.float32)
    for i in range(quarter):
        inv_freq = jnp.where(index == i, rotary_base ** (-(2.0 * i) / (HD // 2)), inv_freq)
    place = jnp.where(lane < HD // 2, position // GRID_W, position % GRID_W).astype(jnp.float32)
    angle = inv_freq * place
    sine = jnp.sin(angle)
    return jnp.cos(angle), jnp.where((lane // quarter) % 2 == 0, -sine, sine)


def turn_kernel(groups, chunks, *refs):
    sources, gain_ref, out_refs, held, sems = refs[:3], refs[3], refs[4:-4], refs[-4:-1], refs[-1]
    q_ref, k_ref, v_ref = held
    copies = [pltpu.make_async_copy(src, dst, sems.at[i]) for i, (src, dst) in enumerate(zip(sources, held))]
    for copy in copies:
        copy.start()
    quarter = HD // 4
    home = home_of(groups)
    row_head = (lax.broadcasted_iota(jnp.int32, (2 * TILE, TILE), 0) % TILE) // HD
    col_head = lax.broadcasted_iota(jnp.int32, (2 * TILE, TILE), 1) // HD
    average = jnp.where(row_head == col_head, 1.0 / HD, 0.0).astype(jnp.bfloat16)
    tok = q_ref.shape[0]
    cos_table, sin_table = rotary_lanes(lax.axis_index("sp") * tok, tok)
    even = (lax.broadcasted_iota(jnp.int32, cos_table.shape, 1) // quarter) % 2 == 0
    for copy in copies:
        copy.wait()
    q_gain, k_gain = gain_ref[0:1, :], gain_ref[1:2, :]

    def turned(tile, gain):
        field = tile.astype(jnp.float32)
        square = field * field
        coarse = square.astype(jnp.bfloat16)
        fine = (square - coarse.astype(jnp.float32)).astype(jnp.bfloat16)
        mean = jnp.dot(
            jnp.concatenate([coarse, fine], axis=1), average, preferred_element_type=jnp.float32
        )
        normed = field * lax.rsqrt(mean + epsilon) * gain
        partner = jnp.where(even, pltpu.roll(normed, TILE - quarter, 1), pltpu.roll(normed, quarter, 1))
        return (normed * cos_table + partner * sin_table).astype(jnp.bfloat16)

    for c in range(chunks):
        for j in range(groups):
            place = (home ^ j) * chunks + c
            both, kv = out_refs[c * groups + j], out_refs[groups * chunks + c * groups + j]
            for p in range(2):
                lanes = pl.ds(pl.multiple_of((place * 2 + p) * TILE, TILE), TILE)
                both[:, p * TILE : (p + 1) * TILE] = turned(q_ref[:, lanes], q_gain)
            lanes = pl.ds(pl.multiple_of(place * TILE, TILE), TILE)
            key, value = turned(k_ref[:, lanes], k_gain), v_ref[:, lanes]
            both[:, 2 * TILE : 3 * TILE] = key
            both[:, 3 * TILE :] = value
            kv[:, :TILE] = key
            kv[:, TILE:] = value


def in_vmem(count):
    return [pl.BlockSpec(memory_space=pltpu.VMEM)] * count


def params(mib):
    return pltpu.CompilerParams(vmem_limit_bytes=mib << 20)


def turn_and_pack(queries, keys, values, q_gain, k_gain, groups, chunks):
    tok = queries.shape[0]
    made = groups * chunks
    shapes = [jax.ShapeDtypeStruct((tok, 4 * TILE), jnp.bfloat16)] * made
    shapes += [jax.ShapeDtypeStruct((tok, 2 * TILE), jnp.bfloat16)] * made
    out = pl.pallas_call(
        functools.partial(turn_kernel, groups, chunks),
        in_specs=[pl.BlockSpec(memory_space=pltpu.HBM)] * 3 + in_vmem(1),
        out_specs=in_vmem(2 * made),
        out_shape=shapes,
        scratch_shapes=[pltpu.VMEM(x.shape, x.dtype) for x in (queries, keys, values)]
        + [pltpu.SemaphoreType.DMA((3,))],
        compiler_params=params(52),
        cost_estimate=pl.CostEstimate(flops=40 * 3072 * tok, bytes_accessed=6 * 4096 * tok, transcendentals=0),
        name="turn",
    )(queries, keys, values, jnp.concatenate([q_gain, q_gain, k_gain, k_gain]).reshape(2, TILE))
    both = [out[c * groups : (c + 1) * groups] for c in range(chunks)]
    kv = [out[made + c * groups : made + (c + 1) * groups] for c in range(chunks)]
    return both, kv


def spread_tiles(tiles, out_ref):
    rows = tiles[0].shape[0]
    half = len(tiles) * rows
    low = lax.broadcasted_iota(jnp.int32, (rows, TILE), 1) < HD
    for i, tile in enumerate(tiles):
        tile = tile.astype(jnp.float32)
        other = pltpu.roll(tile, HD, 1)
        here = slice(i * rows, (i + 1) * rows)
        there = slice(half + i * rows, half + (i + 1) * rows)
        out_ref[0, here, :] = jnp.where(low, tile, 0.0).astype(jnp.bfloat16)
        out_ref[0, there, :] = jnp.where(low, 0.0, other).astype(jnp.bfloat16)
        out_ref[1, here, :] = jnp.where(low, other, 0.0).astype(jnp.bfloat16)
        out_ref[1, there, :] = jnp.where(low, 0.0, tile).astype(jnp.bfloat16)


def near_kernel(*refs):
    spread_tiles([ref[:, 2 * TILE : 3 * TILE] for ref in refs[:-1]], refs[-1])


def far_kernel(*refs):
    groups = len(refs[:-2]) // 2
    near_refs, far_refs, (keys_ref, vals_ref) = refs[:groups], refs[groups : 2 * groups], refs[-2:]
    spread_tiles([ref[:, :TILE] for ref in far_refs], keys_ref)
    spread_tiles([ref[:, 3 * TILE :] for ref in near_refs] + [ref[:, TILE:] for ref in far_refs], vals_ref)


def spread(kernel, sources, made):
    rows = GROUP * sources[0].shape[0]
    return pl.pallas_call(
        kernel,
        in_specs=in_vmem(len(sources)),
        out_specs=in_vmem(len(made)),
        out_shape=[jax.ShapeDtypeStruct((2, count * rows, TILE), jnp.bfloat16) for count in made],
        compiler_params=params(16),
        cost_estimate=pl.CostEstimate(flops=1 << 21, bytes_accessed=1 << 21, transcendentals=0),
        name="spread",
    )(*sources)


def score(query_refs, keys_ref, p):
    query = jnp.concatenate([ref[:, p * TILE : (p + 1) * TILE] for ref in query_refs], axis=0)
    return lax.dot_general(query, keys_ref[p], (((1,), (1,)), ((), ())), preferred_element_type=jnp.float32)


def score_kernel(*refs):
    for p in range(2):
        refs[-1][p] = score(refs[:-2], refs[-2], p)


def early_scores(near, keys):
    rows = len(near) * near[0].shape[0]
    return pl.pallas_call(
        score_kernel,
        in_specs=in_vmem(len(near) + 1),
        out_specs=pl.BlockSpec(memory_space=pltpu.VMEM),
        out_shape=jax.ShapeDtypeStruct((2, rows, keys.shape[1]), jnp.float32),
        compiler_params=params(16),
        cost_estimate=pl.CostEstimate(
            flops=4 * rows * keys.shape[1] * TILE, bytes_accessed=1 << 22, transcendentals=0
        ),
        name="score",
    )(*near, keys)


SOFT_ROWS = 8


def attend_kernel(count, given, *refs):
    query_refs, (near_keys, far_keys, vals), refs = refs[:count], refs[count : count + 3], refs[count + 3 :]
    out_refs, (near_s, far_s, w_scr) = refs[given : given + count], refs[given + count :]
    if given:
        near_s = refs[0]
    rows = query_refs[0].shape[0]
    half = near_keys.shape[1] // GROUP
    wide = near_keys.shape[1]
    factor = HD ** (-0.5) * 1.4426950408889634

    def scores(p):
        if not given:
            near_s[p] = score(query_refs, near_keys, p)
        far_s[p] = score(query_refs, far_keys, p)

    scores(0)
    for p in range(2):
        if p == 0:
            scores(1)
        for g in range(GROUP):
            lanes = slice(g * half, (g + 1) * half)
            for r in range(0, count * rows, SOFT_ROWS):
                s = jnp.concatenate([part[p, r : r + SOFT_ROWS, lanes] for part in (near_s, far_s)], axis=1)
                e = jnp.exp2((s - jnp.max(s, axis=-1, keepdims=True)) * factor)
                w = e * (1.0 / jnp.sum(e, axis=-1, keepdims=True))
                w_scr[p, r : r + SOFT_ROWS, g * wide : (g + 1) * wide] = w.astype(jnp.bfloat16)
        attended = jnp.dot(w_scr[p], vals[p], preferred_element_type=jnp.float32).astype(jnp.bfloat16)
        for i, out_ref in enumerate(out_refs):
            out_ref[:, p * TILE : (p + 1) * TILE] = attended[i * rows : (i + 1) * rows]


def attend(near, ready, early=None):
    count, rows = len(near), near[0].shape[0]
    wide = ready[0].shape[1]
    given = [] if early is None else [early]
    held = count * rows if early is None else SOFT_ROWS
    return pl.pallas_call(
        functools.partial(attend_kernel, count, len(given)),
        in_specs=in_vmem(count + 3 + len(given)),
        out_specs=in_vmem(count),
        out_shape=[jax.ShapeDtypeStruct((rows, 2 * TILE), jnp.bfloat16)] * count,
        scratch_shapes=[
            pltpu.VMEM((2, held, wide), jnp.float32),
            pltpu.VMEM((2, count * rows, wide), jnp.float32),
            pltpu.VMEM((2, count * rows, 2 * wide), jnp.bfloat16),
        ],
        compiler_params=params(32),
        cost_estimate=pl.CostEstimate(
            flops=16 * count * rows * wide * TILE, bytes_accessed=8 * wide * TILE, transcendentals=0
        ),
        name="attend",
    )(*near, *ready, *given)


def home_of(groups):
    return lax.axis_index("sp") % groups


def term(att_ref, w_ref, groups, j, c):
    deep = w_ref.shape[0] // groups
    start = pl.multiple_of((home_of(groups) ^ j) * deep + c * 2 * TILE, 2 * TILE)
    return jnp.dot(att_ref[...], w_ref[pl.ds(start, 2 * TILE), :], preferred_element_type=jnp.float32)


def first_kernel(groups, *refs):
    att_refs, own_ref, w_refs, sums = refs[:groups], refs[groups], refs[groups + 1 : groups + 4], refs[groups + 4 :]
    for w_ref, sum_ref in zip(w_refs, sums):
        total = term(own_ref, w_ref, groups, 0, 1)
        for j in range(groups):
            total = total + term(att_refs[j], w_ref, groups, j, 0)
        sum_ref[...] = total


def second_kernel(groups, *refs):
    parts, refs = (refs[:groups], refs[groups : 2 * groups]), refs[2 * groups :]
    w_refs, sums, made, whole_ref = refs[0:3], refs[3:6], refs[6:9], refs[9]
    for w_ref, sum_ref, made_ref in zip(w_refs, sums, made):
        total = sum_ref[...]
        for j in range(1, groups):
            total = total + term(parts[1][j], w_ref, groups, j, 1)
        made_ref[...] = total.astype(jnp.bfloat16)
    for c in range(2):
        for j in range(groups):
            start = pl.multiple_of(((home_of(groups) ^ j) * 2 + c) * 2 * TILE, 2 * TILE)
            whole_ref[:, pl.ds(start, 2 * TILE)] = parts[c][j][...]


def third_kernel(groups, *refs):
    whole_ref, source, made, (out_ref, last, sems) = refs[0], refs[1], refs[2:5], refs[5:]
    width = source.shape[1]
    half = width // 2

    def leave(i, ready, shift, n):
        column = pl.ds(pl.multiple_of((lax.axis_index("dp") ^ i) * width + shift, half), ready.shape[1])
        copy = pltpu.make_async_copy(ready, out_ref.at[:, column], sems.at[n])
        copy.start()
        return copy

    leaving = [leave(i, ready, 0, i) for i, ready in enumerate(made)]
    for n in range(2):
        lanes = slice(n * half, (n + 1) * half)
        last[n] = jnp.dot(whole_ref[...], source[:, lanes], preferred_element_type=jnp.float32).astype(jnp.bfloat16)
        leaving.append(leave(3, last.at[n], n * half, 3 + n))
    for copy in leaving:
        copy.wait()


def project_call(kernel, groups, inputs, out_shape, scratch, flops):
    many = isinstance(out_shape, list)
    return pl.pallas_call(
        functools.partial(kernel, groups),
        in_specs=in_vmem(len(inputs)),
        out_specs=in_vmem(len(out_shape)) if many else pl.BlockSpec(memory_space=pl.ANY),
        out_shape=out_shape,
        scratch_shapes=scratch,
        compiler_params=params(16),
        cost_estimate=pl.CostEstimate(flops=flops, bytes_accessed=1 << 22, transcendentals=0),
        name="project",
    )(*inputs)


def exchanged(block, axis, flip):
    count = lax.axis_size(axis)
    return lax.ppermute(block, axis, [(i, i ^ flip) for i in range(count)])


def group_form(queries, keys, values, q_gain, k_gain, w_out):
    sp_count = lax.axis_size("sp")
    tok = queries.shape[2]
    groups = sp_count // 2
    chunks = KV // groups // 2
    width = w_out.shape[1]
    across = exchanged(w_out, "dp", 2)
    beside = exchanged(w_out, "dp", 1)
    corner = exchanged(across, "dp", 1)
    both, kv = turn_and_pack(queries[0].T, keys[0].T, values[0].T, q_gain, k_gain, groups, chunks)
    near, far = [], []
    for c in range(chunks):
        near.append([both[c][0]] + [exchanged(both[c][j], "sp", j) for j in range(1, groups)])
        far.append([exchanged(kv[c][j], "sp", groups + j) for j in range(groups)])
    back = []
    for c in range(chunks):
        early = None
        (near_keys,) = spread(near_kernel, near[c], [groups])
        if c:
            early = early_scores(near[c][1:], near_keys)
        ready = [near_keys, *spread(far_kernel, near[c] + far[c], [groups, 2 * groups])]
        away = attend(near[c][1:], ready, early)
        local = attend(near[c][:1], ready)
        back.append(list(local) + [exchanged(away[j - 1], "sp", j) for j in range(1, groups)])

    near_blocks = [w_out, beside, across]
    block = lambda dtype: jax.ShapeDtypeStruct((tok, width), dtype)
    flops = 2 * tok * w_out.shape[0] * width
    sums = project_call(
        first_kernel, groups, [*back[0], back[1][0], *near_blocks], [block(jnp.float32)] * 3, [], 2 * flops
    )
    *made, whole = project_call(
        second_kernel,
        groups,
        [*back[0], *back[1], *near_blocks, *sums],
        [block(jnp.bfloat16)] * 3 + [jax.ShapeDtypeStruct((tok, w_out.shape[0]), jnp.bfloat16)],
        [],
        flops,
    )
    mixed = project_call(
        third_kernel,
        groups,
        [whole, corner, *made],
        jax.ShapeDtypeStruct((tok, 4 * width), jnp.bfloat16),
        [pltpu.VMEM((2, tok, width // 2), jnp.bfloat16), pltpu.SemaphoreType.DMA((5,))],
        flops,
    )
    return mixed[None]


def grouped(sp_count, dp_count):
    return dp_count == 4 and KV == 2 * sp_count and sp_count // 2 == 4


def on_device(*args):
    if grouped(lax.axis_size("sp"), lax.axis_size("dp")):
        return group_form(*args)
    return plain_form(*args)


def solution(mesh):
    placed = (
        P("dp", None, "sp"),
        P("dp", None, "sp"),
        P("dp", None, "sp"),
        P(),
        P(),
        P(None, "dp"),
    )
    return jax.shard_map(
        on_device, mesh=mesh, in_specs=placed, out_specs=P("dp", "sp", None), check_vma=False
    )
```

```python
import functools

import jax
import jax.numpy as jnp
from jax import lax
from jax.experimental import pallas as pl
from jax.experimental.pallas import tpu as pltpu
from jax.sharding import PartitionSpec as P


HD = 64
QH = 32
KV = 16
GRID_W = 64
GROUP = QH // KV

epsilon = 1e-06
rotary_base = 10000.0
block_count = 8


def swapped(block, axis, apart):
    count = lax.axis_size(axis)
    route = []
    for low in range(count):
        high = low | 1 << apart
        if high != low and high < count:
            route += [(low, high), (high, low)]
    return lax.ppermute(block, axis, route)


def rotary_tables(first_row, row_count):
    position = first_row + lax.iota(jnp.int32, row_count)
    grid_row = (position // GRID_W).astype(jnp.float32)
    grid_col = (position % GRID_W).astype(jnp.float32)
    quarter = HD // 4
    inv_freq = rotary_base ** (-(2.0 * lax.iota(jnp.float32, quarter)) / (HD // 2))
    row_angle = inv_freq[:, None] * grid_row[None, :]
    col_angle = inv_freq[:, None] * grid_col[None, :]
    cos_table = jnp.concatenate(
        [jnp.cos(row_angle), jnp.cos(row_angle), jnp.cos(col_angle), jnp.cos(col_angle)], axis=0
    )
    sin_table = jnp.concatenate(
        [jnp.sin(row_angle), jnp.sin(row_angle), jnp.sin(col_angle), jnp.sin(col_angle)], axis=0
    )
    return (cos_table, sin_table)


def normalize_turn(field, gain, cos_table, sin_table):
    head_count = field.shape[0] // HD
    values_f = field.astype(jnp.float32).reshape(head_count, HD, field.shape[1])
    normed = (
        values_f
        * lax.rsqrt(jnp.mean(values_f * values_f, axis=1, keepdims=True) + epsilon)
        * gain[None, :, None]
    )
    quarter = HD // 4
    quarters_of = normed.reshape(head_count, 4, quarter, field.shape[1])
    turned = jnp.concatenate(
        [-quarters_of[:, 1], quarters_of[:, 0], -quarters_of[:, 3], quarters_of[:, 2]], axis=1
    )
    return (normed * cos_table[None] + turned * sin_table[None]).astype(jnp.bfloat16)


def attention_heads(query_heads, key_heads, value_heads, seq_len):
    kv_local = key_heads.shape[0]
    group_local = query_heads.shape[0] // kv_local
    query_split = query_heads.reshape(kv_local, group_local, HD, seq_len)
    score_scale = HD ** (-0.5)
    block_rows = seq_len // block_count

    def one_block(block_index, result):
        row_start = block_index * block_rows
        query_block = lax.dynamic_slice_in_dim(query_split, row_start, block_rows, 3)
        scores = (
            jnp.einsum("hgdq,hdk->hgqk", query_block, key_heads, preferred_element_type=jnp.float32)
            * score_scale
        )
        row_max = jnp.max(scores, axis=-1, keepdims=True)
        weights = jnp.exp(scores - row_max)
        weights = (weights / jnp.sum(weights, axis=-1, keepdims=True)).astype(jnp.bfloat16)
        attended = jnp.einsum(
            "hgqk,hdk->hgdq", weights, value_heads, preferred_element_type=jnp.float32
        )
        return lax.dynamic_update_slice_in_dim(result, attended.astype(jnp.bfloat16), row_start, 3)

    result = jnp.zeros(query_split.shape, jnp.bfloat16)
    result = lax.fori_loop(0, block_count, one_block, result)
    return result.reshape(query_heads.shape)


def plain_form(queries, keys, values, q_gain, k_gain, w_out):
    sp_count = lax.axis_size("sp")
    tok_rows = queries.shape[2]
    seq_len = tok_rows * sp_count
    cos_table, sin_table = rotary_tables(lax.axis_index("sp") * tok_rows, tok_rows)
    query_rot = normalize_turn(queries[0], q_gain, cos_table, sin_table)
    key_rot = normalize_turn(keys[0], k_gain, cos_table, sin_table)
    value_rows = values[0].reshape(KV, HD, tok_rows)
    query_heads = lax.all_to_all(query_rot, "sp", split_axis=0, concat_axis=2, tiled=True)
    share_count = max(sp_count // KV, 1)
    part_rows = tok_rows // share_count
    key_cut = (
        key_rot.reshape(KV, HD, share_count, part_rows)
        .transpose(0, 2, 1, 3)
        .reshape(KV * share_count, HD, part_rows)
    )
    value_cut = (
        value_rows.reshape(KV, HD, share_count, part_rows)
        .transpose(0, 2, 1, 3)
        .reshape(KV * share_count, HD, part_rows)
    )
    key_got, value_got = (
        lax.all_to_all(key_cut, "sp", split_axis=0, concat_axis=2, tiled=True),
        lax.all_to_all(value_cut, "sp", split_axis=0, concat_axis=2, tiled=True),
    )
    kv_local = key_got.shape[0]
    key_got = key_got.reshape(kv_local, HD, sp_count, part_rows)
    value_got = value_got.reshape(kv_local, HD, sp_count, part_rows)
    for bit_index in range(share_count.bit_length() - 1):
        key_other, value_other = swapped((key_got, value_got), "sp", bit_index)
        key_got = jnp.concatenate([key_got, key_other], axis=3)
        value_got = jnp.concatenate([value_got, value_other], axis=3)
    key_heads = key_got.reshape(kv_local, HD, seq_len)
    value_heads = value_got.reshape(kv_local, HD, seq_len)
    attended = attention_heads(query_heads, key_heads, value_heads, seq_len)
    token_heads = lax.all_to_all(attended, "sp", split_axis=2, concat_axis=0, tiled=True)
    token_rows = token_heads.reshape(QH * HD, tok_rows)
    product = lax.dot_general(
        token_rows,
        lax.all_gather(w_out, "dp", axis=1, tiled=True),
        (((0,), (0,)), ((), ())),
        preferred_element_type=jnp.float32,
    )
    mixed_rows = product.astype(jnp.bfloat16)
    return mixed_rows[None]


TILE = 128


def rotary_lanes(first_row, row_count):
    position = first_row + lax.broadcasted_iota(jnp.int32, (row_count, TILE), 0)
    lane = lax.broadcasted_iota(jnp.int32, (row_count, TILE), 1) % HD
    quarter = HD // 4
    index = lax.broadcasted_iota(jnp.int32, (1, TILE), 1) % quarter
    inv_freq = jnp.zeros((1, TILE), jnp.float32)
    for i in range(quarter):
        inv_freq = jnp.where(index == i, rotary_base ** (-(2.0 * i) / (HD // 2)), inv_freq)
    place = jnp.where(lane < HD // 2, position // GRID_W, position % GRID_W).astype(jnp.float32)
    angle = inv_freq * place
    sine = jnp.sin(angle)
    return jnp.cos(angle), jnp.where((lane // quarter) % 2 == 0, -sine, sine)


def turn_kernel(groups, chunks, *refs):
    sources, gain_ref, out_refs, held, sems = refs[:3], refs[3], refs[4:-4], refs[-4:-1], refs[-1]
    q_ref, k_ref, v_ref = held
    copies = [pltpu.make_async_copy(src, dst, sems.at[i]) for i, (src, dst) in enumerate(zip(sources, held))]
    for copy in copies:
        copy.start()
    quarter = HD // 4
    home = home_of(groups)
    row_head = (lax.broadcasted_iota(jnp.int32, (2 * TILE, TILE), 0) % TILE) // HD
    col_head = lax.broadcasted_iota(jnp.int32, (2 * TILE, TILE), 1) // HD
    average = jnp.where(row_head == col_head, 1.0 / HD, 0.0).astype(jnp.bfloat16)
    tok = q_ref.shape[0]
    cos_table, sin_table = rotary_lanes(lax.axis_index("sp") * tok, tok)
    even = (lax.broadcasted_iota(jnp.int32, cos_table.shape, 1) // quarter) % 2 == 0
    for copy in copies:
        copy.wait()
    q_gain, k_gain = gain_ref[0:1, :], gain_ref[1:2, :]

    def turned(tile, gain):
        field = tile.astype(jnp.float32)
        square = field * field
        coarse = square.astype(jnp.bfloat16)
        fine = (square - coarse.astype(jnp.float32)).astype(jnp.bfloat16)
        mean = jnp.dot(
            jnp.concatenate([coarse, fine], axis=1), average, preferred_element_type=jnp.float32
        )
        normed = field * lax.rsqrt(mean + epsilon) * gain
        partner = jnp.where(even, pltpu.roll(normed, TILE - quarter, 1), pltpu.roll(normed, quarter, 1))
        return (normed * cos_table + partner * sin_table).astype(jnp.bfloat16)

    for c in range(chunks):
        for j in range(groups):
            place = (home ^ j) * chunks + c
            both, kv = out_refs[c * groups + j], out_refs[groups * chunks + c * groups + j]
            for p in range(2):
                lanes = pl.ds(pl.multiple_of((place * 2 + p) * TILE, TILE), TILE)
                both[:, p * TILE : (p + 1) * TILE] = turned(q_ref[:, lanes], q_gain)
            lanes = pl.ds(pl.multiple_of(place * TILE, TILE), TILE)
            key, value = turned(k_ref[:, lanes], k_gain), v_ref[:, lanes]
            both[:, 2 * TILE : 3 * TILE] = key
            both[:, 3 * TILE :] = value
            kv[:, :TILE] = key
            kv[:, TILE:] = value


def in_vmem(count):
    return [pl.BlockSpec(memory_space=pltpu.VMEM)] * count


def params(mib):
    return pltpu.CompilerParams(vmem_limit_bytes=mib << 20)


def turn_and_pack(queries, keys, values, q_gain, k_gain, groups, chunks):
    tok = queries.shape[0]
    made = groups * chunks
    shapes = [jax.ShapeDtypeStruct((tok, 4 * TILE), jnp.bfloat16)] * made
    shapes += [jax.ShapeDtypeStruct((tok, 2 * TILE), jnp.bfloat16)] * made
    out = pl.pallas_call(
        functools.partial(turn_kernel, groups, chunks),
        in_specs=[pl.BlockSpec(memory_space=pltpu.HBM)] * 3 + in_vmem(1),
        out_specs=in_vmem(2 * made),
        out_shape=shapes,
        scratch_shapes=[pltpu.VMEM(x.shape, x.dtype) for x in (queries, keys, values)]
        + [pltpu.SemaphoreType.DMA((3,))],
        compiler_params=params(52),
        cost_estimate=pl.CostEstimate(flops=40 * 3072 * tok, bytes_accessed=6 * 4096 * tok, transcendentals=0),
        name="turn",
    )(queries, keys, values, jnp.concatenate([q_gain, q_gain, k_gain, k_gain]).reshape(2, TILE))
    both = [out[c * groups : (c + 1) * groups] for c in range(chunks)]
    kv = [out[made + c * groups : made + (c + 1) * groups] for c in range(chunks)]
    return both, kv


def spread_tiles(tiles, out_ref):
    rows = tiles[0].shape[0]
    half = len(tiles) * rows
    low = lax.broadcasted_iota(jnp.int32, (rows, TILE), 1) < HD
    for i, tile in enumerate(tiles):
        tile = tile.astype(jnp.float32)
        other = pltpu.roll(tile, HD, 1)
        here = slice(i * rows, (i + 1) * rows)
        there = slice(half + i * rows, half + (i + 1) * rows)
        out_ref[0, here, :] = jnp.where(low, tile, 0.0).astype(jnp.bfloat16)
        out_ref[0, there, :] = jnp.where(low, 0.0, other).astype(jnp.bfloat16)
        out_ref[1, here, :] = jnp.where(low, other, 0.0).astype(jnp.bfloat16)
        out_ref[1, there, :] = jnp.where(low, 0.0, tile).astype(jnp.bfloat16)


def near_kernel(*refs):
    spread_tiles([ref[:, 2 * TILE : 3 * TILE] for ref in refs[:-1]], refs[-1])


def far_kernel(*refs):
    groups = len(refs[:-2]) // 2
    near_refs, far_refs, (keys_ref, vals_ref) = refs[:groups], refs[groups : 2 * groups], refs[-2:]
    spread_tiles([ref[:, :TILE] for ref in far_refs], keys_ref)
    spread_tiles([ref[:, 3 * TILE :] for ref in near_refs] + [ref[:, TILE:] for ref in far_refs], vals_ref)


def spread(kernel, sources, made):
    rows = GROUP * sources[0].shape[0]
    return pl.pallas_call(
        kernel,
        in_specs=in_vmem(len(sources)),
        out_specs=in_vmem(len(made)),
        out_shape=[jax.ShapeDtypeStruct((2, count * rows, TILE), jnp.bfloat16) for count in made],
        compiler_params=params(16),
        cost_estimate=pl.CostEstimate(flops=1 << 21, bytes_accessed=1 << 21, transcendentals=0),
        name="spread",
    )(*sources)


def score(query_refs, keys_ref, p):
    query = jnp.concatenate([ref[:, p * TILE : (p + 1) * TILE] for ref in query_refs], axis=0)
    return lax.dot_general(query, keys_ref[p], (((1,), (1,)), ((), ())), preferred_element_type=jnp.float32)


def score_kernel(*refs):
    for p in range(2):
        refs[-1][p] = score(refs[:-2], refs[-2], p)


def early_scores(near, keys):
    rows = len(near) * near[0].shape[0]
    return pl.pallas_call(
        score_kernel,
        in_specs=in_vmem(len(near) + 1),
        out_specs=pl.BlockSpec(memory_space=pltpu.VMEM),
        out_shape=jax.ShapeDtypeStruct((2, rows, keys.shape[1]), jnp.float32),
        compiler_params=params(16),
        cost_estimate=pl.CostEstimate(
            flops=4 * rows * keys.shape[1] * TILE, bytes_accessed=1 << 22, transcendentals=0
        ),
        name="score",
    )(*near, keys)


SOFT_ROWS = 8


def attend_kernel(count, given, *refs):
    query_refs, (near_keys, far_keys, vals), refs = refs[:count], refs[count : count + 3], refs[count + 3 :]
    out_refs, (near_s, far_s, w_scr) = refs[given : given + count], refs[given + count :]
    if given:
        near_s = refs[0]
    rows = query_refs[0].shape[0]
    half = near_keys.shape[1] // GROUP
    wide = near_keys.shape[1]
    factor = HD ** (-0.5) * 1.4426950408889634

    def scores(p):
        if not given:
            near_s[p] = score(query_refs, near_keys, p)
        far_s[p] = score(query_refs, far_keys, p)

    scores(0)
    for p in range(2):
        if p == 0:
            scores(1)
        for g in range(GROUP):
            lanes = slice(g * half, (g + 1) * half)
            for r in range(0, count * rows, SOFT_ROWS):
                s = jnp.concatenate([part[p, r : r + SOFT_ROWS, lanes] for part in (near_s, far_s)], axis=1)
                e = jnp.exp2((s - jnp.max(s, axis=-1, keepdims=True)) * factor)
                w = e * (1.0 / jnp.sum(e, axis=-1, keepdims=True))
                w_scr[p, r : r + SOFT_ROWS, g * wide : (g + 1) * wide] = w.astype(jnp.bfloat16)
        attended = jnp.dot(w_scr[p], vals[p], preferred_element_type=jnp.float32).astype(jnp.bfloat16)
        for i, out_ref in enumerate(out_refs):
            out_ref[:, p * TILE : (p + 1) * TILE] = attended[i * rows : (i + 1) * rows]


def attend(near, ready, early=None):
    count, rows = len(near), near[0].shape[0]
    wide = ready[0].shape[1]
    given = [] if early is None else [early]
    held = count * rows if early is None else SOFT_ROWS
    return pl.pallas_call(
        functools.partial(attend_kernel, count, len(given)),
        in_specs=in_vmem(count + 3 + len(given)),
        out_specs=in_vmem(count),
        out_shape=[jax.ShapeDtypeStruct((rows, 2 * TILE), jnp.bfloat16)] * count,
        scratch_shapes=[
            pltpu.VMEM((2, held, wide), jnp.float32),
            pltpu.VMEM((2, count * rows, wide), jnp.float32),
            pltpu.VMEM((2, count * rows, 2 * wide), jnp.bfloat16),
        ],
        compiler_params=params(32),
        cost_estimate=pl.CostEstimate(
            flops=16 * count * rows * wide * TILE, bytes_accessed=8 * wide * TILE, transcendentals=0
        ),
        name="attend",
    )(*near, *ready, *given)


def home_of(groups):
    return lax.axis_index("sp") % groups


def term(att_ref, w_ref, groups, j, c):
    deep = w_ref.shape[0] // groups
    start = pl.multiple_of((home_of(groups) ^ j) * deep + c * 2 * TILE, 2 * TILE)
    return jnp.dot(att_ref[...], w_ref[pl.ds(start, 2 * TILE), :], preferred_element_type=jnp.float32)


def first_kernel(groups, *refs):
    att_refs, own_ref, w_refs, sums = refs[:groups], refs[groups], refs[groups + 1 : groups + 4], refs[groups + 4 :]
    for w_ref, sum_ref in zip(w_refs, sums):
        total = term(own_ref, w_ref, groups, 0, 1)
        for j in range(groups):
            total = total + term(att_refs[j], w_ref, groups, j, 0)
        sum_ref[...] = total


def second_kernel(groups, *refs):
    parts, refs = (refs[:groups], refs[groups : 2 * groups]), refs[2 * groups :]
    w_refs, sums, made, whole_ref = refs[0:3], refs[3:6], refs[6:9], refs[9]
    for w_ref, sum_ref, made_ref in zip(w_refs, sums, made):
        total = sum_ref[...]
        for j in range(1, groups):
            total = total + term(parts[1][j], w_ref, groups, j, 1)
        made_ref[...] = total.astype(jnp.bfloat16)
    for c in range(2):
        for j in range(groups):
            start = pl.multiple_of(((home_of(groups) ^ j) * 2 + c) * 2 * TILE, 2 * TILE)
            whole_ref[:, pl.ds(start, 2 * TILE)] = parts[c][j][...]


def third_kernel(groups, *refs):
    whole_ref, source, made, (out_ref, last, sems) = refs[0], refs[1], refs[2:5], refs[5:]
    width, tok = source.shape[1], whole_ref.shape[0]
    half = tok // 2
    column = lambda i: pl.ds(pl.multiple_of((lax.axis_index("dp") ^ i) * width, width), width)

    def leave(ready, rows, lanes, n):
        copy = pltpu.make_async_copy(ready, out_ref.at[rows, lanes], sems.at[n])
        copy.start()
        return copy

    leaving = [leave(ready, slice(0, tok), column(i), i) for i, ready in enumerate(made)]
    total = jnp.dot(whole_ref[...], source[...], preferred_element_type=jnp.float32).astype(jnp.bfloat16)
    for n in range(2):
        last[n] = total[n * half : (n + 1) * half]
        leaving.append(leave(last.at[n], slice(n * half, (n + 1) * half), column(3), 3 + n))
    for copy in leaving:
        copy.wait()


def project_call(kernel, groups, inputs, out_shape, scratch, flops):
    many = isinstance(out_shape, list)
    return pl.pallas_call(
        functools.partial(kernel, groups),
        in_specs=in_vmem(len(inputs)),
        out_specs=in_vmem(len(out_shape)) if many else pl.BlockSpec(memory_space=pl.ANY),
        out_shape=out_shape,
        scratch_shapes=scratch,
        compiler_params=params(16),
        cost_estimate=pl.CostEstimate(flops=flops, bytes_accessed=1 << 22, transcendentals=0),
        name="project",
    )(*inputs)


def exchanged(block, axis, flip):
    count = lax.axis_size(axis)
    return lax.ppermute(block, axis, [(i, i ^ flip) for i in range(count)])


def group_form(queries, keys, values, q_gain, k_gain, w_out):
    sp_count = lax.axis_size("sp")
    tok = queries.shape[2]
    groups = sp_count // 2
    chunks = KV // groups // 2
    width = w_out.shape[1]
    across = exchanged(w_out, "dp", 2)
    beside = exchanged(w_out, "dp", 1)
    corner = exchanged(across, "dp", 1)
    both, kv = turn_and_pack(queries[0].T, keys[0].T, values[0].T, q_gain, k_gain, groups, chunks)
    near, far = [], []
    for c in range(chunks):
        near.append([both[c][0]] + [exchanged(both[c][j], "sp", j) for j in range(1, groups)])
        far.append([exchanged(kv[c][j], "sp", groups + j) for j in range(groups)])
    back = []
    for c in range(chunks):
        early = None
        (near_keys,) = spread(near_kernel, near[c], [groups])
        if c:
            early = early_scores(near[c][1:], near_keys)
        ready = [near_keys, *spread(far_kernel, near[c] + far[c], [groups, 2 * groups])]
        away = attend(near[c][1:], ready, early)
        local = attend(near[c][:1], ready)
        back.append(list(local) + [exchanged(away[j - 1], "sp", j) for j in range(1, groups)])

    near_blocks = [w_out, beside, across]
    block = lambda dtype: jax.ShapeDtypeStruct((tok, width), dtype)
    flops = 2 * tok * w_out.shape[0] * width
    sums = project_call(
        first_kernel, groups, [*back[0], back[1][0], *near_blocks], [block(jnp.float32)] * 3, [], 2 * flops
    )
    *made, whole = project_call(
        second_kernel,
        groups,
        [*back[0], *back[1], *near_blocks, *sums],
        [block(jnp.bfloat16)] * 3 + [jax.ShapeDtypeStruct((tok, w_out.shape[0]), jnp.bfloat16)],
        [],
        flops,
    )
    mixed = project_call(
        third_kernel,
        groups,
        [whole, corner, *made],
        jax.ShapeDtypeStruct((tok, 4 * width), jnp.bfloat16),
        [pltpu.VMEM((2, tok // 2, width), jnp.bfloat16), pltpu.SemaphoreType.DMA((5,))],
        flops,
    )
    return mixed[None]


def grouped(sp_count, dp_count):
    return dp_count == 4 and KV == 2 * sp_count and sp_count // 2 == 4


def on_device(*args):
    if grouped(lax.axis_size("sp"), lax.axis_size("dp")):
        return group_form(*args)
    return plain_form(*args)


def solution(mesh):
    placed = (
        P("dp", None, "sp"),
        P("dp", None, "sp"),
        P("dp", None, "sp"),
        P(),
        P(),
        P(None, "dp"),
    )
    return jax.shard_map(
        on_device, mesh=mesh, in_specs=placed, out_specs=P("dp", "sp", None), check_vma=False
    )
```
